32 devices in a mesh: sp: 4 (over z), fs: 4 (over y, x), tp: 2 (over core).
Axes of the slice: x: 2, y: 2, z: 4, core: 2. Of those that a mesh axis runs over, the one named last changes fastest.
Arguments:
- tokens: bfloat16 [4, 1024, 2048], P('fs', 'sp', 'tp'), may hold values from -6 to 6
- norm_gain: float32 [2048], replicated, may hold values from 0.1 to 1.9
- w_query: bfloat16 [2048, 1024], P(('sp', 'fs'), 'tp'), may hold values from -0.125 to 0.125
- forget_weight: bfloat16 [2048, 1024], P(('sp', 'fs'), 'tp'), may hold values from -0.125 to 0.125
- w_input: bfloat16 [2048, 1024], P(('sp', 'fs'), 'tp'), may hold values from -8 to 8
- w_outgate: bfloat16 [2048, 1024], P(('sp', 'fs'), 'tp'), may hold values from -0.125 to 0.125
- w_pool: bfloat16 [2048, 1024], P(('sp', 'fs'), 'tp'), may hold values from -0.125 to 0.125
- forget_gap: float32 [1024], P('tp'), may hold values from 0 to 0.07
- extra_decay: float32 [4, 1024, 8], P('fs', 'sp', 'tp'), may hold values from -0.61 to 0
- rec_gain: float32 [1024], P('tp'), may hold values from 0.1 to 1.9
- group_weight: bfloat16 [4, 256, 256], replicated, may hold values from -0.375 to 0.375
- pool_gain: float32 [1024], P('tp'), may hold values from 0.1 to 1.9
- recurrent_output_weight: bfloat16 [1024, 2048], P('tp', ('sp', 'fs')), may hold values from -0.1875 to 0.1875
- w_out_pool: bfloat16 [1024, 2048], P('tp', ('sp', 'fs')), may hold values from -0.1875 to 0.1875
Outputs:
- mixed_out: bfloat16 [4, 1024, 2048], P('fs', ('sp', 'tp'))
The draws below stay inside these ranges and needn't reach their ends.
All inputs are finite; a program needn't handle non-finite values.
Results may differ from the reference program's by a relative error of at most 0.011.
Values may be sent and summed in bfloat16 or wider, within the bound.
A program may use at most 64 MiB of HBM per device.

```python
import math
import jax
import jax.numpy as jnp
from jax import lax

D = 2048
HGRN_HEADS = 8
HEAD_DIM = 128
D_HGRN = 1024
D_POOL = 1024
POOL_GROUPS = 4
GROUP_DIM = 256
BLOCK = 64
TOK_DEV = 256
SEQ_LEN = 1024
SEQS = 4
N_TP = 2


def head_speeds(key):
    order = jax.random.permutation(jax.random.fold_in(key, 17), HGRN_HEADS)
    fast_count = HGRN_HEADS // 2
    return order < fast_count


def draw_forget_gap(key, part):
    fast_heads = head_speeds(key)
    spread = jax.random.uniform(jax.random.fold_in(key, 5), (HGRN_HEADS, HEAD_DIM), jnp.float32)
    fast_gap = 0.025 * jnp.exp(spread * math.log(2.8))
    slow_gap = 0.3 * jnp.exp(spread * math.log(4.0)) / SEQ_LEN
    return jnp.where(fast_heads[:, None], fast_gap, slow_gap).reshape(D_HGRN).astype(jnp.float32)


def draw_w_input(key, part):
    fast_heads = head_speeds(key)
    normal_draw = jnp.clip(jax.random.normal(jax.random.fold_in(key, 3), (D, D_HGRN), jnp.float32), -6.0, 6.0)
    slow_scale = math.sqrt(SEQ_LEN) / 4.0
    column_scale = jnp.repeat(jnp.where(fast_heads, 1.0, slow_scale), HEAD_DIM)
    return (normal_draw * column_scale[None, :] / math.sqrt(D)).astype(jnp.bfloat16)


def draw_extra_decay(key, part):
    base_key = jax.random.fold_in(key, 9)
    rate_key, spot_key, depth_key = jax.random.split(base_key, 3)
    block_total = SEQ_LEN // TOK_DEV
    level = jax.random.uniform(rate_key, (SEQS, block_total, 1, HGRN_HEADS), jnp.float32)
    shrink_factor_list = 0.15 * jnp.exp(level * math.log(4.0)) / SEQ_LEN
    shrink_factor_list = jnp.broadcast_to(shrink_factor_list, (SEQS, block_total, TOK_DEV, HGRN_HEADS)).reshape(SEQS, SEQ_LEN, HGRN_HEADS)
    first_spot = jax.random.randint(jax.random.fold_in(spot_key, 1), (SEQS, 1, HGRN_HEADS, 1), 0, SEQ_LEN)
    spot_offset = jax.random.randint(jax.random.fold_in(spot_key, 2), (SEQS, 1, HGRN_HEADS, 1), 1, SEQ_LEN)
    second_spot = (first_spot + spot_offset) % SEQ_LEN
    probe_locations = jnp.concatenate([first_spot, second_spot], axis=3)
    layer_tiers = jnp.log(0.55 + 0.25 * jax.random.uniform(depth_key, (SEQS, 1, HGRN_HEADS, 2), jnp.float32))
    symbol_indices = jnp.arange(SEQ_LEN, dtype=jnp.int32)[None, :, None, None]
    spike_clusters = jnp.sum(jnp.where(symbol_indices == probe_locations, layer_tiers, 0.0), axis=3)
    return (spike_clusters - shrink_factor_list).astype(jnp.float32)


def level_of(key, dims, cuts, smallest, largest):
    gain = 1.0
    for axis_at, shards_of in cuts:
        draws = jax.random.uniform(jax.random.fold_in(jax.random.fold_in(key, 6), axis_at), (shards_of,), jnp.float32, smallest / len(cuts), largest / len(cuts))
        gain = gain * jnp.repeat(jnp.exp(draws), dims[axis_at] // shards_of).reshape((-1,) + (1,) * (len(dims) - 1 - axis_at))
    return gain


def noise(key, extent, scale, bound, cuts=(), held_as=jnp.bfloat16):
    drawn = jax.random.normal(key, extent, jnp.float32) * scale
    if len(cuts) > 0:
        drawn = level_of(key, extent, cuts, -0.22, 0.18) * drawn
    return jnp.clip(drawn, min=-bound, max=bound).astype(held_as)


def setup_inputs(seed: int = 0) -> dict:
    key_list = jax.random.split(jax.random.key(seed), 15)
    return {
        "tokens": noise(key_list[0], (SEQS, SEQ_LEN, D), 1.0, 6.0, ((0, 4), (1, 4), (2, 2))),
        "norm_gain": jnp.clip(1.0 + 0.18 * jax.random.normal(key_list[1], (D,), jnp.float32), 0.1, 1.9),
        "w_query": noise(key_list[2], (D, D_HGRN), D ** -0.5, 0.125, ((0, 16), (1, 2))),
        "forget_weight": noise(key_list[3], (D, D_HGRN), D ** -0.5, 0.125, ((0, 16), (1, 2))),
        "w_input": draw_w_input(jax.random.fold_in(key_list[14], 71), 0),
        "w_outgate": noise(key_list[5], (D, D_HGRN), D ** -0.5, 0.125, ((0, 16), (1, 2))),
        "w_pool": noise(key_list[6], (D, D_POOL), D ** -0.5, 0.125, ((0, 16), (1, 2))),
        "forget_gap": draw_forget_gap(jax.random.fold_in(key_list[14], 71), 0),
        "extra_decay": draw_extra_decay(jax.random.fold_in(key_list[14], 71), 0),
        "rec_gain": jnp.clip(1.0 + 0.18 * jax.random.normal(key_list[9], (D_HGRN,), jnp.float32), 0.1, 1.9),
        "group_weight": noise(key_list[10], (POOL_GROUPS, GROUP_DIM, GROUP_DIM), GROUP_DIM ** -0.5, 0.375),
        "pool_gain": jnp.clip(1.0 + 0.18 * jax.random.normal(key_list[11], (D_POOL,), jnp.float32), 0.1, 1.9),
        "recurrent_output_weight": noise(key_list[12], (D_HGRN, D), D_HGRN ** -0.5, 0.1875, ((0, 2), (1, 16))),
        "w_out_pool": noise(key_list[13], (D_POOL, D), D_POOL ** -0.5, 0.1875, ((0, 2), (1, 16))),
    }


EPS = 1e-06
HIGH = lax.Precision.HIGHEST

def recurrence(queries, input_gate, values, log_forget):
    block_count = queries.shape[0] // BLOCK
    shaped = tuple((arr.reshape(block_count, BLOCK, HGRN_HEADS, HEAD_DIM) for arr in (queries, input_gate, values, log_forget)))
    causal = jnp.tril(jnp.ones((BLOCK, BLOCK), jnp.bool_))

    def advance(carried, pieces):
        q_blk, k_blk, v_blk, g_blk = pieces
        within = jnp.cumsum(g_blk, axis=0)
        block_end = within[-1]
        q_up = q_blk * jnp.exp(within)
        scores = jnp.einsum('thd,shd->hts', q_up, k_blk * jnp.exp(-within), precision=HIGH)
        scores = jnp.where(causal, scores, 0.0)
        result = jnp.einsum('hts,she->the', scores, v_blk, precision=HIGH)
        result = result + jnp.einsum('thd,hde->the', q_up, carried, precision=HIGH)
        fresh_input = jnp.einsum('shd,she->hde', k_blk * jnp.exp(block_end[None] - within), v_blk, precision=HIGH)
        carried = jnp.exp(block_end)[:, :, None] * carried + fresh_input
        return (carried, result)
    initial = jnp.zeros((HGRN_HEADS, HEAD_DIM, HEAD_DIM), jnp.float32)
    _, results = lax.scan(advance, initial, shaped)
    return results.reshape(queries.shape[0], D_HGRN)

def pooling(z_pool, group_weight, pool_gain):
    seq_rows = z_pool.shape[0]
    reach_rows = 2 ** POOL_GROUPS
    values = z_pool.astype(jnp.float32)
    padded = jnp.pad(values, ((reach_rows, 0), (0, 0)))
    symbol_indices = jnp.arange(seq_rows, dtype=jnp.int32)
    outputs = []
    for group_idx in range(POOL_GROUPS):
        window_len = 2 ** (group_idx + 1)
        lowest_column_index = group_idx * GROUP_DIM
        high_col = lowest_column_index + GROUP_DIM
        window = padded[reach_rows:reach_rows + seq_rows, lowest_column_index:high_col]
        for shift_idx in range(1, window_len):
            window = window + padded[reach_rows - shift_idx:reach_rows - shift_idx + seq_rows, lowest_column_index:high_col]
        counts_here = jnp.minimum(symbol_indices + 1, window_len).astype(jnp.float32)[:, None]
        pooled = (window / counts_here - values[:, lowest_column_index:high_col]).astype(jnp.bfloat16)
        mapped = jnp.dot(pooled, group_weight[group_idx], preferred_element_type=jnp.float32)
        outputs.append((mapped * pool_gain[lowest_column_index:high_col]).astype(jnp.bfloat16))
    return jnp.concatenate(outputs, axis=1)

def one_sequence(tokens_seq, extra_seq, weights):
    norm_gain, w_query, forget_weight, w_input, w_outgate, w_pool, forget_gap, rec_gain, group_weight, pool_gain, recurrent_output_weight, w_out_pool = weights
    features_f = tokens_seq.astype(jnp.float32)
    token_scale = lax.rsqrt(lax.optimization_barrier(jnp.mean(features_f * features_f, axis=-1, keepdims=True)) + EPS)
    normed = (features_f * token_scale * norm_gain).astype(jnp.bfloat16)

    def project(matrix):
        return jnp.dot(normed, matrix, preferred_element_type=jnp.float32).astype(jnp.bfloat16)
    z_query = project(w_query)
    z_forget = project(forget_weight)
    z_input = project(w_input)
    z_outgate = project(w_outgate)
    z_pool = project(w_pool)
    input_gate = forget_gap * jax.nn.sigmoid(-z_forget.astype(jnp.float32))
    log_forget = jnp.log1p(-input_gate) + jnp.repeat(extra_seq, HEAD_DIM, axis=1)
    queries = jax.nn.silu(z_query.astype(jnp.float32))
    recurrent = recurrence(queries, input_gate, z_input.astype(jnp.float32), log_forget)
    rec_scale = lax.rsqrt(lax.optimization_barrier(jnp.mean(recurrent * recurrent, axis=-1, keepdims=True)) + EPS)
    recurrent_output = (recurrent * rec_scale * rec_gain * jax.nn.silu(z_outgate.astype(jnp.float32))).astype(jnp.bfloat16)
    pool_out = pooling(z_pool, group_weight, pool_gain)
    rec_rows = D_HGRN // N_TP
    pool_rows = D_POOL // N_TP
    summed_out = jnp.zeros((tokens_seq.shape[0], D), jnp.float32)
    for block_idx in range(N_TP):
        rec_lo = block_idx * rec_rows
        pool_lo = block_idx * pool_rows
        partial_sum = jnp.dot(recurrent_output[:, rec_lo:rec_lo + rec_rows], recurrent_output_weight[rec_lo:rec_lo + rec_rows], preferred_element_type=jnp.float32) + jnp.dot(pool_out[:, pool_lo:pool_lo + pool_rows], w_out_pool[pool_lo:pool_lo + pool_rows], preferred_element_type=jnp.float32)
        rounded = lax.optimization_barrier(partial_sum.astype(jnp.bfloat16))
        summed_out = summed_out + rounded.astype(jnp.float32)
    return summed_out.astype(jnp.bfloat16)

def reference(tokens, norm_gain, w_query, forget_weight, w_input, w_outgate, w_pool, forget_gap, extra_decay, rec_gain, group_weight, pool_gain, recurrent_output_weight, w_out_pool):
    weights = (norm_gain, w_query, forget_weight, w_input, w_outgate, w_pool, forget_gap, rec_gain, group_weight, pool_gain, recurrent_output_weight, w_out_pool)

    def per_sequence(pair):
        return one_sequence(pair[0], pair[1], weights)
    return lax.map(per_sequence, (tokens, extra_decay))
```

```python
import functools
import jax
import jax.numpy as jnp
from jax import lax
from jax.experimental import pallas as pl
from jax.experimental.pallas import tpu as pltpu
from jax.sharding import PartitionSpec as P

HEAD_DIM = 128
POOL_GROUPS = 4
BLOCK = 64
EPS = 1e-06
HIGH = lax.Precision.HIGHEST
MESH = pl.DeviceIdType.MESH
BF = jnp.bfloat16
F32 = jnp.float32


def place():
    return lax.axis_index("sp"), lax.axis_index("fs"), lax.axis_index("tp")


def rcopy(src, dst, ssem, rsem, dev):
    return pltpu.make_async_remote_copy(
        src_ref=src, dst_ref=dst, send_sem=ssem, recv_sem=rsem, device_id=dev, device_id_type=MESH
    )


def greet(devs):
    barrier = pltpu.get_barrier_semaphore()
    for cond, dev in devs:
        def tell(dev=dev):
            pl.semaphore_signal(barrier, inc=1, device_id=dev, device_id_type=MESH)
        if cond is None:
            tell()
        else:
            pl.when(cond)(tell)
    pl.semaphore_wait(barrier, sum(1 if cond is None else jnp.where(cond, 1, 0) for cond, _ in devs))


def square(f):
    near = f + 1 - 2 * lax.rem(f, 2)
    return near, lax.rem(f + 2, 4), lax.rem(near + 2, 4)


def project_kernel(
    n_sp, n_fs, n_tp, tok, wq, wf, wi, wo, wp, extra, gain, gmap, pgain, wor, wop, z_ref, e_ref, ow_ref,
    wsrc, xs, ws, acc, x_send, x_recv, f_send, d_send, d_recv, w_send, w_recv, zr_send, zl_send, e_send, e_recv,
):
    s, f, t = place()
    rows, half = tok.shape
    part = rows // 2
    mats = (wq, wf, wi, wo, wp)
    wr, width = wq.shape
    ch = width // n_fs
    for i, w in enumerate(mats):
        for g in range(n_fs):
            wsrc[g, :, i * ch : (i + 1) * ch] = w[:, g * ch : (g + 1) * ch]
    other = (s, f, 1 - t)
    px, py, pd = square(f)
    order = (f, px, py, pd)
    up, down = (s + 1, f, t), (s - 1, f, t)
    has_up, has_down = s < n_sp - 1, s > 0
    greet([(None, other)] + [(None, (s, g, t)) for g in order[1:]] + [(has_up, up), (has_down, down)])

    def cols(c):
        return pl.ds(pl.multiple_of(c * half, half), half)

    def span(a, b):
        return pl.ds(pl.multiple_of((a * n_fs + b) * wr, wr), wr)

    def slot(a, b):
        return ws.at[span(a, b), :]

    def to_up(src, a, b):
        return rcopy(src, slot(a, b), zr_send.at[a, b], w_recv.at[a, b], up)

    def to_down(src, a, b):
        return rcopy(src, slot(a, b), zl_send.at[a, b], w_recv.at[a, b], down)

    sends = []

    def send(c):
        c.start()
        sends.append(c)

    def x_slot(g, h, c):
        return xs.at[g, h * part : (h + 1) * part, cols(c)]

    own = wsrc.at[f]
    pl.when(has_up)(lambda: to_up(own, s, f).start())
    pl.when(has_down)(lambda: to_down(own, s, f).start())
    for i, g in enumerate((pd, px, py)):
        send(rcopy(wsrc.at[g], slot(s, f), w_send.at[i], w_recv.at[s, f], (s, g, t)))
    for i, (p, hs) in enumerate(((px, (0, 1)), (py, (1, 0)))):
        for h in hs:
            send(rcopy(tok.at[h * part : (h + 1) * part, :], x_slot(f, h, t), x_send.at[i, h], x_recv.at[f, h], (s, p, t)))
    for h in range(2):
        send(rcopy(tok.at[h * part : (h + 1) * part, :], x_slot(f, h, t), d_send.at[f, h], d_recv.at[f, h], other))
    for i, g in enumerate(order[1:]):
        send(rcopy(extra.at[g], e_ref.at[f], e_send.at[i], e_recv.at[f], (s, g, t)))
    ws[span(s, f), :] = wsrc[f]
    xs[f, :, cols(t)] = tok[...]
    e_ref[f] = extra[f]
    ow_ref[0:width, :] = wor[...]
    gd = gmap.shape[1]
    for i in range(width // gd):
        at = slice(i * gd, (i + 1) * gd)
        scaled = (gmap[t * (width // gd) + i].astype(F32) * pgain[:, at]).astype(BF)
        folded = jnp.dot(scaled, wop[at, :], preferred_element_type=F32)
        ow_ref[width + i * gd : width + (i + 1) * gd, :] = folded.astype(BF)

    for g in order[1:]:
        to_up(slot(s, g), s, g).wait_recv()
        pl.when(has_up)(lambda: to_up(slot(s, g), s, g).start())
        pl.when(has_down)(lambda: to_down(slot(s, g), s, g).start())

    def landed(g, h):
        here = x_slot(g, h, t)
        rcopy(here, here, d_send.at[g, h], x_recv.at[g, h], other).wait_recv()
        return here

    def hand_on(g, h, here):
        send(rcopy(here, here, d_send.at[g, h], d_recv.at[g, h], other))

    for i, (g, h, onto) in enumerate(((px, 0, py), (py, 1, px))):
        here = landed(g, h)
        send(rcopy(here, here, f_send.at[i], x_recv.at[g, h], (s, onto, t)))
        hand_on(g, h, here)

    def relay(d):
        for g in order:
            a = s - d

            @pl.when(a >= 0)
            def _():
                to_up(slot(a, g), a, g).wait_recv()
                pl.when(has_up)(lambda: to_up(slot(a, g), a, g).start())
            b = s + d

            @pl.when(b < n_sp)
            def _():
                to_down(slot(b, g), b, g).wait_recv()
                pl.when(has_down)(lambda: to_down(slot(b, g), b, g).start())

    def add(a):
        k = pl.ds(pl.multiple_of(a * n_fs * wr, n_fs * wr), n_fs * wr)

        def each(i, _):
            acc[i] += jnp.dot(xs[i, :, k], ws[k, :], preferred_element_type=F32)
            return 0

        lax.fori_loop(0, n_fs, each, 0)

    def multiply(d):
        pl.when(s - d >= 0)(lambda: add(s - d))
        pl.when(s + d < n_sp)(lambda: add(s + d))

    relay(1)
    for g, h in ((px, 1), (py, 0), (pd, 0), (pd, 1)):
        hand_on(g, h, landed(g, h))
    for d in range(2, n_sp - 1):
        relay(d)
    for g in order:
        for h in range(2):
            here = x_slot(g, h, 1 - t)
            rcopy(here, here, d_send.at[g, h], d_recv.at[g, h], other).wait_recv()
    for g in order[1:]:
        rcopy(extra.at[f], e_ref.at[g], e_send.at[0], e_recv.at[g], other).wait_recv()
    for c in sends:
        c.wait_send()

    def norm(j, _):
        tile = 16
        per = rows // tile
        at = (j // per, pl.ds(pl.multiple_of(lax.rem(j, per) * tile, tile), tile))
        feats = xs[at[0], at[1], :].astype(F32)
        scale = lax.rsqrt(jnp.mean(feats * feats, axis=-1, keepdims=True) + EPS)
        xs[at[0], at[1], :] = (feats * scale * gain[...]).astype(BF)
        return 0

    lax.fori_loop(0, n_fs * rows // 16, norm, 0, unroll=2)

    if n_fs * wr % 128 == 0:
        own_k = pl.ds(pl.multiple_of(s * n_fs * wr, n_fs * wr), n_fs * wr)

        def begin(i, _):
            acc[i] = jnp.dot(xs[i, :, own_k], ws[own_k, :], preferred_element_type=F32)
            return 0

        lax.fori_loop(0, n_fs, begin, 0)
        for d in range(1, n_sp - 1):
            multiply(d)
        relay(n_sp - 1)
        multiply(n_sp - 1)

        def finish(i, _):
            z_ref[i] = acc[i].astype(BF)
            return 0
    else:
        relay(n_sp - 1)

        def finish(i, _):
            z_ref[i] = jnp.dot(xs[i], ws[...], preferred_element_type=F32).astype(BF)
            return 0

    lax.fori_loop(0, n_fs, finish, 0)

    for d in range(n_sp):
        for g in order:
            a = s - d

            @pl.when((a >= 0) & has_up)
            def _():
                to_up(slot(a, g), a, g).wait_send()
            b = s + d

            @pl.when((b < n_sp) & has_down)
            def _():
                to_down(slot(b, g), b, g).wait_send()


def dot(a, b, dims):
    return lax.dot_general(a, b, (dims, ((), ())), precision=HIGH, preferred_element_type=F32)


def state_kernel(
    n_sp, group_dim, z, e_all, gap, rec_gain, act, sq_out,
    local, qd, own_st, own_de, st_in, de_in, rim, s_send, s_recv, c_send, c_recv, g_send, g_recv,
):
    s, f, t = place()
    n_fs, rows, _ = z.shape
    ch = HEAD_DIM
    reach = rim.shape[1]
    devs = []
    for d in range(1, n_sp):
        devs.append((s + d < n_sp, (s + d, f, t)))
        devs.append((s - d >= 0, (s - d, f, t)))
    greet(devs)
    edge = rcopy(z.at[:, rows - reach :, 4 * ch :], rim, g_send, g_recv, (s + 1, f, t))
    pl.when(s < n_sp - 1)(edge.start)
    mine = pl.ds(pl.multiple_of(f * ch, ch), ch)
    gap_f = gap[:, mine]
    gain_f = rec_gain[:, mine]
    at = lax.broadcasted_iota(jnp.int32, (BLOCK, BLOCK), 0)
    causal = at >= lax.broadcasted_iota(jnp.int32, (BLOCK, BLOCK), 1)
    lower = causal.astype(F32)

    def one(g, _):
        state = jnp.zeros((ch, ch), F32)
        so_far = jnp.zeros((1, ch), F32)
        e_cols = e_all[g].T
        for n in range(rows // BLOCK):
            here = slice(n * BLOCK, (n + 1) * BLOCK)
            q, fo, v = (z[g, here, i * ch : (i + 1) * ch].astype(F32) for i in range(3))
            q = jax.nn.silu(q)
            k = gap_f * jax.nn.sigmoid(-fo)
            lo = n * BLOCK % 128
            lane = n * BLOCK // 128
            logs = jnp.log1p(-k) + e_cols[lo : lo + BLOCK, lane : lane + 1]
            within = dot(lower, logs, ((1,), (0,)))
            end = within[BLOCK - 1 :]
            q_up = q * jnp.exp(within)
            scores = jnp.where(causal, dot(q_up, k * jnp.exp(-within), ((1,), (1,))), 0.0)
            out = dot(scores, v, ((1,), (0,)))
            if n:
                out = out + dot(q_up, state, ((1,), (1,)))
            local[g, here, :] = out
            qd[g, here, :] = q_up * jnp.exp(so_far)
            state = state * jnp.exp(end) + dot(v.T, k * jnp.exp(end - within), ((1,), (0,)))
            so_far = so_far + end
        own_st[g] = state.astype(BF)
        own_de[g] = jnp.broadcast_to(jnp.exp(so_far), (8, ch))
        return 0

    lax.fori_loop(0, n_fs, one, 0)

    def pair(d):
        dev = (s + d, f, t)
        return (
            rcopy(own_st, st_in.at[d - 1], s_send.at[d - 1], s_recv.at[d - 1], dev),
            rcopy(own_de, de_in.at[d - 1], c_send.at[d - 1], c_recv.at[d - 1], dev),
        )

    for d in range(1, n_sp):
        @pl.when(s + d < n_sp)
        def _():
            for c in pair(d):
                c.start()

        @pl.when(s - d < 0)
        def _():
            st_in[d - 1] = jnp.zeros(st_in.shape[1:], st_in.dtype)
            de_in[d - 1] = jnp.ones(de_in.shape[1:], de_in.dtype)
    pl.when(s == 0)(lambda: rim.__setitem__(Ellipsis, jnp.zeros(rim.shape, rim.dtype)))
    pl.when(s > 0)(edge.wait_recv)
    group = (t * n_fs * ch + f * ch) // group_dim
    spot = s * rows + lax.broadcasted_iota(jnp.int32, (rows, ch), 0)
    window = 2
    for level in range(1, POOL_GROUPS):
        window = jnp.where(group == level, 2 ** (level + 1), window)
    counts = jnp.minimum(spot + 1, window).astype(F32)
    for g in range(n_fs):
        zp = z[g, :, 4 * ch :].astype(F32)
        running = jnp.concatenate([rim[g].astype(F32), zp], axis=0)
        total = None
        for level in range(POOL_GROUPS):
            stride = 2**level
            running = running[stride:] + running[:-stride]
            now = running[running.shape[0] - rows :]
            total = now if level == 0 else jnp.where(group == level, now, total)
        act[1, g * rows : (g + 1) * rows, :] = (total / counts - zp).astype(BF)
    for d in range(1, n_sp):
        @pl.when(s - d >= 0)
        def _():
            for c in pair(d):
                c.wait_recv()

    ones = jnp.ones((8, ch), F32)

    def finish(g, _):
        total = jnp.zeros((ch, ch), F32)
        for d in range(n_sp - 2, -1, -1):
            total = de_in[d, g, 0:1, :] * total + st_in[d, g].astype(F32)
        rec = local[g] + dot(qd[g], total, ((1,), (1,)))
        sums = dot(ones, rec * rec, ((1,), (1,)))
        for i in range(rows // 128):
            sq_out[g, i : i + 1, :] = sums[0:1, i * 128 : (i + 1) * 128]
        gate = jax.nn.silu(z[g, :, 3 * ch : 4 * ch].astype(F32))
        act[0, pl.ds(pl.multiple_of(g * rows, rows), rows), :] = (rec * gain_f * gate).astype(BF)
        return 0

    sq_out[...] = jnp.zeros(sq_out.shape, F32)
    lax.fori_loop(0, n_fs, finish, 0)
    for d in range(1, n_sp):
        @pl.when(s + d < n_sp)
        def _():
            for c in pair(d):
                c.wait_send()
    pl.when(s < n_sp - 1)(edge.wait_send)


def mix_kernel(
    n_sp, n_fs, n_tp, act, sq, ow, final,
    out, acts, sq_all, ow_all, relay_buf, wbuf, part,
    a_send, a_recv, f_send, d_send, d_recv, q_send, q_recv,
    up_send, down_send, o_recv, od_send, od_recv, m_send, m_recv,
):
    s, f, t = place()
    n_half = n_sp // n_tp
    rows = act.shape[1] // n_fs
    half = rows // n_tp
    width, cw = ow.shape[0] // 2, ow.shape[1]
    other = (s, f, 1 - t)
    px, py, pd = square(f)
    up, down = (s + 1, f, t), (s - 1, f, t)
    has_up, has_down = s < n_sp - 1, s > 0
    greet(
        [(None, other)]
        + [(None, (s, g, u)) for g in (px, py, pd) for u in (t, 1 - t)]
        + [(has_up, up), (has_down, down)]
    )

    def to_up(src, a):
        return rcopy(src, relay_buf.at[a], up_send.at[a], o_recv.at[a], up)

    def to_down(src, a):
        return rcopy(src, relay_buf.at[a], down_send.at[a], o_recv.at[a], down)

    def to_other(src, a):
        return rcopy(src, ow_all.at[lax.rem(a, n_half), t], od_send.at[a], od_recv.at[a], other)

    def keep(src, a):
        mine = a // n_half == t

        @pl.when(mine)
        def _():
            ow_all[lax.rem(a, n_half), t] = src[...]

        pl.when(jnp.logical_not(mine))(lambda: to_other(src, a).start())

    sends = []

    def send(c):
        c.start()
        sends.append(c)

    for i, (p, order) in enumerate(((px, (0, 1)), (py, (1, 0)))):
        for h in order:
            send(rcopy(act.at[h], acts.at[t, f, h], a_send.at[i, h], a_recv.at[f, h], (s, p, t)))
    pl.when(has_up)(lambda: to_up(ow, s).start())
    pl.when(has_down)(lambda: to_down(ow, s).start())
    for h in range(2):
        send(rcopy(act.at[h], acts.at[t, f, h], d_send.at[f, h], d_recv.at[f, h], other))
    for i, g in enumerate((px, py, pd)):
        for u in range(n_tp):
            send(rcopy(sq, sq_all.at[t, f], q_send.at[i, u], q_recv.at[t, f], (s, g, u)))
    send(rcopy(sq, sq_all.at[t, f], q_send.at[n_fs - 1, 0], q_recv.at[t, f], other))
    acts[t, f] = act[...]
    sq_all[t, f] = sq[...]
    keep(ow, s)

    def landed(g, h):
        here = acts.at[t, g, h]
        rcopy(here, here, d_send.at[g, h], a_recv.at[g, h], other).wait_recv()
        return here

    def hand_on(g, h, here):
        send(rcopy(here, here, d_send.at[g, h], d_recv.at[g, h], other))

    for i, (g, h, onto) in enumerate(((px, 0, py), (py, 1, px))):
        here = landed(g, h)
        send(rcopy(here, here, f_send.at[i], a_recv.at[g, h], (s, onto, t)))
        hand_on(g, h, here)

    def step(d):
        a = s - d

        @pl.when(a >= 0)
        def _():
            to_up(relay_buf.at[a], a).wait_recv()
            pl.when(has_up)(lambda: to_up(relay_buf.at[a], a).start())
            keep(relay_buf.at[a], a)
        b = s + d

        @pl.when(b < n_sp)
        def _():
            to_down(relay_buf.at[b], b).wait_recv()
            pl.when(has_down)(lambda: to_down(relay_buf.at[b], b).start())
            keep(relay_buf.at[b], b)

    for d in range(1, n_sp):
        step(d)
    for g, h in ((px, 1), (py, 0), (pd, 0), (pd, 1)):
        hand_on(g, h, landed(g, h))
    for i in range(n_half):
        a = t * n_half + i
        here = ow_all.at[i, 1 - t]
        rcopy(here, here, od_send.at[a], od_recv.at[a], other).wait_recv()
    for i in range(n_half):
        for u in range(n_tp):
            for k in range(2):
                wbuf[k, u * width : (u + 1) * width, i * cw : (i + 1) * cw] = ow_all[i, u, k * width : (k + 1) * width, :]
    for g in (px, py, pd):
        for u in range(n_tp):
            here = sq_all.at[u, g]
            rcopy(here, here, q_send.at[0, 0], q_recv.at[u, g], other).wait_recv()
    here = sq_all.at[1 - t, f]
    rcopy(here, here, q_send.at[0, 0], q_recv.at[1 - t, f], other).wait_recv()
    for g in (f, px, py, pd):
        for h in range(2):
            here = acts.at[1 - t, g, h]
            rcopy(here, here, d_send.at[g, h], d_recv.at[g, h], other).wait_recv()

    def piece(g, u):
        return rcopy(part.at[g, u], out.at[f, t], m_send.at[g, u], m_recv.at[f, t], (s, g, u))

    def spread(g):
        for u in range(n_tp):
            c = piece(g, u)
            c.start()
            sends.append(c)

    last = None
    for g in (pd, f, px, py):
        here = pl.ds(pl.multiple_of(g * rows, rows), rows)
        sums = sum(sq_all[u, i, g] for u in range(n_tp) for i in range(n_fs))
        scale = lax.rsqrt(sums / (n_tp * width) + EPS).T
        scale = jnp.concatenate([scale[:, i : i + 1] for i in range(rows // 128)], axis=0)
        left = [
            jnp.concatenate([acts[u, i, h, here, :] for u in range(n_tp) for i in range(n_fs)], axis=1)
            for h in range(2)
        ]
        mixed = (
            jnp.dot(left[0], wbuf[0], preferred_element_type=F32) * scale
            + jnp.dot(left[1], wbuf[1], preferred_element_type=F32)
        ).astype(BF)
        for u in range(n_tp):
            part[g, u] = mixed[u * half : (u + 1) * half]
        if last is not None and last is not f:
            spread(last)
        if last is f:
            c = piece(f, 1 - t)
            c.start()
            sends.append(c)
        last = g
    out[f, t] = part[f, t]
    for i in range(n_half):
        to_other(ow, (1 - t) * n_half + i).wait_send()
    for d in range(n_sp):
        a, b = s - d, s + d

        @pl.when((a >= 0) & has_up)
        def _():
            to_up(ow, a).wait_send()

        @pl.when((b < n_sp) & has_down)
        def _():
            to_down(ow, b).wait_send()
    spread(last)
    for c in sends:
        c.wait_send()
    for g in (px, py, pd):
        for u in range(n_tp):
            here = out.at[g, u]
            rcopy(here, here, m_send.at[g, u], m_recv.at[g, u], other).wait_recv()
    here = out.at[f, 1 - t]
    rcopy(here, here, m_send.at[f, 1 - t], m_recv.at[f, 1 - t], other).wait_recv()
    for u in range(n_tp):
        for i in range(n_half):
            for g in range(n_fs):
                lo = ((u * n_half + i) * n_fs + g) * cw
                final[:, lo : lo + cw] = out[g, u, :, i * cw : (i + 1) * cw]


def vmem(count):
    return [pl.BlockSpec(memory_space=pltpu.VMEM)] * count


def dma(*shape):
    return pltpu.SemaphoreType.DMA(shape) if shape else pltpu.SemaphoreType.DMA


def comm(kernel, outs, scratch, number, name):
    return pl.pallas_call(
        kernel,
        out_shape=[jax.ShapeDtypeStruct(a, b) for a, b in outs],
        out_specs=vmem(len(outs)),
        scratch_shapes=scratch,
        compiler_params=pltpu.CompilerParams(
            collective_id=number, has_side_effects=True, vmem_limit_bytes=60 * 1024 * 1024
        ),
        name=name,
    )


def body(
    n_sp, n_fs, n_tp, tokens, norm_gain, w_query, forget_weight, w_input, w_outgate, w_pool, forget_gap,
    extra_decay, rec_gain, group_weight, pool_gain, recurrent_output_weight, w_out_pool,
):
    s, f, t = place()
    rows, half = tokens.shape[1:]
    width = w_query.shape[1]
    ch = width // n_fs
    n_w = 5
    wr = w_query.shape[0]
    lanes = rows // 128
    extra = jnp.pad(extra_decay[0].T.reshape(n_fs, lanes, 128), ((0, 0), (0, 8 - lanes), (0, 0)))
    cw = w_out_pool.shape[1]
    z, e_all, ow = comm(
        functools.partial(project_kernel, n_sp, n_fs, n_tp),
        [((n_fs, rows, n_w * ch), BF), ((n_fs, 8, 128), F32), ((2 * width, cw), BF)],
        [
            pltpu.VMEM((n_fs, wr, n_w * ch), BF), pltpu.VMEM((n_fs, rows, n_tp * half), BF),
            pltpu.VMEM((n_sp * n_fs * wr, n_w * ch), BF), pltpu.VMEM((n_fs, rows, n_w * ch), F32),
            dma(2, 2), dma(n_fs, 2), dma(2), dma(n_fs, 2), dma(n_fs, 2), dma(n_fs - 1), dma(n_sp, n_fs),
            dma(n_sp, n_fs), dma(n_sp, n_fs), dma(n_fs - 1), dma(n_fs),
        ],
        1, "project",
    )(
        tokens[0], w_query, forget_weight, w_input, w_outgate, w_pool, extra, norm_gain[None],
        group_weight, pool_gain[None], recurrent_output_weight, w_out_pool,
    )
    n_half = n_sp // n_tp
    act, sq = comm(
        functools.partial(state_kernel, n_sp, group_weight.shape[1]),
        [((2, n_fs * rows, ch), BF), ((n_fs, 8, 128), F32)],
        [
            pltpu.VMEM((n_fs, rows, ch), F32), pltpu.VMEM((n_fs, rows, ch), F32),
            pltpu.VMEM((n_fs, ch, ch), BF), pltpu.VMEM((n_fs, 8, ch), F32),
            pltpu.VMEM((n_sp - 1, n_fs, ch, ch), BF), pltpu.VMEM((n_sp - 1, n_fs, 8, ch), F32),
            pltpu.VMEM((n_fs, 2**POOL_GROUPS, ch), BF),
            dma(n_sp - 1), dma(n_sp - 1), dma(n_sp - 1), dma(n_sp - 1), dma(), dma(),
        ],
        2, "state",
    )(z, e_all, forget_gap[None], rec_gain[None])
    out_shape = (n_fs, n_tp, rows // n_tp, n_half * cw)
    (final,) = comm(
        functools.partial(mix_kernel, n_sp, n_fs, n_tp),
        [((rows // n_tp, n_tp * n_half * n_fs * cw), BF)],
        [
            pltpu.VMEM(out_shape, BF), pltpu.VMEM((n_tp, n_fs) + act.shape, BF), pltpu.VMEM((n_tp, n_fs) + sq.shape, F32),
            pltpu.VMEM((n_half, n_tp) + ow.shape, BF), pltpu.VMEM((n_sp,) + ow.shape, BF),
            pltpu.VMEM((2, n_tp * width, n_half * cw), BF), pltpu.VMEM(out_shape, BF),
            dma(2, 2), dma(n_fs, 2), dma(2), dma(n_fs, 2), dma(n_fs, 2), dma(n_fs, n_tp), dma(n_tp, n_fs),
            dma(n_sp), dma(n_sp), dma(n_sp), dma(n_sp), dma(n_sp), dma(n_fs, n_tp), dma(n_fs, n_tp),
        ],
        3, "mix",
    )(act, sq, ow)
    return final[None]


def mm(a, b, dims):
    return lax.dot_general(a, b, (dims, ((), ())), preferred_element_type=F32)


NN, NT, TN = ((1,), (0,)), ((1,), (1,)), ((0,), (0,))


def layer_kernel(
    n_sp, n_fs, n_tp, tok, wq, wf, wi, wo, wp, extra, gain, gap, rec_gain, gmap, pgain, wor, wop, final,
    src0, src1, src2, ws0, ws1, ws2, xs, xn, acc0, acc1, acc2, e_src, e_all, local, qd, own_st, own_de,
    t_out, t_in, rim_src, rim, acts, sq_src, sq_all, ow_buf, ow_oth, part,
    x_send, x_recv, xf_send, xd_send, xd_recv, w_send, w_recv, up_send, dn_send, e_send, e_recv,
    t_send, t_recv, g_send, g_recv, a_send, a_recv, af_send, ad_send, ad_recv, q_send, q_recv,
    ou_send, on_send, o_recv, od_send, od_recv, m_send, m_recv,
):
    s, f, t = place()
    rows, half = tok.shape
    cut = rows // 2
    wr, width = wq.shape
    ch = width // n_fs
    cw = wor.shape[1]
    n_half = n_sp // n_tp
    out_rows = rows // n_tp
    lanes = rows // 128
    size = 128
    groups = ((wq, wf, wi), (wp,), (wo,))
    srcs, wss, accs = (src0, src1, src2), (ws0, ws1, ws2), (acc0, acc1, acc2)
    other = (s, f, 1 - t)
    px, py, pd = square(f)
    order = (f, px, py, pd)
    up, down = (s + 1, f, t), (s - 1, f, t)
    has_up, has_down = s < n_sp - 1, s > 0
    sends = []

    def send(c):
        c.start()
        sends.append(c)

    def when(cond, *copies):
        @pl.when(cond)
        def _():
            for c in copies:
                c.start()

    def pack(c):
        for i, w in enumerate(groups[c]):
            for g in range(n_fs):
                srcs[c][g, :, i * ch : (i + 1) * ch] = w[:, g * ch : (g + 1) * ch]

    pack(0)
    e_rows = extra[...].T
    for g in range(n_fs):
        e_src[g] = jnp.broadcast_to(e_rows[g : g + 1, :], e_src.shape[1:])
    greet(
        [(None, other)]
        + [(None, (s, g, u)) for g in order[1:] for u in (t, 1 - t)]
        + [(has_up, up), (has_down, down)]
    )

    def cols(c):
        return pl.ds(pl.multiple_of(c * half, half), half)

    def span(a, b):
        return pl.ds(pl.multiple_of((a * n_fs + b) * wr, wr), wr)

    def slot(c, a, b):
        return wss[c].at[span(a, b), :]

    def to_up(c, src, a, b):
        return rcopy(src, slot(c, a, b), up_send.at[c, a, b], w_recv.at[c, a, b], up)

    def to_down(c, src, a, b):
        return rcopy(src, slot(c, a, b), dn_send.at[c, a, b], w_recv.at[c, a, b], down)

    def both(c, src, a, b):
        when(has_up, to_up(c, src, a, b))
        when(has_down, to_down(c, src, a, b))

    def spread(c):
        for i, g in enumerate(order[1:]):
            send(rcopy(srcs[c].at[g], slot(c, s, f), w_send.at[c, i], w_recv.at[c, s, f], (s, g, t)))

    def from_square(c, g):
        to_up(c, slot(c, s, g), s, g).wait_recv()
        both(c, slot(c, s, g), s, g)

    def relay(c, d, gs):
        for g in gs:
            a, b = s - d, s + d

            @pl.when((a >= 0) & has_up)
            def _():
                to_up(c, slot(c, a, g), a, g).wait_recv()
                to_up(c, slot(c, a, g), a, g).start()

            @pl.when((b < n_sp) & has_down)
            def _():
                to_down(c, slot(c, b, g), b, g).wait_recv()
                to_down(c, slot(c, b, g), b, g).start()

    def arrive(c, d):
        for g in order:
            a, b = s - d, s + d

            @pl.when((a >= 0) & jnp.logical_not(has_up))
            def _():
                to_up(c, slot(c, a, g), a, g).wait_recv()

            @pl.when((b < n_sp) & jnp.logical_not(has_down))
            def _():
                to_down(c, slot(c, b, g), b, g).wait_recv()

    def gemm(c, a, first=False):
        k = pl.ds(pl.multiple_of(a * n_fs * wr, n_fs * wr), n_fs * wr)
        acc, w = accs[c], wss[c]

        def each(i, _):
            out = jnp.dot(xn[i, :, k], w[k, :], preferred_element_type=F32)
            acc[i] = out if first else acc[i] + out
            return 0

        lax.fori_loop(0, n_fs, each, 0)

    def gemm_at(c, d):
        pl.when(s - d >= 0)(lambda: gemm(c, s - d))
        pl.when(s + d < n_sp)(lambda: gemm(c, s + d))

    def x_slot(g, h, c):
        return xs.at[g, h * cut : (h + 1) * cut, cols(c)]

    def landed(g, h):
        here = x_slot(g, h, t)
        rcopy(here, here, xd_send.at[g, h], x_recv.at[g, h], other).wait_recv()
        return here

    def hand_on(g, h, here):
        send(rcopy(here, here, xd_send.at[g, h], xd_recv.at[g, h], other))

    def norm(g):
        for h in range(2):
            here = x_slot(g, h, 1 - t)
            rcopy(here, here, xd_send.at[g, h], xd_recv.at[g, h], other).wait_recv()
        tile = 16

        def each(j, _):
            at = pl.ds(pl.multiple_of(j * tile, tile), tile)
            feats = xs[g, at, :].astype(F32)
            scale = lax.rsqrt(jnp.mean(feats * feats, axis=-1, keepdims=True) + EPS)
            xn[g, at, :] = (feats * scale * gain[...]).astype(BF)
            return 0

        lax.fori_loop(0, rows // tile, each, 0, unroll=2)

    def ow_up(src, a, k):
        return rcopy(src, ow_buf.at[a, k], ou_send.at[a, k], o_recv.at[a, k], up)

    def ow_down(src, a, k):
        return rcopy(src, ow_buf.at[a, k], on_send.at[a, k], o_recv.at[a, k], down)

    def ow_other(a, k):
        return rcopy(ow_buf.at[a, k], ow_oth.at[lax.rem(a, n_half), k], od_send.at[a, k], od_recv.at[lax.rem(a, n_half), k], other)

    def ow_share(a, k):
        when(a // n_half != t, ow_other(a, k))

    def ow_relay(d, k):
        a, b = s - d, s + d

        @pl.when((a >= 0) & has_up)
        def _():
            here = ow_buf.at[a, k]
            ow_up(here, a, k).wait_recv()
            ow_up(here, a, k).start()
            ow_share(a, k)

        @pl.when((b < n_sp) & has_down)
        def _():
            here = ow_buf.at[b, k]
            ow_down(here, b, k).wait_recv()
            ow_down(here, b, k).start()
            ow_share(b, k)

    def ow_take(d, k):
        a, b = s - d, s + d

        @pl.when((a >= 0) & jnp.logical_not(has_up))
        def _():
            ow_up(ow_buf.at[a, k], a, k).wait_recv()
            ow_share(a, k)

        @pl.when((b < n_sp) & jnp.logical_not(has_down))
        def _():
            ow_down(ow_buf.at[b, k], b, k).wait_recv()
            ow_share(b, k)

    both(0, src0.at[f], s, f)
    spread(0)
    for i, (p, hs) in enumerate(((px, (0, 1)), (py, (1, 0)))):
        for h in hs:
            send(rcopy(tok.at[h * cut : (h + 1) * cut, :], x_slot(f, h, t), x_send.at[i, h], x_recv.at[f, h], (s, p, t)))
    for h in range(2):
        send(rcopy(tok.at[h * cut : (h + 1) * cut, :], x_slot(f, h, t), xd_send.at[f, h], xd_recv.at[f, h], other))
    when(has_up, ow_up(wor, s, 0))
    when(has_down, ow_down(wor, s, 0))
    for i, g in enumerate(order[1:]):
        send(rcopy(e_src.at[g], e_all.at[f], e_send.at[i], e_recv.at[f], (s, g, t)))
    pack(1)
    pack(2)
    spread(1)
    spread(2)
    for c in range(3):
        wss[c][span(s, f), :] = srcs[c][f]
    xs[f, :, cols(t)] = tok[...]
    e_all[f] = e_src[f]
    for g in order[1:]:
        from_square(0, g)
    ow_buf[s, 0] = wor[...]
    gd = gmap.shape[1]
    for i in range(width // gd):
        at = slice(i * gd, (i + 1) * gd)
        scaled = (gmap[t * (width // gd) + i].astype(F32) * pgain[:, at]).astype(BF)
        ow_buf[s, 1, at, :] = jnp.dot(scaled, wop[at, :], preferred_element_type=F32).astype(BF)
    norm(f)
    relay(0, 1, order[:2])
    for i, (g, h, onto) in enumerate(((px, 0, py), (py, 1, px))):
        here = landed(g, h)
        send(rcopy(here, here, xf_send.at[i], x_recv.at[g, h], (s, onto, t)))
        hand_on(g, h, here)
    relay(0, 1, order[2:])
    for g, h in ((px, 1), (py, 0)):
        hand_on(g, h, landed(g, h))
    for d in range(2, n_sp - 1):
        relay(0, d, order[:2])
    norm(px)
    norm(py)
    for d in range(2, n_sp - 1):
        relay(0, d, order[2:])
    both(1, src1.at[f], s, f)
    for g in order[1:]:
        from_square(1, g)
    for h in range(2):
        hand_on(pd, h, landed(pd, h))
    norm(pd)

    for d in range(1, n_sp - 1):
        arrive(0, d)
    gemm(0, s, True)
    for d in range(1, n_sp - 1):
        gemm_at(0, d)
    relay(1, 1, order)
    arrive(0, n_sp - 1)
    gemm_at(0, n_sp - 1)
    for g in order[1:]:
        rcopy(e_src.at[f], e_all.at[g], e_send.at[0], e_recv.at[g], other).wait_recv()

    mine = pl.ds(pl.multiple_of(f * ch, ch), ch)
    gap_f = gap[:, mine]
    gain_f = rec_gain[:, mine]
    at = lax.broadcasted_iota(jnp.int32, (size, size), 0)
    causal = at >= lax.broadcasted_iota(jnp.int32, (size, size), 1)
    lower = jnp.where(causal, 1.0, 0.0).astype(BF)
    lower = jnp.concatenate([lower, lower], axis=1)

    def scan(g):
        state = None
        so_far = jnp.zeros((1, ch), F32)
        e_cols = e_all[g].T
        for n in range(rows // size):
            here = slice(n * size, (n + 1) * size)
            v = acc0[g, here, 2 * ch : 3 * ch].astype(BF)
            q = jax.nn.silu(acc0[g, here, 0:ch].astype(BF).astype(F32))
            k = gap_f * jax.nn.sigmoid(-acc0[g, here, ch : 2 * ch].astype(BF).astype(F32))
            logs = jnp.log1p(-k) + e_cols[here, 0:1]
            high = logs.astype(BF)
            low = (logs - high.astype(F32)).astype(BF)
            within = mm(lower, jnp.concatenate([high, low], axis=0), NN)
            mid = within[size // 2 - 1 : size // 2]
            end = within[size - 1 :]
            q = q * jnp.exp(within - mid)
            k = (k * jnp.exp(mid - within)).astype(BF)
            q_up = q.astype(BF)
            scores = jnp.where(causal, mm(q_up, k, NT), 0.0).astype(BF)
            out = mm(scores, v, NN)
            if n:
                out = out + mm(q_up, (state * jnp.exp(mid)).astype(BF), NT)
            local[g, here, :] = out
            qd[g, here, :] = (q * jnp.exp(mid + so_far)).astype(BF)
            fresh = mm(v, k, TN) * jnp.exp(end - mid)
            state = state * jnp.exp(end) + fresh if n else fresh
            so_far = so_far + end
        own_st[g] = state
        own_de[g] = jnp.broadcast_to(jnp.exp(so_far), own_de.shape[1:])

    scan(0)
    scan(1)
    for d in range(2, n_sp - 1):
        relay(1, d, order)
    both(2, src2.at[f], s, f)
    for g in order[1:]:
        from_square(2, g)
    scan(2)
    scan(3)

    def carry(g):
        return rcopy(t_out.at[g], t_in.at[g], t_send.at[g], t_recv.at[g], up)

    @pl.when(jnp.logical_not(has_down))
    def _():
        t_in[...] = jnp.zeros(t_in.shape, BF)
        rim[...] = jnp.zeros(rim.shape, BF)
        t_out[...] = own_st[...].astype(BF)
        for g in range(n_fs):
            carry(g).start()

    for d in range(1, n_sp - 1):
        relay(2, d, order)

    def project(c):
        gemm(c, s, True)
        for d in range(1, n_sp - 1):
            arrive(c, d)
            gemm_at(c, d)
        arrive(c, n_sp - 1)
        gemm_at(c, n_sp - 1)

    project(1)
    reach = rim.shape[1]
    rim_src[...] = acc1[:, rows - reach :, :].astype(BF)
    edge = rcopy(rim_src, rim, g_send, g_recv, up)
    when(has_up, edge)

    @pl.when(has_down & has_up)
    def _():
        for g in range(n_fs):
            carry(g).wait_recv()
            t_out[g] = (own_st[g] + t_in[g].astype(F32) * own_de[g, 0:1, :]).astype(BF)
            carry(g).start()

    when(has_up, ow_up(ow_buf.at[s, 1], s, 1))
    when(has_down, ow_down(ow_buf.at[s, 1], s, 1))
    for k in range(2):
        ow_share(s, k)
    ow_relay(1, 0)
    pl.when(has_down)(edge.wait_recv)

    group = (t * n_fs * ch + f * ch) // gd
    spot = s * rows + lax.broadcasted_iota(jnp.int32, (rows, ch), 0)
    window = 2
    for level in range(1, POOL_GROUPS):
        window = jnp.where(group == level, 2 ** (level + 1), window)
    share = 1.0 / jnp.minimum(spot + 1, window).astype(F32)

    def pool(g):
        zp = acc1[g].astype(BF).astype(F32)
        running = jnp.concatenate([rim[g].astype(F32), zp], axis=0)
        total = None
        for level in range(POOL_GROUPS):
            stride = 2**level
            running = running[stride:] + running[:-stride]
            now = running[running.shape[0] - rows :]
            total = now if level == 0 else jnp.where(group == level, now, total)
        acts[1, t, f, g * rows : (g + 1) * rows, :] = (total * share - zp).astype(BF)

    part_rows = n_fs * rows // 2

    def a_slot(k, u, g, h):
        return acts.at[k, u, g, h * part_rows : (h + 1) * part_rows, :]

    def publish(k, h):
        here = a_slot(k, t, f, h)
        for i, p in enumerate((px, py)):
            send(rcopy(here, here, a_send.at[k, i, h], a_recv.at[k, f, h], (s, p, t)))
        send(rcopy(here, here, ad_send.at[k, f, h], ad_recv.at[k, f, h], other))

    def a_landed(k, g, h):
        here = a_slot(k, t, g, h)
        rcopy(here, here, ad_send.at[k, g, h], a_recv.at[k, g, h], other).wait_recv()
        return here

    def a_hand_on(k, g, h, here):
        send(rcopy(here, here, ad_send.at[k, g, h], ad_recv.at[k, g, h], other))

    def a_forward(k):
        for i, (g, h, onto) in enumerate(((px, 0, py), (py, 1, px))):
            here = a_landed(k, g, h)
            send(rcopy(here, here, af_send.at[k, i], a_recv.at[k, g, h], (s, onto, t)))
            a_hand_on(k, g, h, here)

    def a_rest(k):
        for g, h in ((px, 1), (py, 0), (pd, 0), (pd, 1)):
            a_hand_on(k, g, h, a_landed(k, g, h))

    def a_other(k):
        for g in order:
            for h in range(2):
                here = a_slot(k, 1 - t, g, h)
                rcopy(here, here, ad_send.at[k, g, h], ad_recv.at[k, g, h], other).wait_recv()

    for h in range(2):
        for g in range(h * n_fs // 2, (h + 1) * n_fs // 2):
            pool(g)
        publish(1, h)
    ow_relay(1, 1)
    for d in range(2, n_sp - 1):
        ow_relay(d, 0)
    gemm(2, s, True)
    for d in range(1, n_sp - 1):
        arrive(2, d)
        gemm_at(2, d)
    a_forward(1)
    arrive(2, n_sp - 1)
    gemm_at(2, n_sp - 1)

    @pl.when(has_down & jnp.logical_not(has_up))
    def _():
        for g in range(n_fs):
            carry(g).wait_recv()

    ones = jnp.ones((8, ch), BF)

    def finish(g):
        rec = local[g] + mm(qd[g], t_in[g], NT)
        sums = mm(ones, (rec * rec).astype(BF), NT)
        for i in range(lanes):
            sq_src[g * lanes + i : g * lanes + i + 1, :] = sums[0:1, i * 128 : (i + 1) * 128]
        gate = jax.nn.silu(acc2[g].astype(BF).astype(F32))
        acts[0, t, f, g * rows : (g + 1) * rows, :] = (rec * gain_f * gate).astype(BF)

    for h in range(2):
        for g in range(h * n_fs // 2, (h + 1) * n_fs // 2):
            finish(g)
        publish(0, h)
    for i, g in enumerate(order[1:]):
        for u in range(n_tp):
            send(rcopy(sq_src, sq_all.at[t, f], q_send.at[i, u], q_recv.at[t, f], (s, g, u)))
    send(rcopy(sq_src, sq_all.at[t, f], q_send.at[n_fs - 1, 0], q_recv.at[t, f], other))
    sq_all[t, f] = sq_src[...]
    for d in range(2, n_sp - 1):
        ow_relay(d, 1)
    a_rest(1)
    for k in range(2):
        ow_take(1, k)
    a_forward(0)
    for d in range(2, n_sp - 1):
        for k in range(2):
            ow_take(d, k)
    a_rest(0)
    a_other(1)
    a_other(0)
    for g in order[1:]:
        for u in range(n_tp):
            here = sq_all.at[u, g]
            rcopy(here, here, q_send.at[0, 0], q_recv.at[u, g], other).wait_recv()
    here = sq_all.at[1 - t, f]
    rcopy(here, here, q_send.at[0, 0], q_recv.at[1 - t, f], other).wait_recv()
    sums = sum(sq_all[u, i] for u in range(n_tp) for i in range(n_fs))
    scale = lax.rsqrt(sums / (n_tp * width) + EPS).T
    scales = [
        jnp.concatenate([scale[:, g * lanes + i : g * lanes + i + 1] for i in range(lanes)], axis=0) for g in range(n_fs)
    ]
    late = s - t * n_half >= n_half - 1

    def spot_of(a, g):
        return pl.ds(pl.multiple_of((a * n_fs + g) * cw, cw), cw)

    def piece(i, g, u):
        return rcopy(
            part.at[i, g, u], final.at[:, spot_of(t * n_half + i, f)], m_send.at[i, g, u], m_recv.at[i, f, t], (s, g, u)
        )

    for j in range(n_half):
        i = jnp.where(late, n_half - 1 - j, j)
        a = t * n_half + i
        if j == n_half - 1:
            for k in range(2):
                ow_take(n_sp - 1, k)
        for k in range(2):
            rcopy(ow_buf.at[a, k], ow_oth.at[i, k], od_send.at[a, k], od_recv.at[i, k], other).wait_recv()
        for g in range(n_fs):
            here = pl.ds(g * rows, rows)
            made = []
            for k in range(2):
                total = None
                for u, w in ((t, ow_buf.at[a, k]), (1 - t, ow_oth.at[i, k])):
                    left = jnp.concatenate([acts[k, u, b, here, :] for b in range(n_fs)], axis=1)
                    now = jnp.dot(left, w[...], preferred_element_type=F32)
                    total = now if total is None else total + now
                made.append(total)
            mixed = (made[0] * scales[g] + made[1]).astype(BF)
            for u in range(n_tp):
                part[i, g, u] = mixed[u * out_rows : (u + 1) * out_rows]
                when((g != f) | (u != t), piece(i, g, u))
        final[:, spot_of(a, f)] = part[i, f, t]

    for i in range(n_half):
        for g in range(n_fs):
            for u in range(n_tp):
                @pl.when((g != f) | (u != t))
                def _():
                    here = final.at[:, spot_of(u * n_half + i, g)]
                    rcopy(here, here, m_send.at[i, g, u], m_recv.at[i, g, u], other).wait_recv()
                    piece(i, g, u).wait_send()
    for c in sends:
        c.wait_send()
    for c in range(3):
        for d in range(n_sp):
            for g in order:
                a, b = s - d, s + d

                @pl.when((a >= 0) & has_up)
                def _():
                    to_up(c, slot(c, a, g), a, g).wait_send()

                @pl.when((b < n_sp) & has_down)
                def _():
                    to_down(c, slot(c, b, g), b, g).wait_send()
    for d in range(n_sp):
        for k in range(2):
            a, b = s - d, s + d

            @pl.when((a >= 0) & has_up)
            def _():
                ow_up(ow_buf.at[a, k], a, k).wait_send()

            @pl.when((b < n_sp) & has_down)
            def _():
                ow_down(ow_buf.at[b, k], b, k).wait_send()
    for i in range(n_half):
        for k in range(2):
            ow_other((1 - t) * n_half + i, k).wait_send()

    @pl.when(has_up)
    def _():
        edge.wait_send()
        for g in range(n_fs):
            carry(g).wait_send()


def fused(
    n_sp, n_fs, n_tp, tokens, norm_gain, w_query, forget_weight, w_input, w_outgate, w_pool, forget_gap,
    extra_decay, rec_gain, group_weight, pool_gain, recurrent_output_weight, w_out_pool,
):
    rows, half = tokens.shape[1:]
    wr, width = w_query.shape
    ch = width // n_fs
    cw = w_out_pool.shape[1]
    n_half = n_sp // n_tp
    feats = n_sp * n_fs * wr
    lanes = rows // 128

    def buf(kind, *shape):
        return pltpu.VMEM(shape, kind)

    (final,) = comm(
        functools.partial(layer_kernel, n_sp, n_fs, n_tp),
        [((rows // n_tp, n_sp * n_fs * cw), BF)],
        [
            buf(BF, n_fs, wr, 3 * ch), buf(BF, n_fs, wr, ch), buf(BF, n_fs, wr, ch),
            buf(BF, feats, 3 * ch), buf(BF, feats, ch), buf(BF, feats, ch),
            buf(BF, n_fs, rows, n_tp * half), buf(BF, n_fs, rows, n_tp * half),
            buf(F32, n_fs, rows, 3 * ch), buf(F32, n_fs, rows, ch), buf(F32, n_fs, rows, ch),
            buf(F32, n_fs, 8, rows), buf(F32, n_fs, 8, rows),
            buf(F32, n_fs, rows, ch), buf(BF, n_fs, rows, ch),
            buf(F32, n_fs, ch, ch), buf(F32, n_fs, 8, ch),
            buf(BF, n_fs, ch, ch), buf(BF, n_fs, ch, ch),
            buf(BF, n_fs, 2**POOL_GROUPS, ch), buf(BF, n_fs, 2**POOL_GROUPS, ch),
            buf(BF, 2, n_tp, n_fs, n_fs * rows, ch),
            buf(F32, n_fs * lanes, 128), buf(F32, n_tp, n_fs, n_fs * lanes, 128),
            buf(BF, n_sp, 2, width, cw), buf(BF, n_half, 2, width, cw),
            buf(BF, n_half, n_fs, n_tp, rows // n_tp, cw),
            dma(2, 2), dma(n_fs, 2), dma(2), dma(n_fs, 2), dma(n_fs, 2),
            dma(3, n_fs - 1), dma(3, n_sp, n_fs), dma(3, n_sp, n_fs), dma(3, n_sp, n_fs), dma(n_fs - 1), dma(n_fs),
            dma(n_fs), dma(n_fs), dma(), dma(),
            dma(2, 2, 2), dma(2, n_fs, 2), dma(2, 2), dma(2, n_fs, 2), dma(2, n_fs, 2), dma(n_fs, n_tp), dma(n_tp, n_fs),
            dma(n_sp, 2), dma(n_sp, 2), dma(n_sp, 2), dma(n_sp, 2), dma(n_half, 2), dma(n_half, n_fs, n_tp), dma(n_half, n_fs, n_tp),
        ],
        1, "layer",
    )(
        tokens[0], w_query, forget_weight, w_input, w_outgate, w_pool, extra_decay[0], norm_gain[None],
        forget_gap[None], rec_gain[None], group_weight, pool_gain[None], recurrent_output_weight, w_out_pool,
    )
    return final[None]


def run(n_sp, n_fs, n_tp, *args):
    wr, width = args[2].shape
    whole = n_fs * wr % 128 == 0 and args[-1].shape[1] % 128 == 0 and args[0].shape[1] % 256 == 0
    return (fused if whole and width == n_fs * HEAD_DIM else body)(n_sp, n_fs, n_tp, *args)


def solution(mesh):
    sizes = dict(mesh.shape)
    weight = P(("sp", "fs"), "tp")
    placed = (
        P("fs", "sp", "tp"), P(), weight, weight, weight, weight, weight, P("tp"),
        P("fs", "sp", "tp"), P("tp"), P(), P("tp"), P("tp", ("sp", "fs")), P("tp", ("sp", "fs")),
    )
    return jax.shard_map(
        functools.partial(run, sizes["sp"], sizes["fs"], sizes["tp"]),
        mesh=mesh, in_specs=placed, out_specs=P("fs", ("sp", "tp"), None), check_vma=False,
    )
```

```python
import functools
import jax
import jax.numpy as jnp
from jax import lax
from jax.experimental import pallas as pl
from jax.experimental.pallas import tpu as pltpu
from jax.sharding import PartitionSpec as P

HEAD_DIM = 128
POOL_GROUPS = 4
BLOCK = 64
EPS = 1e-06
HIGH = lax.Precision.HIGHEST
MESH = pl.DeviceIdType.MESH
BF = jnp.bfloat16
F32 = jnp.float32


def place():
    return lax.axis_index("sp"), lax.axis_index("fs"), lax.axis_index("tp")


def rcopy(src, dst, ssem, rsem, dev):
    return pltpu.make_async_remote_copy(
        src_ref=src, dst_ref=dst, send_sem=ssem, recv_sem=rsem, device_id=dev, device_id_type=MESH
    )


def greet(devs):
    barrier = pltpu.get_barrier_semaphore()
    for cond, dev in devs:
        def tell(dev=dev):
            pl.semaphore_signal(barrier, inc=1, device_id=dev, device_id_type=MESH)
        if cond is None:
            tell()
        else:
            pl.when(cond)(tell)
    pl.semaphore_wait(barrier, sum(1 if cond is None else jnp.where(cond, 1, 0) for cond, _ in devs))


def square(f):
    near = f + 1 - 2 * lax.rem(f, 2)
    return near, lax.rem(f + 2, 4), lax.rem(near + 2, 4)


def project_kernel(
    n_sp, n_fs, n_tp, tok, wq, wf, wi, wo, wp, extra, gain, gmap, pgain, wor, wop, z_ref, e_ref, ow_ref,
    wsrc, xs, ws, acc, x_send, x_recv, f_send, d_send, d_recv, w_send, w_recv, zr_send, zl_send, e_send, e_recv,
):
    s, f, t = place()
    rows, half = tok.shape
    part = rows // 2
    mats = (wq, wf, wi, wo, wp)
    wr, width = wq.shape
    ch = width // n_fs
    for i, w in enumerate(mats):
        for g in range(n_fs):
            wsrc[g, :, i * ch : (i + 1) * ch] = w[:, g * ch : (g + 1) * ch]
    other = (s, f, 1 - t)
    px, py, pd = square(f)
    order = (f, px, py, pd)
    up, down = (s + 1, f, t), (s - 1, f, t)
    has_up, has_down = s < n_sp - 1, s > 0
    greet([(None, other)] + [(None, (s, g, t)) for g in order[1:]] + [(has_up, up), (has_down, down)])

    def cols(c):
        return pl.ds(pl.multiple_of(c * half, half), half)

    def span(a, b):
        return pl.ds(pl.multiple_of((a * n_fs + b) * wr, wr), wr)

    def slot(a, b):
        return ws.at[span(a, b), :]

    def to_up(src, a, b):
        return rcopy(src, slot(a, b), zr_send.at[a, b], w_recv.at[a, b], up)

    def to_down(src, a, b):
        return rcopy(src, slot(a, b), zl_send.at[a, b], w_recv.at[a, b], down)

    sends = []

    def send(c):
        c.start()
        sends.append(c)

    def x_slot(g, h, c):
        return xs.at[g, h * part : (h + 1) * part, cols(c)]

    own = wsrc.at[f]
    pl.when(has_up)(lambda: to_up(own, s, f).start())
    pl.when(has_down)(lambda: to_down(own, s, f).start())
    for i, g in enumerate((pd, px, py)):
        send(rcopy(wsrc.at[g], slot(s, f), w_send.at[i], w_recv.at[s, f], (s, g, t)))
    for i, (p, hs) in enumerate(((px, (0, 1)), (py, (1, 0)))):
        for h in hs:
            send(rcopy(tok.at[h * part : (h + 1) * part, :], x_slot(f, h, t), x_send.at[i, h], x_recv.at[f, h], (s, p, t)))
    for h in range(2):
        send(rcopy(tok.at[h * part : (h + 1) * part, :], x_slot(f, h, t), d_send.at[f, h], d_recv.at[f, h], other))
    for i, g in enumerate(order[1:]):
        send(rcopy(extra.at[g], e_ref.at[f], e_send.at[i], e_recv.at[f], (s, g, t)))
    ws[span(s, f), :] = wsrc[f]
    xs[f, :, cols(t)] = tok[...]
    e_ref[f] = extra[f]
    ow_ref[0:width, :] = wor[...]
    gd = gmap.shape[1]
    for i in range(width // gd):
        at = slice(i * gd, (i + 1) * gd)
        scaled = (gmap[t * (width // gd) + i].astype(F32) * pgain[:, at]).astype(BF)
        folded = jnp.dot(scaled, wop[at, :], preferred_element_type=F32)
        ow_ref[width + i * gd : width + (i + 1) * gd, :] = folded.astype(BF)

    for g in order[1:]:
        to_up(slot(s, g), s, g).wait_recv()
        pl.when(has_up)(lambda: to_up(slot(s, g), s, g).start())
        pl.when(has_down)(lambda: to_down(slot(s, g), s, g).start())

    def landed(g, h):
        here = x_slot(g, h, t)
        rcopy(here, here, d_send.at[g, h], x_recv.at[g, h], other).wait_recv()
        return here

    def hand_on(g, h, here):
        send(rcopy(here, here, d_send.at[g, h], d_recv.at[g, h], other))

    for i, (g, h, onto) in enumerate(((px, 0, py), (py, 1, px))):
        here = landed(g, h)
        send(rcopy(here, here, f_send.at[i], x_recv.at[g, h], (s, onto, t)))
        hand_on(g, h, here)

    def relay(d):
        for g in order:
            a = s - d

            @pl.when(a >= 0)
            def _():
                to_up(slot(a, g), a, g).wait_recv()
                pl.when(has_up)(lambda: to_up(slot(a, g), a, g).start())
            b = s + d

            @pl.when(b < n_sp)
            def _():
                to_down(slot(b, g), b, g).wait_recv()
                pl.when(has_down)(lambda: to_down(slot(b, g), b, g).start())

    def add(a):
        k = pl.ds(pl.multiple_of(a * n_fs * wr, n_fs * wr), n_fs * wr)

        def each(i, _):
            acc[i] += jnp.dot(xs[i, :, k], ws[k, :], preferred_element_type=F32)
            return 0

        lax.fori_loop(0, n_fs, each, 0)

    def multiply(d):
        pl.when(s - d >= 0)(lambda: add(s - d))
        pl.when(s + d < n_sp)(lambda: add(s + d))

    relay(1)
    for g, h in ((px, 1), (py, 0), (pd, 0), (pd, 1)):
        hand_on(g, h, landed(g, h))
    for d in range(2, n_sp - 1):
        relay(d)
    for g in order:
        for h in range(2):
            here = x_slot(g, h, 1 - t)
            rcopy(here, here, d_send.at[g, h], d_recv.at[g, h], other).wait_recv()
    for g in order[1:]:
        rcopy(extra.at[f], e_ref.at[g], e_send.at[0], e_recv.at[g], other).wait_recv()
    for c in sends:
        c.wait_send()

    def norm(j, _):
        tile = 16
        per = rows // tile
        at = (j // per, pl.ds(pl.multiple_of(lax.rem(j, per) * tile, tile), tile))
        feats = xs[at[0], at[1], :].astype(F32)
        scale = lax.rsqrt(jnp.mean(feats * feats, axis=-1, keepdims=True) + EPS)
        xs[at[0], at[1], :] = (feats * scale * gain[...]).astype(BF)
        return 0

    lax.fori_loop(0, n_fs * rows // 16, norm, 0, unroll=2)

    if n_fs * wr % 128 == 0:
        own_k = pl.ds(pl.multiple_of(s * n_fs * wr, n_fs * wr), n_fs * wr)

        def begin(i, _):
            acc[i] = jnp.dot(xs[i, :, own_k], ws[own_k, :], preferred_element_type=F32)
            return 0

        lax.fori_loop(0, n_fs, begin, 0)
        for d in range(1, n_sp - 1):
            multiply(d)
        relay(n_sp - 1)
        multiply(n_sp - 1)

        def finish(i, _):
            z_ref[i] = acc[i].astype(BF)
            return 0
    else:
        relay(n_sp - 1)

        def finish(i, _):
            z_ref[i] = jnp.dot(xs[i], ws[...], preferred_element_type=F32).astype(BF)
            return 0

    lax.fori_loop(0, n_fs, finish, 0)

    for d in range(n_sp):
        for g in order:
            a = s - d

            @pl.when((a >= 0) & has_up)
            def _():
                to_up(slot(a, g), a, g).wait_send()
            b = s + d

            @pl.when((b < n_sp) & has_down)
            def _():
                to_down(slot(b, g), b, g).wait_send()


def dot(a, b, dims):
    return lax.dot_general(a, b, (dims, ((), ())), precision=HIGH, preferred_element_type=F32)


def state_kernel(
    n_sp, group_dim, z, e_all, gap, rec_gain, act, sq_out,
    local, qd, own_st, own_de, st_in, de_in, rim, s_send, s_recv, c_send, c_recv, g_send, g_recv,
):
    s, f, t = place()
    n_fs, rows, _ = z.shape
    ch = HEAD_DIM
    reach = rim.shape[1]
    devs = []
    for d in range(1, n_sp):
        devs.append((s + d < n_sp, (s + d, f, t)))
        devs.append((s - d >= 0, (s - d, f, t)))
    greet(devs)
    edge = rcopy(z.at[:, rows - reach :, 4 * ch :], rim, g_send, g_recv, (s + 1, f, t))
    pl.when(s < n_sp - 1)(edge.start)
    mine = pl.ds(pl.multiple_of(f * ch, ch), ch)
    gap_f = gap[:, mine]
    gain_f = rec_gain[:, mine]
    at = lax.broadcasted_iota(jnp.int32, (BLOCK, BLOCK), 0)
    causal = at >= lax.broadcasted_iota(jnp.int32, (BLOCK, BLOCK), 1)
    lower = causal.astype(F32)

    def one(g, _):
        state = jnp.zeros((ch, ch), F32)
        so_far = jnp.zeros((1, ch), F32)
        e_cols = e_all[g].T
        for n in range(rows // BLOCK):
            here = slice(n * BLOCK, (n + 1) * BLOCK)
            q, fo, v = (z[g, here, i * ch : (i + 1) * ch].astype(F32) for i in range(3))
            q = jax.nn.silu(q)
            k = gap_f * jax.nn.sigmoid(-fo)
            lo = n * BLOCK % 128
            lane = n * BLOCK // 128
            logs = jnp.log1p(-k) + e_cols[lo : lo + BLOCK, lane : lane + 1]
            within = dot(lower, logs, ((1,), (0,)))
            end = within[BLOCK - 1 :]
            q_up = q * jnp.exp(within)
            scores = jnp.where(causal, dot(q_up, k * jnp.exp(-within), ((1,), (1,))), 0.0)
            out = dot(scores, v, ((1,), (0,)))
            if n:
                out = out + dot(q_up, state, ((1,), (1,)))
            local[g, here, :] = out
            qd[g, here, :] = q_up * jnp.exp(so_far)
            state = state * jnp.exp(end) + dot(v.T, k * jnp.exp(end - within), ((1,), (0,)))
            so_far = so_far + end
        own_st[g] = state.astype(BF)
        own_de[g] = jnp.broadcast_to(jnp.exp(so_far), (8, ch))
        return 0

    lax.fori_loop(0, n_fs, one, 0)

    def pair(d):
        dev = (s + d, f, t)
        return (
            rcopy(own_st, st_in.at[d - 1], s_send.at[d - 1], s_recv.at[d - 1], dev),
            rcopy(own_de, de_in.at[d - 1], c_send.at[d - 1], c_recv.at[d - 1], dev),
        )

    for d in range(1, n_sp):
        @pl.when(s + d < n_sp)
        def _():
            for c in pair(d):
                c.start()

        @pl.when(s - d < 0)
        def _():
            st_in[d - 1] = jnp.zeros(st_in.shape[1:], st_in.dtype)
            de_in[d - 1] = jnp.ones(de_in.shape[1:], de_in.dtype)
    pl.when(s == 0)(lambda: rim.__setitem__(Ellipsis, jnp.zeros(rim.shape, rim.dtype)))
    pl.when(s > 0)(edge.wait_recv)
    group = (t * n_fs * ch + f * ch) // group_dim
    spot = s * rows + lax.broadcasted_iota(jnp.int32, (rows, ch), 0)
    window = 2
    for level in range(1, POOL_GROUPS):
        window = jnp.where(group == level, 2 ** (level + 1), window)
    counts = jnp.minimum(spot + 1, window).astype(F32)
    for g in range(n_fs):
        zp = z[g, :, 4 * ch :].astype(F32)
        running = jnp.concatenate([rim[g].astype(F32), zp], axis=0)
        total = None
        for level in range(POOL_GROUPS):
            stride = 2**level
            running = running[stride:] + running[:-stride]
            now = running[running.shape[0] - rows :]
            total = now if level == 0 else jnp.where(group == level, now, total)
        act[1, g * rows : (g + 1) * rows, :] = (total / counts - zp).astype(BF)
    for d in range(1, n_sp):
        @pl.when(s - d >= 0)
        def _():
            for c in pair(d):
                c.wait_recv()

    ones = jnp.ones((8, ch), F32)

    def finish(g, _):
        total = jnp.zeros((ch, ch), F32)
        for d in range(n_sp - 2, -1, -1):
            total = de_in[d, g, 0:1, :] * total + st_in[d, g].astype(F32)
        rec = local[g] + dot(qd[g], total, ((1,), (1,)))
        sums = dot(ones, rec * rec, ((1,), (1,)))
        for i in range(rows // 128):
            sq_out[g, i : i + 1, :] = sums[0:1, i * 128 : (i + 1) * 128]
        gate = jax.nn.silu(z[g, :, 3 * ch : 4 * ch].astype(F32))
        act[0, pl.ds(pl.multiple_of(g * rows, rows), rows), :] = (rec * gain_f * gate).astype(BF)
        return 0

    sq_out[...] = jnp.zeros(sq_out.shape, F32)
    lax.fori_loop(0, n_fs, finish, 0)
    for d in range(1, n_sp):
        @pl.when(s + d < n_sp)
        def _():
            for c in pair(d):
                c.wait_send()
    pl.when(s < n_sp - 1)(edge.wait_send)


def mix_kernel(
    n_sp, n_fs, n_tp, act, sq, ow, final,
    out, acts, sq_all, ow_all, relay_buf, wbuf, part,
    a_send, a_recv, f_send, d_send, d_recv, q_send, q_recv,
    up_send, down_send, o_recv, od_send, od_recv, m_send, m_recv,
):
    s, f, t = place()
    n_half = n_sp // n_tp
    rows = act.shape[1] // n_fs
    half = rows // n_tp
    width, cw = ow.shape[0] // 2, ow.shape[1]
    other = (s, f, 1 - t)
    px, py, pd = square(f)
    up, down = (s + 1, f, t), (s - 1, f, t)
    has_up, has_down = s < n_sp - 1, s > 0
    greet(
        [(None, other)]
        + [(None, (s, g, u)) for g in (px, py, pd) for u in (t, 1 - t)]
        + [(has_up, up), (has_down, down)]
    )

    def to_up(src, a):
        return rcopy(src, relay_buf.at[a], up_send.at[a], o_recv.at[a], up)

    def to_down(src, a):
        return rcopy(src, relay_buf.at[a], down_send.at[a], o_recv.at[a], down)

    def to_other(src, a):
        return rcopy(src, ow_all.at[lax.rem(a, n_half), t], od_send.at[a], od_recv.at[a], other)

    def keep(src, a):
        mine = a // n_half == t

        @pl.when(mine)
        def _():
            ow_all[lax.rem(a, n_half), t] = src[...]

        pl.when(jnp.logical_not(mine))(lambda: to_other(src, a).start())

    sends = []

    def send(c):
        c.start()
        sends.append(c)

    for i, (p, order) in enumerate(((px, (0, 1)), (py, (1, 0)))):
        for h in order:
            send(rcopy(act.at[h], acts.at[t, f, h], a_send.at[i, h], a_recv.at[f, h], (s, p, t)))
    pl.when(has_up)(lambda: to_up(ow, s).start())
    pl.when(has_down)(lambda: to_down(ow, s).start())
    for h in range(2):
        send(rcopy(act.at[h], acts.at[t, f, h], d_send.at[f, h], d_recv.at[f, h], other))
    for i, g in enumerate((px, py, pd)):
        for u in range(n_tp):
            send(rcopy(sq, sq_all.at[t, f], q_send.at[i, u], q_recv.at[t, f], (s, g, u)))
    send(rcopy(sq, sq_all.at[t, f], q_send.at[n_fs - 1, 0], q_recv.at[t, f], other))
    acts[t, f] = act[...]
    sq_all[t, f] = sq[...]
    keep(ow, s)

    def landed(g, h):
        here = acts.at[t, g, h]
        rcopy(here, here, d_send.at[g, h], a_recv.at[g, h], other).wait_recv()
        return here

    def hand_on(g, h, here):
        send(rcopy(here, here, d_send.at[g, h], d_recv.at[g, h], other))

    for i, (g, h, onto) in enumerate(((px, 0, py), (py, 1, px))):
        here = landed(g, h)
        send(rcopy(here, here, f_send.at[i], a_recv.at[g, h], (s, onto, t)))
        hand_on(g, h, here)

    def step(d):
        a = s - d

        @pl.when(a >= 0)
        def _():
            to_up(relay_buf.at[a], a).wait_recv()
            pl.when(has_up)(lambda: to_up(relay_buf.at[a], a).start())
            keep(relay_buf.at[a], a)
        b = s + d

        @pl.when(b < n_sp)
        def _():
            to_down(relay_buf.at[b], b).wait_recv()
            pl.when(has_down)(lambda: to_down(relay_buf.at[b], b).start())
            keep(relay_buf.at[b], b)

    for d in range(1, n_sp):
        step(d)
    for g, h in ((px, 1), (py, 0), (pd, 0), (pd, 1)):
        hand_on(g, h, landed(g, h))
    for i in range(n_half):
        a = t * n_half + i
        here = ow_all.at[i, 1 - t]
        rcopy(here, here, od_send.at[a], od_recv.at[a], other).wait_recv()
    for i in range(n_half):
        for u in range(n_tp):
            for k in range(2):
                wbuf[k, u * width : (u + 1) * width, i * cw : (i + 1) * cw] = ow_all[i, u, k * width : (k + 1) * width, :]
    for g in (px, py, pd):
        for u in range(n_tp):
            here = sq_all.at[u, g]
            rcopy(here, here, q_send.at[0, 0], q_recv.at[u, g], other).wait_recv()
    here = sq_all.at[1 - t, f]
    rcopy(here, here, q_send.at[0, 0], q_recv.at[1 - t, f], other).wait_recv()
    for g in (f, px, py, pd):
        for h in range(2):
            here = acts.at[1 - t, g, h]
            rcopy(here, here, d_send.at[g, h], d_recv.at[g, h], other).wait_recv()

    def piece(g, u):
        return rcopy(part.at[g, u], out.at[f, t], m_send.at[g, u], m_recv.at[f, t], (s, g, u))

    def spread(g):
        for u in range(n_tp):
            c = piece(g, u)
            c.start()
            sends.append(c)

    last = None
    for g in (pd, f, px, py):
        here = pl.ds(pl.multiple_of(g * rows, rows), rows)
        sums = sum(sq_all[u, i, g] for u in range(n_tp) for i in range(n_fs))
        scale = lax.rsqrt(sums / (n_tp * width) + EPS).T
        scale = jnp.concatenate([scale[:, i : i + 1] for i in range(rows // 128)], axis=0)
        left = [
            jnp.concatenate([acts[u, i, h, here, :] for u in range(n_tp) for i in range(n_fs)], axis=1)
            for h in range(2)
        ]
        mixed = (
            jnp.dot(left[0], wbuf[0], preferred_element_type=F32) * scale
            + jnp.dot(left[1], wbuf[1], preferred_element_type=F32)
        ).astype(BF)
        for u in range(n_tp):
            part[g, u] = mixed[u * half : (u + 1) * half]
        if last is not None and last is not f:
            spread(last)
        if last is f:
            c = piece(f, 1 - t)
            c.start()
            sends.append(c)
        last = g
    out[f, t] = part[f, t]
    for i in range(n_half):
        to_other(ow, (1 - t) * n_half + i).wait_send()
    for d in range(n_sp):
        a, b = s - d, s + d

        @pl.when((a >= 0) & has_up)
        def _():
            to_up(ow, a).wait_send()

        @pl.when((b < n_sp) & has_down)
        def _():
            to_down(ow, b).wait_send()
    spread(last)
    for c in sends:
        c.wait_send()
    for g in (px, py, pd):
        for u in range(n_tp):
            here = out.at[g, u]
            rcopy(here, here, m_send.at[g, u], m_recv.at[g, u], other).wait_recv()
    here = out.at[f, 1 - t]
    rcopy(here, here, m_send.at[f, 1 - t], m_recv.at[f, 1 - t], other).wait_recv()
    for u in range(n_tp):
        for i in range(n_half):
            for g in range(n_fs):
                lo = ((u * n_half + i) * n_fs + g) * cw
                final[:, lo : lo + cw] = out[g, u, :, i * cw : (i + 1) * cw]


def vmem(count):
    return [pl.BlockSpec(memory_space=pltpu.VMEM)] * count


def dma(*shape):
    return pltpu.SemaphoreType.DMA(shape) if shape else pltpu.SemaphoreType.DMA


def comm(kernel, outs, scratch, number, name):
    return pl.pallas_call(
        kernel,
        out_shape=[jax.ShapeDtypeStruct(a, b) for a, b in outs],
        out_specs=vmem(len(outs)),
        scratch_shapes=scratch,
        compiler_params=pltpu.CompilerParams(
            collective_id=number, has_side_effects=True, vmem_limit_bytes=60 * 1024 * 1024
        ),
        name=name,
    )


def body(
    n_sp, n_fs, n_tp, tokens, norm_gain, w_query, forget_weight, w_input, w_outgate, w_pool, forget_gap,
    extra_decay, rec_gain, group_weight, pool_gain, recurrent_output_weight, w_out_pool,
):
    s, f, t = place()
    rows, half = tokens.shape[1:]
    width = w_query.shape[1]
    ch = width // n_fs
    n_w = 5
    wr = w_query.shape[0]
    lanes = rows // 128
    extra = jnp.pad(extra_decay[0].T.reshape(n_fs, lanes, 128), ((0, 0), (0, 8 - lanes), (0, 0)))
    cw = w_out_pool.shape[1]
    z, e_all, ow = comm(
        functools.partial(project_kernel, n_sp, n_fs, n_tp),
        [((n_fs, rows, n_w * ch), BF), ((n_fs, 8, 128), F32), ((2 * width, cw), BF)],
        [
            pltpu.VMEM((n_fs, wr, n_w * ch), BF), pltpu.VMEM((n_fs, rows, n_tp * half), BF),
            pltpu.VMEM((n_sp * n_fs * wr, n_w * ch), BF), pltpu.VMEM((n_fs, rows, n_w * ch), F32),
            dma(2, 2), dma(n_fs, 2), dma(2), dma(n_fs, 2), dma(n_fs, 2), dma(n_fs - 1), dma(n_sp, n_fs),
            dma(n_sp, n_fs), dma(n_sp, n_fs), dma(n_fs - 1), dma(n_fs),
        ],
        1, "project",
    )(
        tokens[0], w_query, forget_weight, w_input, w_outgate, w_pool, extra, norm_gain[None],
        group_weight, pool_gain[None], recurrent_output_weight, w_out_pool,
    )
    n_half = n_sp // n_tp
    act, sq = comm(
        functools.partial(state_kernel, n_sp, group_weight.shape[1]),
        [((2, n_fs * rows, ch), BF), ((n_fs, 8, 128), F32)],
        [
            pltpu.VMEM((n_fs, rows, ch), F32), pltpu.VMEM((n_fs, rows, ch), F32),
            pltpu.VMEM((n_fs, ch, ch), BF), pltpu.VMEM((n_fs, 8, ch), F32),
            pltpu.VMEM((n_sp - 1, n_fs, ch, ch), BF), pltpu.VMEM((n_sp - 1, n_fs, 8, ch), F32),
            pltpu.VMEM((n_fs, 2**POOL_GROUPS, ch), BF),
            dma(n_sp - 1), dma(n_sp - 1), dma(n_sp - 1), dma(n_sp - 1), dma(), dma(),
        ],
        2, "state",
    )(z, e_all, forget_gap[None], rec_gain[None])
    out_shape = (n_fs, n_tp, rows // n_tp, n_half * cw)
    (final,) = comm(
        functools.partial(mix_kernel, n_sp, n_fs, n_tp),
        [((rows // n_tp, n_tp * n_half * n_fs * cw), BF)],
        [
            pltpu.VMEM(out_shape, BF), pltpu.VMEM((n_tp, n_fs) + act.shape, BF), pltpu.VMEM((n_tp, n_fs) + sq.shape, F32),
            pltpu.VMEM((n_half, n_tp) + ow.shape, BF), pltpu.VMEM((n_sp,) + ow.shape, BF),
            pltpu.VMEM((2, n_tp * width, n_half * cw), BF), pltpu.VMEM(out_shape, BF),
            dma(2, 2), dma(n_fs, 2), dma(2), dma(n_fs, 2), dma(n_fs, 2), dma(n_fs, n_tp), dma(n_tp, n_fs),
            dma(n_sp), dma(n_sp), dma(n_sp), dma(n_sp), dma(n_sp), dma(n_fs, n_tp), dma(n_fs, n_tp),
        ],
        3, "mix",
    )(act, sq, ow)
    return final[None]


def mm(a, b, dims):
    return lax.dot_general(a, b, (dims, ((), ())), preferred_element_type=F32)


NN, NT, TN = ((1,), (0,)), ((1,), (1,)), ((0,), (0,))


def layer_kernel(
    n_sp, n_fs, n_tp, tok, wq, wf, wi, wo, wp, extra, gain, gap, rec_gain, gmap, pgain, wor, wop, final,
    src0, src1, src2, ws0, ws1, ws2, xs, xn, acc0, acc1, acc2, e_src, e_all, local, qd, own_st, own_de,
    t_out, t_in, rim_src, rim, acts, sq_src, sq_all, ow_buf, ow_oth, part, half_way,
    x_send, x_recv, xf_send, xd_send, xd_recv, w_send, w_recv, up_send, dn_send, e_send, e_recv,
    t_send, t_recv, g_send, g_recv, a_send, a_recv, af_send, ad_send, ad_recv, q_send, q_recv,
    ou_send, on_send, o_recv, od_send, od_recv, m_send, m_recv,
):
    s, f, t = place()
    rows, half = tok.shape
    cut = rows // 2
    wr, width = wq.shape
    ch = width // n_fs
    cw = wor.shape[1]
    n_half = n_sp // n_tp
    out_rows = rows // n_tp
    lanes = rows // 128
    size = 128
    groups = ((wq, wf, wi), (wp,), (wo,))
    srcs, wss, accs = (src0, src1, src2), (ws0, ws1, ws2), (acc0, acc1, acc2)
    other = (s, f, 1 - t)
    px, py, pd = square(f)
    order = (f, px, py, pd)
    up, down = (s + 1, f, t), (s - 1, f, t)
    has_up, has_down = s < n_sp - 1, s > 0
    sends = []

    def send(c):
        c.start()
        sends.append(c)

    def when(cond, *copies):
        @pl.when(cond)
        def _():
            for c in copies:
                c.start()

    def pack(c):
        for i, w in enumerate(groups[c]):
            for g in range(n_fs):
                srcs[c][g, :, i * ch : (i + 1) * ch] = w[:, g * ch : (g + 1) * ch]

    pack(0)
    e_rows = extra[...].T
    for g in range(n_fs):
        e_src[g] = jnp.broadcast_to(e_rows[g : g + 1, :], e_src.shape[1:])
    greet(
        [(None, other)]
        + [(None, (s, g, u)) for g in order[1:] for u in (t, 1 - t)]
        + [(has_up, up), (has_down, down)]
    )

    def cols(c):
        return pl.ds(pl.multiple_of(c * half, half), half)

    def span(a, b):
        return pl.ds(pl.multiple_of((a * n_fs + b) * wr, wr), wr)

    def slot(c, a, b):
        return wss[c].at[span(a, b), :]

    def to_up(c, src, a, b):
        return rcopy(src, slot(c, a, b), up_send.at[c, a, b], w_recv.at[c, a, b], up)

    def to_down(c, src, a, b):
        return rcopy(src, slot(c, a, b), dn_send.at[c, a, b], w_recv.at[c, a, b], down)

    def both(c, src, a, b):
        when(has_up, to_up(c, src, a, b))
        when(has_down, to_down(c, src, a, b))

    def spread(c):
        for i, g in enumerate(order[1:]):
            send(rcopy(srcs[c].at[g], slot(c, s, f), w_send.at[c, i], w_recv.at[c, s, f], (s, g, t)))

    def from_square(c, g):
        to_up(c, slot(c, s, g), s, g).wait_recv()
        both(c, slot(c, s, g), s, g)

    def relay(c, d, gs):
        for g in gs:
            a, b = s - d, s + d

            @pl.when((a >= 0) & has_up)
            def _():
                to_up(c, slot(c, a, g), a, g).wait_recv()
                to_up(c, slot(c, a, g), a, g).start()

            @pl.when((b < n_sp) & has_down)
            def _():
                to_down(c, slot(c, b, g), b, g).wait_recv()
                to_down(c, slot(c, b, g), b, g).start()

    def arrive(c, d):
        for g in order:
            a, b = s - d, s + d

            @pl.when((a >= 0) & jnp.logical_not(has_up))
            def _():
                to_up(c, slot(c, a, g), a, g).wait_recv()

            @pl.when((b < n_sp) & jnp.logical_not(has_down))
            def _():
                to_down(c, slot(c, b, g), b, g).wait_recv()

    blk = n_fs * wr
    total_k = n_sp * blk
    is_end = jnp.logical_not(has_up & has_down)
    near = pl.ds(pl.multiple_of(jnp.where(has_down, blk, 0), blk), total_k - blk)
    far = pl.ds(pl.multiple_of(jnp.where(has_down, 0, total_k - blk), blk), blk)

    def gemm(c, p, k, more):
        out = jnp.dot(xn[p, :, k], wss[c][k, :], preferred_element_type=F32)
        accs[c][p] = accs[c][p] + out if more else out

    def main(c, p):
        pl.when(is_end)(lambda: gemm(c, p, near, False))
        pl.when(jnp.logical_not(is_end))(lambda: gemm(c, p, slice(0, total_k), False))

    def each_pair(step):
        def one(p, _):
            step(p)
            return 0

        lax.fori_loop(0, 2, one, 0)

    def last(c):
        arrive(c, n_sp - 1)
        pl.when(is_end)(lambda: each_pair(lambda p: gemm(c, p, far, True)))

    def x_slot(g, h, c):
        return xs.at[g, h * cut : (h + 1) * cut, cols(c)]

    def landed(g, h):
        here = x_slot(g, h, t)
        rcopy(here, here, xd_send.at[g, h], x_recv.at[g, h], other).wait_recv()
        return here

    def hand_on(g, h, here):
        send(rcopy(here, here, xd_send.at[g, h], xd_recv.at[g, h], other))

    def norm(j):
        g = order[j]
        for h in range(2):
            here = x_slot(g, h, 1 - t)
            rcopy(here, here, xd_send.at[g, h], xd_recv.at[g, h], other).wait_recv()
        tile = 16

        def each(i, _):
            at = pl.ds(pl.multiple_of(i * tile, tile), tile)
            feats = xs[g, at, :].astype(F32)
            scale = lax.rsqrt(jnp.mean(feats * feats, axis=-1, keepdims=True) + EPS)
            to = pl.ds(pl.multiple_of((j % 2) * rows + i * tile, tile), tile)
            xn[j // 2, to, :] = (feats * scale * gain[...]).astype(BF)
            return 0

        lax.fori_loop(0, rows // tile, each, 0, unroll=2)

    def ow_up(src, a, k):
        return rcopy(src, ow_buf.at[a, k], ou_send.at[a, k], o_recv.at[a, k], up)

    def ow_down(src, a, k):
        return rcopy(src, ow_buf.at[a, k], on_send.at[a, k], o_recv.at[a, k], down)

    def ow_other(a, k):
        return rcopy(ow_buf.at[a, k], ow_oth.at[lax.rem(a, n_half), k], od_send.at[a, k], od_recv.at[lax.rem(a, n_half), k], other)

    def ow_share(a, k):
        when(a // n_half != t, ow_other(a, k))

    def ow_relay(d, k):
        a, b = s - d, s + d

        @pl.when((a >= 0) & has_up)
        def _():
            here = ow_buf.at[a, k]
            ow_up(here, a, k).wait_recv()
            ow_up(here, a, k).start()
            ow_share(a, k)

        @pl.when((b < n_sp) & has_down)
        def _():
            here = ow_buf.at[b, k]
            ow_down(here, b, k).wait_recv()
            ow_down(here, b, k).start()
            ow_share(b, k)

    def ow_take(d, k):
        a, b = s - d, s + d

        @pl.when((a >= 0) & jnp.logical_not(has_up))
        def _():
            ow_up(ow_buf.at[a, k], a, k).wait_recv()
            ow_share(a, k)

        @pl.when((b < n_sp) & jnp.logical_not(has_down))
        def _():
            ow_down(ow_buf.at[b, k], b, k).wait_recv()
            ow_share(b, k)

    both(0, src0.at[f], s, f)
    spread(0)
    for i, (p, hs) in enumerate(((px, (0, 1)), (py, (1, 0)))):
        for h in hs:
            send(rcopy(tok.at[h * cut : (h + 1) * cut, :], x_slot(f, h, t), x_send.at[i, h], x_recv.at[f, h], (s, p, t)))
    for h in range(2):
        send(rcopy(tok.at[h * cut : (h + 1) * cut, :], x_slot(f, h, t), xd_send.at[f, h], xd_recv.at[f, h], other))
    when(has_up, ow_up(wor, s, 0))
    when(has_down, ow_down(wor, s, 0))
    for i, g in enumerate(order[1:]):
        send(rcopy(e_src.at[g], e_all.at[f], e_send.at[i], e_recv.at[f], (s, g, t)))
    pack(1)
    pack(2)
    spread(1)
    spread(2)
    for c in range(3):
        wss[c][span(s, f), :] = srcs[c][f]
    xs[f, :, cols(t)] = tok[...]
    e_all[f] = e_src[f]
    for g in order[1:]:
        from_square(0, g)
    ow_buf[s, 0] = wor[...]
    gd = gmap.shape[1]
    for i in range(width // gd):
        at = slice(i * gd, (i + 1) * gd)
        scaled = (gmap[t * (width // gd) + i].astype(F32) * pgain[:, at]).astype(BF)
        ow_buf[s, 1, at, :] = jnp.dot(scaled, wop[at, :], preferred_element_type=F32).astype(BF)
    norm(0)
    relay(0, 1, order[:2])
    for i, (g, h, onto) in enumerate(((px, 0, py), (py, 1, px))):
        here = landed(g, h)
        send(rcopy(here, here, xf_send.at[i], x_recv.at[g, h], (s, onto, t)))
        hand_on(g, h, here)
    relay(0, 1, order[2:])
    for d in range(2, n_sp - 1):
        relay(0, d, order[:2])
    for g, h in ((px, 1), (py, 0)):
        hand_on(g, h, landed(g, h))
    norm(1)
    for d in range(2, n_sp - 1):
        relay(0, d, order[2:])
    both(1, src1.at[f], s, f)
    for g in order[1:]:
        from_square(1, g)
    norm(2)
    for d in range(1, n_sp - 1):
        arrive(0, d)
    main(0, 0)
    relay(1, 1, order)
    for h in range(2):
        hand_on(pd, h, landed(pd, h))
    for d in range(2, n_sp - 1):
        relay(1, d, order)
    both(2, src2.at[f], s, f)
    for g in order[1:]:
        from_square(2, g)
    norm(3)
    main(0, 1)
    relay(2, 1, order)
    last(0)
    for g in order[1:]:
        rcopy(e_src.at[f], e_all.at[g], e_send.at[0], e_recv.at[g], other).wait_recv()

    mine = pl.ds(pl.multiple_of(f * ch, ch), ch)
    gap_f = gap[:, mine]
    gain_f = rec_gain[:, mine]
    at = lax.broadcasted_iota(jnp.int32, (size, size), 0)
    causal = at >= lax.broadcasted_iota(jnp.int32, (size, size), 1)
    lower = jnp.where(causal, 1.0, 0.0).astype(BF)
    lower = jnp.concatenate([lower, lower], axis=1)

    def scan(j):
        p, base = j // 2, j % 2 * rows
        state = None
        so_far = jnp.zeros((1, ch), F32)
        e_cols = e_all[order[j]].T
        for n in range(rows // size):
            here = slice(n * size, (n + 1) * size)
            there = slice(base + n * size, base + (n + 1) * size)
            v = acc0[p, there, 2 * ch : 3 * ch].astype(BF)
            q = jax.nn.silu(acc0[p, there, 0:ch].astype(BF).astype(F32))
            k = gap_f * jax.nn.sigmoid(-acc0[p, there, ch : 2 * ch].astype(BF).astype(F32))
            logs = jnp.log1p(-k) + e_cols[here, 0:1]
            high = logs.astype(BF)
            low = (logs - high.astype(F32)).astype(BF)
            within = mm(lower, jnp.concatenate([high, low], axis=0), NN)
            mid = within[size // 2 - 1 : size // 2]
            end = within[size - 1 :]
            q = q * jnp.exp(within - mid)
            k = (k * jnp.exp(mid - within)).astype(BF)
            q_up = q.astype(BF)
            scores = jnp.where(causal, mm(q_up, k, NT), 0.0).astype(BF)
            out = mm(scores, v, NN)
            if n:
                out = out + mm(q_up, (state * jnp.exp(mid)).astype(BF), NT)
            local[j, here, :] = out
            qd[j, here, :] = (q * jnp.exp(mid + so_far)).astype(BF)
            fresh = mm(v, k, TN) * jnp.exp(end - mid)
            state = state * jnp.exp(end) + fresh if n else fresh
            so_far = so_far + end
        own_st[j] = state
        own_de[j] = jnp.broadcast_to(jnp.exp(so_far), own_de.shape[1:])

    scan(0)
    scan(1)
    scan(2)
    scan(3)

    def carry(g):
        return rcopy(t_out.at[g], t_in.at[g], t_send.at[g], t_recv.at[g], up)

    @pl.when(jnp.logical_not(has_down))
    def _():
        t_in[...] = jnp.zeros(t_in.shape, BF)
        rim[...] = jnp.zeros(rim.shape, BF)
        t_out[...] = own_st[...].astype(BF)
        for g in range(n_fs):
            carry(g).start()

    for d in range(2, n_sp - 1):
        relay(2, d, order)
    for d in range(1, n_sp - 1):
        arrive(1, d)
    each_pair(lambda p: main(1, p))
    last(1)
    reach = rim.shape[1]
    for j in range(n_fs):
        rim_src[j] = acc1[j // 2, (j % 2 + 1) * rows - reach : (j % 2 + 1) * rows, :].astype(BF)
    edge = rcopy(rim_src, rim, g_send, g_recv, up)
    when(has_up, edge)

    pl.when(jnp.logical_not(is_end))(lambda: each_pair(lambda p: main(2, p)))
    @pl.when(has_down & has_up)
    def _():
        for g in range(n_fs):
            carry(g).wait_recv()
            t_out[g] = (own_st[g] + t_in[g].astype(F32) * own_de[g, 0:1, :]).astype(BF)
            carry(g).start()

    when(has_up, ow_up(ow_buf.at[s, 1], s, 1))
    when(has_down, ow_down(ow_buf.at[s, 1], s, 1))
    for k in range(2):
        ow_share(s, k)
    ow_relay(1, 0)
    pl.when(has_down)(edge.wait_recv)

    group = (t * n_fs * ch + f * ch) // gd
    spot = s * rows + lax.broadcasted_iota(jnp.int32, (rows, ch), 0)
    window = 2
    for level in range(1, POOL_GROUPS):
        window = jnp.where(group == level, 2 ** (level + 1), window)
    share = 1.0 / jnp.minimum(spot + 1, window).astype(F32)

    def rows_of(g):
        return pl.ds(pl.multiple_of(g * rows, rows), rows)

    def pool(j):
        zp = acc1[j // 2, j % 2 * rows : (j % 2 + 1) * rows, :].astype(BF).astype(F32)
        running = jnp.concatenate([rim[j].astype(F32), zp], axis=0)
        total = None
        for level in range(POOL_GROUPS):
            stride = 2**level
            running = running[stride:] + running[:-stride]
            now = running[running.shape[0] - rows :]
            total = now if level == 0 else jnp.where(group == level, now, total)
        acts[1, t, f, rows_of(order[j]), :] = (total * share - zp).astype(BF)

    part_rows = n_fs * rows // 2

    def a_slot(k, u, g, h):
        return acts.at[k, u, g, pl.ds(pl.multiple_of(h * part_rows, part_rows), part_rows), :]

    def publish(k, h):
        here = a_slot(k, t, f, h)
        for i, p in enumerate((px, py)):
            send(rcopy(here, here, a_send.at[k, i, h], a_recv.at[k, f, h], (s, p, t)))
        send(rcopy(here, here, ad_send.at[k, f, h], ad_recv.at[k, f, h], other))

    def a_landed(k, g, h):
        here = a_slot(k, t, g, h)
        rcopy(here, here, ad_send.at[k, g, h], a_recv.at[k, g, h], other).wait_recv()
        return here

    def a_hand_on(k, g, h, here):
        send(rcopy(here, here, ad_send.at[k, g, h], ad_recv.at[k, g, h], other))

    def a_forward(k):
        for i, (g, h, onto) in enumerate(((px, 0, py), (py, 1, px))):
            here = a_landed(k, g, h)
            send(rcopy(here, here, af_send.at[k, i], a_recv.at[k, g, h], (s, onto, t)))
            a_hand_on(k, g, h, here)

    def a_rest(k):
        for g, h in ((px, 1), (py, 0), (pd, 0), (pd, 1)):
            a_hand_on(k, g, h, a_landed(k, g, h))

    def a_other(k):
        for g in order:
            for h in range(2):
                here = a_slot(k, 1 - t, g, h)
                rcopy(here, here, ad_send.at[k, g, h], ad_recv.at[k, g, h], other).wait_recv()

    halves = (f // 2, 1 - f // 2)
    for i, h in enumerate(halves):
        pool(2 * i)
        pool(2 * i + 1)
        publish(1, h)
    for d in range(1, n_sp - 1):
        arrive(2, d)
    pl.when(is_end)(lambda: each_pair(lambda p: gemm(2, p, near, False)))
    a_forward(1)
    last(2)
    @pl.when(has_down & jnp.logical_not(has_up))
    def _():
        for g in range(n_fs):
            carry(g).wait_recv()

    ones = jnp.ones((8, ch), BF)

    def finish(j):
        g = order[j]
        rec = local[j] + mm(qd[j], t_in[j], NT)
        sums = mm(ones, (rec * rec).astype(BF), NT)
        for i in range(lanes):
            sq_src[pl.ds(g * lanes + i, 1), :] = sums[0:1, i * 128 : (i + 1) * 128]
        gate = jax.nn.silu(acc2[j // 2, j % 2 * rows : (j % 2 + 1) * rows, :].astype(BF).astype(F32))
        acts[0, t, f, rows_of(g), :] = (rec * gain_f * gate).astype(BF)

    for i, h in enumerate(halves):
        finish(2 * i)
        finish(2 * i + 1)
        publish(0, h)
    for i, g in enumerate(order[1:]):
        for u in range(n_tp):
            send(rcopy(sq_src, sq_all.at[t, f], q_send.at[i, u], q_recv.at[t, f], (s, g, u)))
    send(rcopy(sq_src, sq_all.at[t, f], q_send.at[n_fs - 1, 0], q_recv.at[t, f], other))
    sq_all[t, f] = sq_src[...]
    ow_relay(1, 1)
    a_rest(1)
    for d in range(2, n_sp - 1):
        ow_relay(d, 0)
    a_forward(0)
    for d in range(2, n_sp - 1):
        ow_relay(d, 1)
    for k in range(2):
        ow_take(1, k)
    a_rest(0)
    for d in range(2, n_sp - 1):
        for k in range(2):
            ow_take(d, k)
    a_other(1)
    a_other(0)
    for g in order[1:]:
        for u in range(n_tp):
            here = sq_all.at[u, g]
            rcopy(here, here, q_send.at[0, 0], q_recv.at[u, g], other).wait_recv()
    here = sq_all.at[1 - t, f]
    rcopy(here, here, q_send.at[0, 0], q_recv.at[1 - t, f], other).wait_recv()
    sums = sum(sq_all[u, i] for u in range(n_tp) for i in range(n_fs))
    scale = lax.rsqrt(sums / (n_tp * width) + EPS).T
    scales = [
        jnp.concatenate([scale[:, g * lanes + i : g * lanes + i + 1] for i in range(lanes)], axis=0) for g in range(n_fs)
    ]
    late = s - t * n_half >= n_half - 1

    def spot_of(a, g):
        return pl.ds(pl.multiple_of((a * n_fs + g) * cw, cw), cw)

    def piece(i, g, u):
        return rcopy(
            part.at[i, g, u], final.at[:, spot_of(t * n_half + i, f)], m_send.at[i, g, u], m_recv.at[i, f, t], (s, g, u)
        )

    def weight_side(k, a, i, g):
        here = pl.ds(g * rows, rows)
        total = None
        for u, w in ((t, ow_buf.at[a, k]), (1 - t, ow_oth.at[i, k])):
            left = jnp.concatenate([acts[k, u, b, here, :] for b in range(n_fs)], axis=1)
            now = jnp.dot(left, w[...], preferred_element_type=F32)
            total = now if total is None else total + now
        return total

    for j in range(n_half):
        i = jnp.where(late, n_half - 1 - j, j)
        a = t * n_half + i
        for k in range(2):
            if j == n_half - 1:
                ow_take(n_sp - 1, k)
            rcopy(ow_buf.at[a, k], ow_oth.at[i, k], od_send.at[a, k], od_recv.at[i, k], other).wait_recv()
            for g in range(n_fs):
                if k == 0:
                    half_way[g] = weight_side(0, a, i, g) * scales[g]
                    continue
                mixed = (half_way[g] + weight_side(1, a, i, g)).astype(BF)
                for u in range(n_tp):
                    part[i, g, u] = mixed[u * out_rows : (u + 1) * out_rows]
                    when((g != f) | (u != t), piece(i, g, u))
        final[:, spot_of(a, f)] = part[i, f, t]

    for i in range(n_half):
        for g in range(n_fs):
            for u in range(n_tp):
                @pl.when((g != f) | (u != t))
                def _():
                    here = final.at[:, spot_of(u * n_half + i, g)]
                    rcopy(here, here, m_send.at[i, g, u], m_recv.at[i, g, u], other).wait_recv()
                    piece(i, g, u).wait_send()
    for c in sends:
        c.wait_send()
    for c in range(3):
        for d in range(n_sp):
            for g in order:
                a, b = s - d, s + d

                @pl.when((a >= 0) & has_up)
                def _():
                    to_up(c, slot(c, a, g), a, g).wait_send()

                @pl.when((b < n_sp) & has_down)
                def _():
                    to_down(c, slot(c, b, g), b, g).wait_send()
    for d in range(n_sp):
        for k in range(2):
            a, b = s - d, s + d

            @pl.when((a >= 0) & has_up)
            def _():
                ow_up(ow_buf.at[a, k], a, k).wait_send()

            @pl.when((b < n_sp) & has_down)
            def _():
                ow_down(ow_buf.at[b, k], b, k).wait_send()
    for i in range(n_half):
        for k in range(2):
            ow_other((1 - t) * n_half + i, k).wait_send()

    @pl.when(has_up)
    def _():
        edge.wait_send()
        for g in range(n_fs):
            carry(g).wait_send()


def fused(
    n_sp, n_fs, n_tp, tokens, norm_gain, w_query, forget_weight, w_input, w_outgate, w_pool, forget_gap,
    extra_decay, rec_gain, group_weight, pool_gain, recurrent_output_weight, w_out_pool,
):
    rows, half = tokens.shape[1:]
    wr, width = w_query.shape
    ch = width // n_fs
    cw = w_out_pool.shape[1]
    n_half = n_sp // n_tp
    feats = n_sp * n_fs * wr
    lanes = rows // 128

    def buf(kind, *shape):
        return pltpu.VMEM(shape, kind)

    (final,) = comm(
        functools.partial(layer_kernel, n_sp, n_fs, n_tp),
        [((rows // n_tp, n_sp * n_fs * cw), BF)],
        [
            buf(BF, n_fs, wr, 3 * ch), buf(BF, n_fs, wr, ch), buf(BF, n_fs, wr, ch),
            buf(BF, feats, 3 * ch), buf(BF, feats, ch), buf(BF, feats, ch),
            buf(BF, n_fs, rows, n_tp * half), buf(BF, 2, n_fs // 2 * rows, n_tp * half),
            buf(F32, 2, n_fs // 2 * rows, 3 * ch), buf(F32, 2, n_fs // 2 * rows, ch), buf(F32, 2, n_fs // 2 * rows, ch),
            buf(F32, n_fs, 8, rows), buf(F32, n_fs, 8, rows),
            buf(F32, n_fs, rows, ch), buf(BF, n_fs, rows, ch),
            buf(F32, n_fs, ch, ch), buf(F32, n_fs, 8, ch),
            buf(BF, n_fs, ch, ch), buf(BF, n_fs, ch, ch),
            buf(BF, n_fs, 2**POOL_GROUPS, ch), buf(BF, n_fs, 2**POOL_GROUPS, ch),
            buf(BF, 2, n_tp, n_fs, n_fs * rows, ch),
            buf(F32, n_fs * lanes, 128), buf(F32, n_tp, n_fs, n_fs * lanes, 128),
            buf(BF, n_sp, 2, width, cw), buf(BF, n_half, 2, width, cw),
            buf(BF, n_half, n_fs, n_tp, rows // n_tp, cw), buf(F32, n_fs, rows, cw),
            dma(2, 2), dma(n_fs, 2), dma(2), dma(n_fs, 2), dma(n_fs, 2),
            dma(3, n_fs - 1), dma(3, n_sp, n_fs), dma(3, n_sp, n_fs), dma(3, n_sp, n_fs), dma(n_fs - 1), dma(n_fs),
            dma(n_fs), dma(n_fs), dma(), dma(),
            dma(2, 2, 2), dma(2, n_fs, 2), dma(2, 2), dma(2, n_fs, 2), dma(2, n_fs, 2), dma(n_fs, n_tp), dma(n_tp, n_fs),
            dma(n_sp, 2), dma(n_sp, 2), dma(n_sp, 2), dma(n_sp, 2), dma(n_half, 2), dma(n_half, n_fs, n_tp), dma(n_half, n_fs, n_tp),
        ],
        1, "layer",
    )(
        tokens[0], w_query, forget_weight, w_input, w_outgate, w_pool, extra_decay[0], norm_gain[None],
        forget_gap[None], rec_gain[None], group_weight, pool_gain[None], recurrent_output_weight, w_out_pool,
    )
    return final[None]


def run(n_sp, n_fs, n_tp, *args):
    wr, width = args[2].shape
    whole = n_fs * wr % 128 == 0 and args[-1].shape[1] % 128 == 0 and args[0].shape[1] % 256 == 0
    return (fused if whole and width == n_fs * HEAD_DIM else body)(n_sp, n_fs, n_tp, *args)


def solution(mesh):
    sizes = dict(mesh.shape)
    weight = P(("sp", "fs"), "tp")
    placed = (
        P("fs", "sp", "tp"), P(), weight, weight, weight, weight, weight, P("tp"),
        P("fs", "sp", "tp"), P("tp"), P(), P("tp"), P("tp", ("sp", "fs")), P("tp", ("sp", "fs")),
    )
    return jax.shard_map(
        functools.partial(run, sizes["sp"], sizes["fs"], sizes["tp"]),
        mesh=mesh, in_specs=placed, out_specs=P("fs", ("sp", "tp"), None), check_vma=False,
    )
```

```python
import functools
import jax
import jax.numpy as jnp
from jax import lax
from jax.experimental import pallas as pl
from jax.experimental.pallas import tpu as pltpu
from jax.sharding import PartitionSpec as P

HEAD_DIM = 128
POOL_GROUPS = 4
BLOCK = 64
EPS = 1e-06
HIGH = lax.Precision.HIGHEST
MESH = pl.DeviceIdType.MESH
BF = jnp.bfloat16
F32 = jnp.float32


def place():
    return lax.axis_index("sp"), lax.axis_index("fs"), lax.axis_index("tp")


def rcopy(src, dst, ssem, rsem, dev):
    return pltpu.make_async_remote_copy(
        src_ref=src, dst_ref=dst, send_sem=ssem, recv_sem=rsem, device_id=dev, device_id_type=MESH
    )


def greet(devs):
    barrier = pltpu.get_barrier_semaphore()
    for cond, dev in devs:
        def tell(dev=dev):
            pl.semaphore_signal(barrier, inc=1, device_id=dev, device_id_type=MESH)
        if cond is None:
            tell()
        else:
            pl.when(cond)(tell)
    pl.semaphore_wait(barrier, sum(1 if cond is None else jnp.where(cond, 1, 0) for cond, _ in devs))


def square(f):
    near = f + 1 - 2 * lax.rem(f, 2)
    return near, lax.rem(f + 2, 4), lax.rem(near + 2, 4)


def project_kernel(
    n_sp, n_fs, n_tp, tok, wq, wf, wi, wo, wp, extra, gain, gmap, pgain, wor, wop, z_ref, e_ref, ow_ref,
    wsrc, xs, ws, acc, x_send, x_recv, f_send, d_send, d_recv, w_send, w_recv, zr_send, zl_send, e_send, e_recv,
):
    s, f, t = place()
    rows, half = tok.shape
    part = rows // 2
    mats = (wq, wf, wi, wo, wp)
    wr, width = wq.shape
    ch = width // n_fs
    for i, w in enumerate(mats):
        for g in range(n_fs):
            wsrc[g, :, i * ch : (i + 1) * ch] = w[:, g * ch : (g + 1) * ch]
    other = (s, f, 1 - t)
    px, py, pd = square(f)
    order = (f, px, py, pd)
    up, down = (s + 1, f, t), (s - 1, f, t)
    has_up, has_down = s < n_sp - 1, s > 0
    greet([(None, other)] + [(None, (s, g, t)) for g in order[1:]] + [(has_up, up), (has_down, down)])

    def cols(c):
        return pl.ds(pl.multiple_of(c * half, half), half)

    def span(a, b):
        return pl.ds(pl.multiple_of((a * n_fs + b) * wr, wr), wr)

    def slot(a, b):
        return ws.at[span(a, b), :]

    def to_up(src, a, b):
        return rcopy(src, slot(a, b), zr_send.at[a, b], w_recv.at[a, b], up)

    def to_down(src, a, b):
        return rcopy(src, slot(a, b), zl_send.at[a, b], w_recv.at[a, b], down)

    sends = []

    def send(c):
        c.start()
        sends.append(c)

    def x_slot(g, h, c):
        return xs.at[g, h * part : (h + 1) * part, cols(c)]

    own = wsrc.at[f]
    pl.when(has_up)(lambda: to_up(own, s, f).start())
    pl.when(has_down)(lambda: to_down(own, s, f).start())
    for i, g in enumerate((pd, px, py)):
        send(rcopy(wsrc.at[g], slot(s, f), w_send.at[i], w_recv.at[s, f], (s, g, t)))
    for i, (p, hs) in enumerate(((px, (0, 1)), (py, (1, 0)))):
        for h in hs:
            send(rcopy(tok.at[h * part : (h + 1) * part, :], x_slot(f, h, t), x_send.at[i, h], x_recv.at[f, h], (s, p, t)))
    for h in range(2):
        send(rcopy(tok.at[h * part : (h + 1) * part, :], x_slot(f, h, t), d_send.at[f, h], d_recv.at[f, h], other))
    for i, g in enumerate(order[1:]):
        send(rcopy(extra.at[g], e_ref.at[f], e_send.at[i], e_recv.at[f], (s, g, t)))
    ws[span(s, f), :] = wsrc[f]
    xs[f, :, cols(t)] = tok[...]
    e_ref[f] = extra[f]
    ow_ref[0:width, :] = wor[...]
    gd = gmap.shape[1]
    for i in range(width // gd):
        at = slice(i * gd, (i + 1) * gd)
        scaled = (gmap[t * (width // gd) + i].astype(F32) * pgain[:, at]).astype(BF)
        folded = jnp.dot(scaled, wop[at, :], preferred_element_type=F32)
        ow_ref[width + i * gd : width + (i + 1) * gd, :] = folded.astype(BF)

    for g in order[1:]:
        to_up(slot(s, g), s, g).wait_recv()
        pl.when(has_up)(lambda: to_up(slot(s, g), s, g).start())
        pl.when(has_down)(lambda: to_down(slot(s, g), s, g).start())

    def landed(g, h):
        here = x_slot(g, h, t)
        rcopy(here, here, d_send.at[g, h], x_recv.at[g, h], other).wait_recv()
        return here

    def hand_on(g, h, here):
        send(rcopy(here, here, d_send.at[g, h], d_recv.at[g, h], other))

    for i, (g, h, onto) in enumerate(((px, 0, py), (py, 1, px))):
        here = landed(g, h)
        send(rcopy(here, here, f_send.at[i], x_recv.at[g, h], (s, onto, t)))
        hand_on(g, h, here)

    def relay(d):
        for g in order:
            a = s - d

            @pl.when(a >= 0)
            def _():
                to_up(slot(a, g), a, g).wait_recv()
                pl.when(has_up)(lambda: to_up(slot(a, g), a, g).start())
            b = s + d

            @pl.when(b < n_sp)
            def _():
                to_down(slot(b, g), b, g).wait_recv()
                pl.when(has_down)(lambda: to_down(slot(b, g), b, g).start())

    def add(a):
        k = pl.ds(pl.multiple_of(a * n_fs * wr, n_fs * wr), n_fs * wr)

        def each(i, _):
            acc[i] += jnp.dot(xs[i, :, k], ws[k, :], preferred_element_type=F32)
            return 0

        lax.fori_loop(0, n_fs, each, 0)

    def multiply(d):
        pl.when(s - d >= 0)(lambda: add(s - d))
        pl.when(s + d < n_sp)(lambda: add(s + d))

    relay(1)
    for g, h in ((px, 1), (py, 0), (pd, 0), (pd, 1)):
        hand_on(g, h, landed(g, h))
    for d in range(2, n_sp - 1):
        relay(d)
    for g in order:
        for h in range(2):
            here = x_slot(g, h, 1 - t)
            rcopy(here, here, d_send.at[g, h], d_recv.at[g, h], other).wait_recv()
    for g in order[1:]:
        rcopy(extra.at[f], e_ref.at[g], e_send.at[0], e_recv.at[g], other).wait_recv()
    for c in sends:
        c.wait_send()

    def norm(j, _):
        tile = 16
        per = rows // tile
        at = (j // per, pl.ds(pl.multiple_of(lax.rem(j, per) * tile, tile), tile))
        feats = xs[at[0], at[1], :].astype(F32)
        scale = lax.rsqrt(jnp.mean(feats * feats, axis=-1, keepdims=True) + EPS)
        xs[at[0], at[1], :] = (feats * scale * gain[...]).astype(BF)
        return 0

    lax.fori_loop(0, n_fs * rows // 16, norm, 0, unroll=2)

    if n_fs * wr % 128 == 0:
        own_k = pl.ds(pl.multiple_of(s * n_fs * wr, n_fs * wr), n_fs * wr)

        def begin(i, _):
            acc[i] = jnp.dot(xs[i, :, own_k], ws[own_k, :], preferred_element_type=F32)
            return 0

        lax.fori_loop(0, n_fs, begin, 0)
        for d in range(1, n_sp - 1):
            multiply(d)
        relay(n_sp - 1)
        multiply(n_sp - 1)

        def finish(i, _):
            z_ref[i] = acc[i].astype(BF)
            return 0
    else:
        relay(n_sp - 1)

        def finish(i, _):
            z_ref[i] = jnp.dot(xs[i], ws[...], preferred_element_type=F32).astype(BF)
            return 0

    lax.fori_loop(0, n_fs, finish, 0)

    for d in range(n_sp):
        for g in order:
            a = s - d

            @pl.when((a >= 0) & has_up)
            def _():
                to_up(slot(a, g), a, g).wait_send()
            b = s + d

            @pl.when((b < n_sp) & has_down)
            def _():
                to_down(slot(b, g), b, g).wait_send()


def dot(a, b, dims):
    return lax.dot_general(a, b, (dims, ((), ())), precision=HIGH, preferred_element_type=F32)


def state_kernel(
    n_sp, group_dim, z, e_all, gap, rec_gain, act, sq_out,
    local, qd, own_st, own_de, st_in, de_in, rim, s_send, s_recv, c_send, c_recv, g_send, g_recv,
):
    s, f, t = place()
    n_fs, rows, _ = z.shape
    ch = HEAD_DIM
    reach = rim.shape[1]
    devs = []
    for d in range(1, n_sp):
        devs.append((s + d < n_sp, (s + d, f, t)))
        devs.append((s - d >= 0, (s - d, f, t)))
    greet(devs)
    edge = rcopy(z.at[:, rows - reach :, 4 * ch :], rim, g_send, g_recv, (s + 1, f, t))
    pl.when(s < n_sp - 1)(edge.start)
    mine = pl.ds(pl.multiple_of(f * ch, ch), ch)
    gap_f = gap[:, mine]
    gain_f = rec_gain[:, mine]
    at = lax.broadcasted_iota(jnp.int32, (BLOCK, BLOCK), 0)
    causal = at >= lax.broadcasted_iota(jnp.int32, (BLOCK, BLOCK), 1)
    lower = causal.astype(F32)

    def one(g, _):
        state = jnp.zeros((ch, ch), F32)
        so_far = jnp.zeros((1, ch), F32)
        e_cols = e_all[g].T
        for n in range(rows // BLOCK):
            here = slice(n * BLOCK, (n + 1) * BLOCK)
            q, fo, v = (z[g, here, i * ch : (i + 1) * ch].astype(F32) for i in range(3))
            q = jax.nn.silu(q)
            k = gap_f * jax.nn.sigmoid(-fo)
            lo = n * BLOCK % 128
            lane = n * BLOCK // 128
            logs = jnp.log1p(-k) + e_cols[lo : lo + BLOCK, lane : lane + 1]
            within = dot(lower, logs, ((1,), (0,)))
            end = within[BLOCK - 1 :]
            q_up = q * jnp.exp(within)
            scores = jnp.where(causal, dot(q_up, k * jnp.exp(-within), ((1,), (1,))), 0.0)
            out = dot(scores, v, ((1,), (0,)))
            if n:
                out = out + dot(q_up, state, ((1,), (1,)))
            local[g, here, :] = out
            qd[g, here, :] = q_up * jnp.exp(so_far)
            state = state * jnp.exp(end) + dot(v.T, k * jnp.exp(end - within), ((1,), (0,)))
            so_far = so_far + end
        own_st[g] = state.astype(BF)
        own_de[g] = jnp.broadcast_to(jnp.exp(so_far), (8, ch))
        return 0

    lax.fori_loop(0, n_fs, one, 0)

    def pair(d):
        dev = (s + d, f, t)
        return (
            rcopy(own_st, st_in.at[d - 1], s_send.at[d - 1], s_recv.at[d - 1], dev),
            rcopy(own_de, de_in.at[d - 1], c_send.at[d - 1], c_recv.at[d - 1], dev),
        )

    for d in range(1, n_sp):
        @pl.when(s + d < n_sp)
        def _():
            for c in pair(d):
                c.start()

        @pl.when(s - d < 0)
        def _():
            st_in[d - 1] = jnp.zeros(st_in.shape[1:], st_in.dtype)
            de_in[d - 1] = jnp.ones(de_in.shape[1:], de_in.dtype)
    pl.when(s == 0)(lambda: rim.__setitem__(Ellipsis, jnp.zeros(rim.shape, rim.dtype)))
    pl.when(s > 0)(edge.wait_recv)
    group = (t * n_fs * ch + f * ch) // group_dim
    spot = s * rows + lax.broadcasted_iota(jnp.int32, (rows, ch), 0)
    window = 2
    for level in range(1, POOL_GROUPS):
        window = jnp.where(group == level, 2 ** (level + 1), window)
    counts = jnp.minimum(spot + 1, window).astype(F32)
    for g in range(n_fs):
        zp = z[g, :, 4 * ch :].astype(F32)
        running = jnp.concatenate([rim[g].astype(F32), zp], axis=0)
        total = None
        for level in range(POOL_GROUPS):
            stride = 2**level
            running = running[stride:] + running[:-stride]
            now = running[running.shape[0] - rows :]
            total = now if level == 0 else jnp.where(group == level, now, total)
        act[1, g * rows : (g + 1) * rows, :] = (total / counts - zp).astype(BF)
    for d in range(1, n_sp):
        @pl.when(s - d >= 0)
        def _():
            for c in pair(d):
                c.wait_recv()

    ones = jnp.ones((8, ch), F32)

    def finish(g, _):
        total = jnp.zeros((ch, ch), F32)
        for d in range(n_sp - 2, -1, -1):
            total = de_in[d, g, 0:1, :] * total + st_in[d, g].astype(F32)
        rec = local[g] + dot(qd[g], total, ((1,), (1,)))
        sums = dot(ones, rec * rec, ((1,), (1,)))
        for i in range(rows // 128):
            sq_out[g, i : i + 1, :] = sums[0:1, i * 128 : (i + 1) * 128]
        gate = jax.nn.silu(z[g, :, 3 * ch : 4 * ch].astype(F32))
        act[0, pl.ds(pl.multiple_of(g * rows, rows), rows), :] = (rec * gain_f * gate).astype(BF)
        return 0

    sq_out[...] = jnp.zeros(sq_out.shape, F32)
    lax.fori_loop(0, n_fs, finish, 0)
    for d in range(1, n_sp):
        @pl.when(s + d < n_sp)
        def _():
            for c in pair(d):
                c.wait_send()
    pl.when(s < n_sp - 1)(edge.wait_send)


def mix_kernel(
    n_sp, n_fs, n_tp, act, sq, ow, final,
    out, acts, sq_all, ow_all, relay_buf, wbuf, part,
    a_send, a_recv, f_send, d_send, d_recv, q_send, q_recv,
    up_send, down_send, o_recv, od_send, od_recv, m_send, m_recv,
):
    s, f, t = place()
    n_half = n_sp // n_tp
    rows = act.shape[1] // n_fs
    half = rows // n_tp
    width, cw = ow.shape[0] // 2, ow.shape[1]
    other = (s, f, 1 - t)
    px, py, pd = square(f)
    up, down = (s + 1, f, t), (s - 1, f, t)
    has_up, has_down = s < n_sp - 1, s > 0
    greet(
        [(None, other)]
        + [(None, (s, g, u)) for g in (px, py, pd) for u in (t, 1 - t)]
        + [(has_up, up), (has_down, down)]
    )

    def to_up(src, a):
        return rcopy(src, relay_buf.at[a], up_send.at[a], o_recv.at[a], up)

    def to_down(src, a):
        return rcopy(src, relay_buf.at[a], down_send.at[a], o_recv.at[a], down)

    def to_other(src, a):
        return rcopy(src, ow_all.at[lax.rem(a, n_half), t], od_send.at[a], od_recv.at[a], other)

    def keep(src, a):
        mine = a // n_half == t

        @pl.when(mine)
        def _():
            ow_all[lax.rem(a, n_half), t] = src[...]

        pl.when(jnp.logical_not(mine))(lambda: to_other(src, a).start())

    sends = []

    def send(c):
        c.start()
        sends.append(c)

    for i, (p, order) in enumerate(((px, (0, 1)), (py, (1, 0)))):
        for h in order:
            send(rcopy(act.at[h], acts.at[t, f, h], a_send.at[i, h], a_recv.at[f, h], (s, p, t)))
    pl.when(has_up)(lambda: to_up(ow, s).start())
    pl.when(has_down)(lambda: to_down(ow, s).start())
    for h in range(2):
        send(rcopy(act.at[h], acts.at[t, f, h], d_send.at[f, h], d_recv.at[f, h], other))
    for i, g in enumerate((px, py, pd)):
        for u in range(n_tp):
            send(rcopy(sq, sq_all.at[t, f], q_send.at[i, u], q_recv.at[t, f], (s, g, u)))
    send(rcopy(sq, sq_all.at[t, f], q_send.at[n_fs - 1, 0], q_recv.at[t, f], other))
    acts[t, f] = act[...]
    sq_all[t, f] = sq[...]
    keep(ow, s)

    def landed(g, h):
        here = acts.at[t, g, h]
        rcopy(here, here, d_send.at[g, h], a_recv.at[g, h], other).wait_recv()
        return here

    def hand_on(g, h, here):
        send(rcopy(here, here, d_send.at[g, h], d_recv.at[g, h], other))

    for i, (g, h, onto) in enumerate(((px, 0, py), (py, 1, px))):
        here = landed(g, h)
        send(rcopy(here, here, f_send.at[i], a_recv.at[g, h], (s, onto, t)))
        hand_on(g, h, here)

    def step(d):
        a = s - d

        @pl.when(a >= 0)
        def _():
            to_up(relay_buf.at[a], a).wait_recv()
            pl.when(has_up)(lambda: to_up(relay_buf.at[a], a).start())
            keep(relay_buf.at[a], a)
        b = s + d

        @pl.when(b < n_sp)
        def _():
            to_down(relay_buf.at[b], b).wait_recv()
            pl.when(has_down)(lambda: to_down(relay_buf.at[b], b).start())
            keep(relay_buf.at[b], b)

    for d in range(1, n_sp):
        step(d)
    for g, h in ((px, 1), (py, 0), (pd, 0), (pd, 1)):
        hand_on(g, h, landed(g, h))
    for i in range(n_half):
        a = t * n_half + i
        here = ow_all.at[i, 1 - t]
        rcopy(here, here, od_send.at[a], od_recv.at[a], other).wait_recv()
    for i in range(n_half):
        for u in range(n_tp):
            for k in range(2):
                wbuf[k, u * width : (u + 1) * width, i * cw : (i + 1) * cw] = ow_all[i, u, k * width : (k + 1) * width, :]
    for g in (px, py, pd):
        for u in range(n_tp):
            here = sq_all.at[u, g]
            rcopy(here, here, q_send.at[0, 0], q_recv.at[u, g], other).wait_recv()
    here = sq_all.at[1 - t, f]
    rcopy(here, here, q_send.at[0, 0], q_recv.at[1 - t, f], other).wait_recv()
    for g in (f, px, py, pd):
        for h in range(2):
            here = acts.at[1 - t, g, h]
            rcopy(here, here, d_send.at[g, h], d_recv.at[g, h], other).wait_recv()

    def piece(g, u):
        return rcopy(part.at[g, u], out.at[f, t], m_send.at[g, u], m_recv.at[f, t], (s, g, u))

    def spread(g):
        for u in range(n_tp):
            c = piece(g, u)
            c.start()
            sends.append(c)

    last = None
    for g in (pd, f, px, py):
        here = pl.ds(pl.multiple_of(g * rows, rows), rows)
        sums = sum(sq_all[u, i, g] for u in range(n_tp) for i in range(n_fs))
        scale = lax.rsqrt(sums / (n_tp * width) + EPS).T
        scale = jnp.concatenate([scale[:, i : i + 1] for i in range(rows // 128)], axis=0)
        left = [
            jnp.concatenate([acts[u, i, h, here, :] for u in range(n_tp) for i in range(n_fs)], axis=1)
            for h in range(2)
        ]
        mixed = (
            jnp.dot(left[0], wbuf[0], preferred_element_type=F32) * scale
            + jnp.dot(left[1], wbuf[1], preferred_element_type=F32)
        ).astype(BF)
        for u in range(n_tp):
            part[g, u] = mixed[u * half : (u + 1) * half]
        if last is not None and last is not f:
            spread(last)
        if last is f:
            c = piece(f, 1 - t)
            c.start()
            sends.append(c)
        last = g
    out[f, t] = part[f, t]
    for i in range(n_half):
        to_other(ow, (1 - t) * n_half + i).wait_send()
    for d in range(n_sp):
        a, b = s - d, s + d

        @pl.when((a >= 0) & has_up)
        def _():
            to_up(ow, a).wait_send()

        @pl.when((b < n_sp) & has_down)
        def _():
            to_down(ow, b).wait_send()
    spread(last)
    for c in sends:
        c.wait_send()
    for g in (px, py, pd):
        for u in range(n_tp):
            here = out.at[g, u]
            rcopy(here, here, m_send.at[g, u], m_recv.at[g, u], other).wait_recv()
    here = out.at[f, 1 - t]
    rcopy(here, here, m_send.at[f, 1 - t], m_recv.at[f, 1 - t], other).wait_recv()
    for u in range(n_tp):
        for i in range(n_half):
            for g in range(n_fs):
                lo = ((u * n_half + i) * n_fs + g) * cw
                final[:, lo : lo + cw] = out[g, u, :, i * cw : (i + 1) * cw]


def vmem(count):
    return [pl.BlockSpec(memory_space=pltpu.VMEM)] * count


def dma(*shape):
    return pltpu.SemaphoreType.DMA(shape) if shape else pltpu.SemaphoreType.DMA


def comm(kernel, outs, scratch, number, name, ins=None):
    return pl.pallas_call(
        kernel,
        out_shape=[jax.ShapeDtypeStruct(a, b) for a, b in outs],
        out_specs=vmem(len(outs)),
        **({} if ins is None else {"in_specs": ins}),
        scratch_shapes=scratch,
        compiler_params=pltpu.CompilerParams(
            collective_id=number, has_side_effects=True, vmem_limit_bytes=60 * 1024 * 1024
        ),
        name=name,
    )


def body(
    n_sp, n_fs, n_tp, tokens, norm_gain, w_query, forget_weight, w_input, w_outgate, w_pool, forget_gap,
    extra_decay, rec_gain, group_weight, pool_gain, recurrent_output_weight, w_out_pool,
):
    s, f, t = place()
    rows, half = tokens.shape[1:]
    width = w_query.shape[1]
    ch = width // n_fs
    n_w = 5
    wr = w_query.shape[0]
    lanes = rows // 128
    extra = jnp.pad(extra_decay[0].T.reshape(n_fs, lanes, 128), ((0, 0), (0, 8 - lanes), (0, 0)))
    cw = w_out_pool.shape[1]
    z, e_all, ow = comm(
        functools.partial(project_kernel, n_sp, n_fs, n_tp),
        [((n_fs, rows, n_w * ch), BF), ((n_fs, 8, 128), F32), ((2 * width, cw), BF)],
        [
            pltpu.VMEM((n_fs, wr, n_w * ch), BF), pltpu.VMEM((n_fs, rows, n_tp * half), BF),
            pltpu.VMEM((n_sp * n_fs * wr, n_w * ch), BF), pltpu.VMEM((n_fs, rows, n_w * ch), F32),
            dma(2, 2), dma(n_fs, 2), dma(2), dma(n_fs, 2), dma(n_fs, 2), dma(n_fs - 1), dma(n_sp, n_fs),
            dma(n_sp, n_fs), dma(n_sp, n_fs), dma(n_fs - 1), dma(n_fs),
        ],
        1, "project",
    )(
        tokens[0], w_query, forget_weight, w_input, w_outgate, w_pool, extra, norm_gain[None],
        group_weight, pool_gain[None], recurrent_output_weight, w_out_pool,
    )
    n_half = n_sp // n_tp
    act, sq = comm(
        functools.partial(state_kernel, n_sp, group_weight.shape[1]),
        [((2, n_fs * rows, ch), BF), ((n_fs, 8, 128), F32)],
        [
            pltpu.VMEM((n_fs, rows, ch), F32), pltpu.VMEM((n_fs, rows, ch), F32),
            pltpu.VMEM((n_fs, ch, ch), BF), pltpu.VMEM((n_fs, 8, ch), F32),
            pltpu.VMEM((n_sp - 1, n_fs, ch, ch), BF), pltpu.VMEM((n_sp - 1, n_fs, 8, ch), F32),
            pltpu.VMEM((n_fs, 2**POOL_GROUPS, ch), BF),
            dma(n_sp - 1), dma(n_sp - 1), dma(n_sp - 1), dma(n_sp - 1), dma(), dma(),
        ],
        2, "state",
    )(z, e_all, forget_gap[None], rec_gain[None])
    out_shape = (n_fs, n_tp, rows // n_tp, n_half * cw)
    (final,) = comm(
        functools.partial(mix_kernel, n_sp, n_fs, n_tp),
        [((rows // n_tp, n_tp * n_half * n_fs * cw), BF)],
        [
            pltpu.VMEM(out_shape, BF), pltpu.VMEM((n_tp, n_fs) + act.shape, BF), pltpu.VMEM((n_tp, n_fs) + sq.shape, F32),
            pltpu.VMEM((n_half, n_tp) + ow.shape, BF), pltpu.VMEM((n_sp,) + ow.shape, BF),
            pltpu.VMEM((2, n_tp * width, n_half * cw), BF), pltpu.VMEM(out_shape, BF),
            dma(2, 2), dma(n_fs, 2), dma(2), dma(n_fs, 2), dma(n_fs, 2), dma(n_fs, n_tp), dma(n_tp, n_fs),
            dma(n_sp), dma(n_sp), dma(n_sp), dma(n_sp), dma(n_sp), dma(n_fs, n_tp), dma(n_fs, n_tp),
        ],
        3, "mix",
    )(act, sq, ow)
    return final[None]


def mm(a, b, dims):
    return lax.dot_general(a, b, (dims, ((), ())), preferred_element_type=F32)


NN, NT, TN = ((1,), (0,)), ((1,), (1,)), ((0,), (0,))


def layer_kernel(
    n_sp, n_fs, n_tp, tok, wq, wf, wi, wo, wp, extra_in, gain_in, gap_in, rec_gain_in, gmap_in, pgain_in, wor, wop_in, final,
    src0, src1, src2, ws0, ws1, ws2, xs, xn, acc0, acc1, acc2, e_src, e_all, local, qd, own_st, own_de,
    t_out, t_in, rim_src, rim, acts, sq_src, sq_all, ow_buf, ow_oth, part, half_way,
    extra, gain, gap, rec_gain, gmap, pgain, wop,
    in_sem, w_in, p_in, x_send, x_recv, xd_send, xd_recv, w_send, w_recv, b_recv, ba_recv, up_send, dn_send, e_send, e_recv,
    t_send, t_recv, g_send, g_recv, a_send, a_recv, ad_send, ad_recv, q_send, q_recv,
    ou_send, on_send, o_recv, od_send, od_recv, m_send, m_recv,
):
    s, f, t = place()
    rows, half = tok.shape
    cut = rows // 2
    wr, width = wq.shape
    ch = width // n_fs
    cw = wor.shape[1]
    n_half = n_sp // n_tp
    out_rows = rows // n_tp
    lanes = rows // 128
    size = 128
    blk = n_fs * wr
    total_k = n_sp * blk
    groups = ((wq, wf, wi), (wp,), (wo,))
    srcs, wss, accs = (src0, src1, src2), (ws0, ws1, ws2), (acc0, acc1, acc2)
    other = (s, f, 1 - t)
    px, py, pd = square(f)
    order = (f, px, py, pd)
    up, down = (s + 1, f, t), (s - 1, f, t)
    has_up, has_down = s < n_sp - 1, s > 0
    is_end = jnp.logical_not(has_up & has_down)

    def when(cond, *copies):
        @pl.when(cond)
        def _():
            for c in copies:
                c.start()

    def sent(ref, sem):
        rcopy(ref, ref, sem, sem, other).wait_send()

    def came(ref, sem):
        rcopy(ref, ref, sem, sem, other).wait_recv()

    def cols(c):
        return pl.ds(pl.multiple_of(c * half, half), half)

    def span(a, b):
        return pl.ds(pl.multiple_of((a * n_fs + b) * wr, wr), wr)

    def slot(c, a, b):
        return wss[c].at[span(a, b), :]

    def block(c, a):
        return wss[c].at[pl.ds(pl.multiple_of(a * blk, blk), blk), :]

    def x_slot(g, h, c):
        return xs.at[g, h * cut : (h + 1) * cut, cols(c)]

    peers = (
        [(None, other)]
        + [(None, (s, g, u)) for g in order[1:] for u in (t, 1 - t)]
        + [(has_up, up), (has_down, down)]
    )
    barrier = pltpu.get_barrier_semaphore()
    for cond, dev in peers:
        def tell(dev=dev):
            pl.semaphore_signal(barrier, inc=1, device_id=dev, device_id_type=MESH)
        if cond is None:
            tell()
        else:
            pl.when(cond)(tell)
    for c in range(3):
        for i, w in enumerate(groups[c]):
            for j, g in enumerate(order):
                lane = pl.ds(pl.multiple_of(g * ch, ch), ch)
                into = wss[c].at[span(s, f), i * ch : (i + 1) * ch] if j == 0 else srcs[c].at[j - 1, :, i * ch : (i + 1) * ch]
                pltpu.make_async_copy(w.at[:, lane], into, w_in.at[c, min(j, 1)]).start()
        if c == 0:
            pltpu.make_async_copy(tok, xs.at[f, :, cols(t)], in_sem.at[0]).start()
            pltpu.make_async_copy(wor, ow_buf.at[s, 0], in_sem.at[1]).start()
    params = ((extra_in, extra), (gain_in, gain), (gmap_in, gmap), (pgain_in, pgain), (wop_in, wop), (gap_in, gap), (rec_gain_in, rec_gain))
    loads = [pltpu.make_async_copy(a, b, p_in.at[i]) for i, (a, b) in enumerate(params)]
    for c in loads:
        c.start()
    pl.semaphore_wait(barrier, sum(1 if cond is None else jnp.where(cond, 1, 0) for cond, _ in peers))

    def took(ref, sem):
        pltpu.make_async_copy(ref, ref, sem).wait()

    def to_up(src, b, a):
        return rcopy(src, slot(0, a, b), up_send.at[0], w_recv.at[a, b], up)

    def to_down(src, b, a):
        return rcopy(src, slot(0, a, b), dn_send.at[0], w_recv.at[a, b], down)

    def both(a, b):
        when(has_up, to_up(slot(0, a, b), b, a))
        when(has_down, to_down(slot(0, a, b), b, a))

    def b_up(c, a):
        return rcopy(block(c, a), block(c, a), up_send.at[c], b_recv.at[c - 1, a], up)

    def b_down(c, a):
        return rcopy(block(c, a), block(c, a), dn_send.at[c], b_recv.at[c - 1, a], down)

    def spread(c):
        for j, g in enumerate(order[1:]):
            rsem = w_recv.at[s, f] if c == 0 else ba_recv.at[c - 1]
            rcopy(srcs[c].at[j], slot(c, s, f), w_send.at[c], rsem, (s, g, t)).start()

    def own_block(c):
        came(wss[c].at[0 : (n_fs - 1) * wr, :], ba_recv.at[c - 1])
        when(has_up, b_up(c, s))
        when(has_down, b_down(c, s))

    low = 2 * s < n_sp

    def relay(c, d, gs=(None,)):
        a, b = s - d, s + d

        def rising(extra):
            for g in gs:
                @pl.when((a >= 0) & has_up & extra)
                def _():
                    hop = to_up(slot(0, a, g), g, a) if c == 0 else b_up(c, a)
                    hop.wait_recv()
                    hop.start()

        def falling():
            for g in gs:
                @pl.when((b < n_sp) & has_down)
                def _():
                    hop = to_down(slot(0, b, g), g, b) if c == 0 else b_down(c, b)
                    hop.wait_recv()
                    hop.start()

        rising(low)
        falling()
        rising(jnp.logical_not(low))

    def arrive(c, d):
        for g in order if c == 0 else (None,):
            a, b = s - d, s + d

            @pl.when((a >= 0) & jnp.logical_not(has_up))
            def _():
                (to_up(slot(0, a, g), g, a) if c == 0 else b_up(c, a)).wait_recv()

            @pl.when((b < n_sp) & jnp.logical_not(has_down))
            def _():
                (to_down(slot(0, b, g), g, b) if c == 0 else b_down(c, b)).wait_recv()

    near = pl.ds(pl.multiple_of(jnp.where(has_down, blk, 0), blk), total_k - blk)
    far = pl.ds(pl.multiple_of(jnp.where(has_down, 0, total_k - blk), blk), blk)

    def gemm(c, p, k, more):
        out = jnp.dot(xn[p, :, k], wss[c][k, :], preferred_element_type=F32)
        accs[c][p] = accs[c][p] + out if more else out

    def main(c, p):
        pl.when(is_end)(lambda: gemm(c, p, near, False))
        pl.when(jnp.logical_not(is_end))(lambda: gemm(c, p, slice(0, total_k), False))

    def each_pair(step):
        def one(p, _):
            step(p)
            return 0

        lax.fori_loop(0, 2, one, 0)

    def last(c):
        arrive(c, n_sp - 1)
        pl.when(is_end)(lambda: each_pair(lambda p: gemm(c, p, far, True)))

    def landed(g, h):
        here = x_slot(g, h, t)
        came(here, x_recv.at[g, h])
        return here

    def hand_on(g, h):
        here = x_slot(g, h, t)
        rcopy(here, here, xd_send, xd_recv.at[g], other).start()

    def norm(j):
        g = order[j]
        came(xs.at[g, :, cols(1 - t)], xd_recv.at[g])
        tile = 16

        def each(i, _):
            at = pl.ds(pl.multiple_of(i * tile, tile), tile)
            feats = xs[g, at, :].astype(F32)
            scale = lax.rsqrt(jnp.mean(feats * feats, axis=-1, keepdims=True) + EPS)
            to = pl.ds(pl.multiple_of((j % 2) * rows + i * tile, tile), tile)
            xn[j // 2, to, :] = (feats * scale * gain[...]).astype(BF)
            return 0

        lax.fori_loop(0, rows // tile, each, 0, unroll=2)

    def ow_up(a, k):
        return rcopy(ow_buf.at[a, k], ow_buf.at[a, k], ou_send, o_recv.at[a, k], up)

    def ow_down(a, k):
        return rcopy(ow_buf.at[a, k], ow_buf.at[a, k], on_send, o_recv.at[a, k], down)

    def ow_share(a, k):
        i = lax.rem(a, n_half)
        when(a // n_half != t, rcopy(ow_buf.at[a, k], ow_oth.at[i, k], od_send, od_recv.at[i, k], other))

    def ow_relay(d, k):
        a, b = s - d, s + d

        @pl.when((a >= 0) & has_up)
        def _():
            ow_up(a, k).wait_recv()
            ow_up(a, k).start()
            ow_share(a, k)

        @pl.when((b < n_sp) & has_down)
        def _():
            ow_down(b, k).wait_recv()
            ow_down(b, k).start()
            ow_share(b, k)

    def ow_take(d, k):
        a, b = s - d, s + d

        @pl.when((a >= 0) & jnp.logical_not(has_up))
        def _():
            ow_up(a, k).wait_recv()
            ow_share(a, k)

        @pl.when((b < n_sp) & jnp.logical_not(has_down))
        def _():
            ow_down(b, k).wait_recv()
            ow_share(b, k)

    took(slot(0, s, f), w_in.at[0, 0])
    both(s, f)
    took(srcs[0], w_in.at[0, 1])
    spread(0)
    took(xs.at[f, :, cols(t)], in_sem.at[0])
    for p, hs in ((px, (0, 1)), (py, (1, 0))):
        for h in hs:
            rcopy(x_slot(f, h, t), x_slot(f, h, t), x_send, x_recv.at[f, h], (s, p, t)).start()
    for h in range(2):
        hand_on(f, h)
    took(ow_buf.at[s, 0], in_sem.at[1])
    when(has_up, ow_up(s, 0))
    when(has_down, ow_down(s, 0))
    for c in loads:
        c.wait()
    e_rows = extra[...].T
    for g in range(n_fs):
        e_src[g] = jnp.broadcast_to(e_rows[g : g + 1, :], e_src.shape[1:])
    for g in order[1:]:
        rcopy(e_src.at[g], e_all.at[f], e_send, e_recv, (s, g, t)).start()
    for c in (1, 2):
        took(slot(c, s, f), w_in.at[c, 0])
        took(srcs[c], w_in.at[c, 1])
        spread(c)
    e_all[f] = e_src[f]
    for g in order[1:]:
        came(slot(0, s, g), w_recv.at[s, g])
        both(s, g)
    gd = gmap.shape[1]
    for i in range(width // gd):
        at = slice(i * gd, (i + 1) * gd)
        scaled = (gmap[t * (width // gd) + i].astype(F32) * pgain[:, at]).astype(BF)
        ow_buf[s, 1, at, :] = jnp.dot(scaled, wop[at, :], preferred_element_type=F32).astype(BF)
    norm(0)
    relay(0, 1, order[:2])
    for g, h, onto in ((px, 0, py), (py, 1, px)):
        here = landed(g, h)
        rcopy(here, here, x_send, x_recv.at[g, h], (s, onto, t)).start()
        hand_on(g, h)
    relay(0, 1, order[2:])
    for d in range(2, n_sp - 1):
        relay(0, d, order[:2])
    for g, h in ((px, 1), (py, 0)):
        landed(g, h)
        hand_on(g, h)
    norm(1)
    for d in range(2, n_sp - 1):
        relay(0, d, order[2:])
    own_block(1)
    pl.when(is_end)(lambda: own_block(2))
    norm(2)
    for d in range(1, n_sp - 1):
        arrive(0, d)
    main(0, 0)
    for h in range(2):
        landed(pd, h)
        hand_on(pd, h)
    norm(3)
    main(0, 1)
    relay(1, 1)

    reach = rim.shape[1]
    edge = rcopy(rim_src, rim, g_send, g_recv, up)

    def send_rim():
        for j in range(n_fs):
            rim_src[j] = acc1[j // 2, (j % 2 + 1) * rows - reach : (j % 2 + 1) * rows, :].astype(BF)
        when(has_up, edge)

    last(0)
    came(e_all.at[0 : n_fs - 1], e_recv)

    mine = pl.ds(pl.multiple_of(f * ch, ch), ch)
    gap_f = gap[:, mine]
    gain_f = rec_gain[:, mine]
    at = lax.broadcasted_iota(jnp.int32, (size, size), 0)
    causal = at >= lax.broadcasted_iota(jnp.int32, (size, size), 1)
    lower = jnp.where(causal, 1.0, 0.0).astype(BF)
    lower = jnp.concatenate([lower, lower], axis=1)

    def scan(j):
        p, base = j // 2, j % 2 * rows
        state = None
        so_far = jnp.zeros((1, ch), F32)
        e_cols = e_all[order[j]].T
        for n in range(rows // size):
            here = slice(n * size, (n + 1) * size)
            there = slice(base + n * size, base + (n + 1) * size)
            v = acc0[p, there, 2 * ch : 3 * ch].astype(BF)
            q = jax.nn.silu(acc0[p, there, 0:ch].astype(BF).astype(F32))
            k = gap_f * jax.nn.sigmoid(-acc0[p, there, ch : 2 * ch].astype(BF).astype(F32))
            logs = jnp.log1p(-k) + e_cols[here, 0:1]
            high = logs.astype(BF)
            low = (logs - high.astype(F32)).astype(BF)
            within = mm(lower, jnp.concatenate([high, low], axis=0), NN)
            mid = within[size // 2 - 1 : size // 2]
            end = within[size - 1 :]
            q = q * jnp.exp(within - mid)
            k = (k * jnp.exp(mid - within)).astype(BF)
            q_up = q.astype(BF)
            scores = jnp.where(causal, mm(q_up, k, NT), 0.0).astype(BF)
            out = mm(scores, v, NN)
            if n:
                out = out + mm(q_up, (state * jnp.exp(mid)).astype(BF), NT)
            local[j, here, :] = out
            qd[j, here, :] = (q * jnp.exp(mid + so_far)).astype(BF)
            fresh = mm(v, k, TN) * jnp.exp(end - mid)
            state = state * jnp.exp(end) + fresh if n else fresh
            so_far = so_far + end
        own_st[j] = state
        own_de[j] = jnp.broadcast_to(jnp.exp(so_far), own_de.shape[1:])

    def carry(g):
        return rcopy(t_out.at[g], t_in.at[g], t_send, t_recv.at[g], up)

    for j in range(n_fs):
        scan(j)

        @pl.when(jnp.logical_not(has_down))
        def _():
            t_in[j] = jnp.zeros(t_in.shape[1:], BF)
            t_out[j] = own_st[j].astype(BF)
            carry(j).start()

    for d in range(2, n_sp - 1):
        relay(1, d)
    pl.when(jnp.logical_not(is_end))(lambda: own_block(2))
    @pl.when(jnp.logical_not(is_end))
    def _():
        each_pair(lambda p: gemm(1, p, slice(0, total_k), False))
        send_rim()

    relay(2, 1)
    def chain():
        for g in range(n_fs):
            carry(g).wait_recv()
            t_out[g] = (own_st[g] + t_in[g].astype(F32) * own_de[g, 0:1, :]).astype(BF)
            carry(g).start()

    group = (t * n_fs * ch + f * ch) // gd
    spot = s * rows + lax.broadcasted_iota(jnp.int32, (rows, ch), 0)
    window = 2
    for level in range(1, POOL_GROUPS):
        window = jnp.where(group == level, 2 ** (level + 1), window)
    share = 1.0 / jnp.minimum(spot + 1, window).astype(F32)

    def rows_of(g):
        return pl.ds(pl.multiple_of(g * rows, rows), rows)

    def pool(j):
        zp = acc1[j // 2, j % 2 * rows : (j % 2 + 1) * rows, :].astype(BF).astype(F32)
        running = jnp.concatenate([rim[j].astype(F32), zp], axis=0)
        total = None
        for level in range(POOL_GROUPS):
            stride = 2**level
            running = running[stride:] + running[:-stride]
            now = running[running.shape[0] - rows :]
            total = now if level == 0 else jnp.where(group == level, now, total)
        acts[1, t, f, rows_of(order[j]), :] = (total * share - zp).astype(BF)

    part_rows = n_fs * rows // 2
    quarter = part_rows // 2

    def a_slot(k, u, g, h, q=None):
        lo, n = (h * part_rows, part_rows) if q is None else (h * part_rows + q * quarter, quarter)
        return acts.at[k, u, g, lo : lo + n, :]

    def a_share(k, g, h):
        here = a_slot(k, t, g, h)
        rcopy(here, here, ad_send, ad_recv.at[k, h], other).start()

    def publish(k):
        for h in range(2):
            here = a_slot(k, t, f, h)
            for p in (px, py):
                rcopy(here, here, a_send, a_recv.at[k, f, h], (s, p, t)).start()
            a_share(k, f, h)

    def a_forward(k, h):
        for g, q, onto in ((px, 0, py), (py, 1, px)):
            came(a_slot(k, t, g, h), a_recv.at[k, g, h])
            here = a_slot(k, t, g, h, q)
            rcopy(here, here, a_send, a_recv.at[k, g, h], (s, onto, t)).start()
            a_share(k, g, h)

    def a_rest(k, h):
        came(a_slot(k, t, pd, h), a_recv.at[k, pd, h])
        a_share(k, pd, h)

    def a_other(k, h):
        came(acts.at[k, 1 - t, :, h * part_rows : (h + 1) * part_rows, :], ad_recv.at[k, h])

    def pool_all():
        pl.when(has_down)(edge.wait_recv)
        for j in range(n_fs):
            pool(j)
        publish(1)

    mid_low = jnp.logical_not(is_end) & low
    mid_high = jnp.logical_not(is_end) & jnp.logical_not(low)
    pl.when(mid_low)(chain)
    for d in range(2, n_sp - 1):
        relay(2, d)
    pl.when(jnp.logical_not(is_end))(lambda: each_pair(lambda p: gemm(2, p, slice(0, total_k), False)))
    pl.when(mid_high)(pool_all)
    pl.when(mid_high)(chain)
    when(has_up, ow_up(s, 1))
    when(has_down, ow_down(s, 1))
    for k in range(2):
        ow_share(s, k)
    ow_relay(1, 0)
    for d in range(1, n_sp - 1):
        arrive(1, d)
    pl.when(is_end)(lambda: each_pair(lambda p: gemm(1, p, near, False)))
    last(1)
    @pl.when(is_end)
    def _():
        send_rim()

        @pl.when(jnp.logical_not(has_down))
        def _():
            rim[...] = jnp.zeros(rim.shape, BF)

    pl.when(jnp.logical_not(mid_high))(pool_all)
    ones = jnp.ones((8, ch), BF)

    def finish(j):
        g = order[j]
        rec = local[j] + mm(qd[j], t_in[j], NT)
        sums = mm(ones, (rec * rec).astype(BF), NT)
        for i in range(lanes):
            sq_src[pl.ds(g * lanes + i, 1), :] = sums[0:1, i * 128 : (i + 1) * 128]
        gate = jax.nn.silu(acc2[j // 2, j % 2 * rows : (j % 2 + 1) * rows, :].astype(BF).astype(F32))
        acts[0, t, f, rows_of(g), :] = (rec * gain_f * gate).astype(BF)

    def finish_all():
        for j in range(n_fs):
            finish(j)
        for u, g in [(1 - t, f)] + [(u, g) for g in order[1:] for u in (t, 1 - t)]:
            rcopy(sq_src, sq_all.at[t * n_fs + f], q_send, q_recv, (s, g, u)).start()
        publish(0)
        sq_all[t * n_fs + f] = sq_src[...]

    pl.when(jnp.logical_not(is_end))(finish_all)
    for d in range(1, n_sp - 1):
        arrive(2, d)
    pl.when(is_end)(lambda: each_pair(lambda p: gemm(2, p, near, False)))
    a_forward(1, 0)
    ow_relay(1, 1)
    a_forward(1, 1)
    last(2)
    @pl.when(has_down & jnp.logical_not(has_up))
    def _():
        for g in range(n_fs):
            carry(g).wait_recv()

    pl.when(is_end)(finish_all)
    for d in range(2, n_sp - 1):
        ow_relay(d, 0)
    for h in range(2):
        a_rest(1, h)
    for d in range(2, n_sp - 1):
        ow_relay(d, 1)
    a_forward(0, 0)
    a_forward(0, 1)
    for d in range(1, n_sp - 1):
        for k in range(2):
            ow_take(d, k)
    came(sq_all.at[0 : n_tp * n_fs - 1], q_recv)
    sums = sum(sq_all[i] for i in range(n_tp * n_fs))
    scale = lax.rsqrt(sums / (n_tp * width) + EPS).T
    half_lanes = n_fs * lanes // 2
    scales = [
        jnp.concatenate([scale[:, h * half_lanes + i : h * half_lanes + i + 1] for i in range(half_lanes)], axis=0)
        for h in range(2)
    ]
    late = s - t * n_half >= n_half - 1

    def spot_of(a, g):
        return pl.ds(pl.multiple_of((a * n_fs + g) * cw, cw), cw)

    def at_part(i, g, u):
        return (i * n_fs + g) * n_tp + u

    def piece(i, g, u):
        return rcopy(part.at[at_part(i, g, u)], final.at[:, spot_of(t * n_half + i, f)], m_send, m_recv, (s, g, u))

    def weight_side(k, a, i, h):
        here = slice(h * part_rows, (h + 1) * part_rows)
        total = None
        for u, w in ((t, ow_buf.at[a, k]), (1 - t, ow_oth.at[i, k])):
            left = jnp.concatenate([acts[k, u, b, here, :] for b in range(n_fs)], axis=1)
            now = jnp.dot(left, w[...], preferred_element_type=F32)
            total = now if total is None else total + now
        return total

    def rec_side(a, i, h):
        half_way[h] = weight_side(0, a, i, h) * scales[h]

    def pool_side(a, i, h):
        mixed = (half_way[h] + weight_side(1, a, i, h)).astype(BF)
        for g in range(h * n_fs // 2, (h + 1) * n_fs // 2):
            for u in range(n_tp):
                lo = (g * n_tp + u) * out_rows - h * part_rows
                part[at_part(i, g, u)] = mixed[lo : lo + out_rows]
                when((g != f) | (u != t), piece(i, g, u))

    def ow_got(j, k):
        i = jnp.where(late, n_half - 1 - j, j)
        if j == n_half - 1:
            ow_take(n_sp - 1, k)
        came(ow_oth.at[i, k], od_recv.at[i, k])
        return t * n_half + i, i

    for j in range(n_half):
        if j == 0:
            for k in range(2):
                a, i = ow_got(0, k)
            for h in range(2):
                a_rest(0, h)
                for k in range(2):
                    a_other(k, h)
                rec_side(a, i, h)
                pool_side(a, i, h)
        else:
            a, i = ow_got(j, 0)
            for h in range(2):
                rec_side(a, i, h)
            a, i = ow_got(j, 1)
            for h in range(2):
                pool_side(a, i, h)
        final[:, spot_of(a, f)] = part[at_part(i, f, t)]

    pieces = part.at[0 : n_half * (n_tp * n_fs - 1)]
    came(pieces, m_recv)
    sent(pieces, m_send)
    sent(xs.at[0:3, :, 0:half], x_send)
    sent(xs.at[:, :, 0:half], xd_send)
    sent(e_src.at[0 : n_fs - 1], e_send)
    for c in range(3):
        sent(srcs[c], w_send.at[c])
    sent(acts.at[:, 0, 0:3], a_send)
    sent(acts.at[:, 0], ad_send)
    sent(sq_all.at[0 : n_tp * n_fs - 1], q_send)
    sent(ow_oth, od_send)
    for v in range(n_sp):
        @pl.when(s == v)
        def _():
            if v < n_sp - 1:
                for c in range(3):
                    sent(wss[c].at[0 : (v + 1) * blk, :], up_send.at[c])
                sent(ow_buf.at[0 : v + 1], ou_send)
                sent(rim_src, g_send)
                sent(t_out, t_send)
            if v > 0:
                for c in range(3):
                    sent(wss[c].at[0 : (n_sp - v) * blk, :], dn_send.at[c])
                sent(ow_buf.at[0 : n_sp - v], on_send)


def fused(
    n_sp, n_fs, n_tp, tokens, norm_gain, w_query, forget_weight, w_input, w_outgate, w_pool, forget_gap,
    extra_decay, rec_gain, group_weight, pool_gain, recurrent_output_weight, w_out_pool,
):
    rows, half = tokens.shape[1:]
    wr, width = w_query.shape
    ch = width // n_fs
    cw = w_out_pool.shape[1]
    n_half = n_sp // n_tp
    feats = n_sp * n_fs * wr
    lanes = rows // 128

    def buf(kind, *shape):
        return pltpu.VMEM(shape, kind)

    args = (
        tokens[0], w_query, forget_weight, w_input, w_outgate, w_pool, extra_decay[0], norm_gain[None],
        forget_gap[None], rec_gain[None], group_weight, pool_gain[None], recurrent_output_weight, w_out_pool,
    )
    extra, gain, gap, r_gain, gmap, pgain = args[6:12]
    (final,) = comm(
        functools.partial(layer_kernel, n_sp, n_fs, n_tp),
        [((rows // n_tp, n_sp * n_fs * cw), BF)],
        [
            buf(BF, n_fs - 1, wr, 3 * ch), buf(BF, n_fs - 1, wr, ch), buf(BF, n_fs - 1, wr, ch),
            buf(BF, feats, 3 * ch), buf(BF, feats, ch), buf(BF, feats, ch),
            buf(BF, n_fs, rows, n_tp * half), buf(BF, 2, n_fs // 2 * rows, n_tp * half),
            buf(F32, 2, n_fs // 2 * rows, 3 * ch), buf(F32, 2, n_fs // 2 * rows, ch), buf(F32, 2, n_fs // 2 * rows, ch),
            buf(F32, n_fs, 8, rows), buf(F32, n_fs, 8, rows),
            buf(F32, n_fs, rows, ch), buf(BF, n_fs, rows, ch),
            buf(F32, n_fs, ch, ch), buf(F32, n_fs, 8, ch),
            buf(BF, n_fs, ch, ch), buf(BF, n_fs, ch, ch),
            buf(BF, n_fs, 2**POOL_GROUPS, ch), buf(BF, n_fs, 2**POOL_GROUPS, ch),
            buf(BF, 2, n_tp, n_fs, n_fs * rows, ch),
            buf(F32, n_fs * lanes, 128), buf(F32, n_tp * n_fs, n_fs * lanes, 128),
            buf(BF, n_sp, 2, width, cw), buf(BF, n_half, 2, width, cw),
            buf(BF, n_half * n_fs * n_tp, rows // n_tp, cw), buf(F32, 2, n_fs // 2 * rows, cw),
        ]
        + [buf(a.dtype, *a.shape) for a in (extra, gain, gap, r_gain, gmap, pgain, w_out_pool)]
        + [
            dma(2), dma(3, 2), dma(7), dma(), dma(n_fs, 2), dma(), dma(n_fs),
            dma(3), dma(n_sp, n_fs), dma(2, n_sp), dma(2), dma(3), dma(3), dma(), dma(),
            dma(), dma(n_fs), dma(), dma(), dma(), dma(2, n_fs, 2), dma(), dma(2, 2), dma(), dma(),
            dma(), dma(), dma(n_sp, 2), dma(), dma(n_half, 2), dma(), dma(),
        ],
        1, "layer", [pl.BlockSpec(memory_space=pl.ANY)] * len(args),
    )(*args)
    return final[None]


def run(n_sp, n_fs, n_tp, *args):
    wr, width = args[2].shape
    whole = n_fs * wr % 128 == 0 and args[-1].shape[1] % 128 == 0 and args[0].shape[1] % 256 == 0
    return (fused if whole and width == n_fs * HEAD_DIM else body)(n_sp, n_fs, n_tp, *args)


def solution(mesh):
    sizes = dict(mesh.shape)
    weight = P(("sp", "fs"), "tp")
    placed = (
        P("fs", "sp", "tp"), P(), weight, weight, weight, weight, weight, P("tp"),
        P("fs", "sp", "tp"), P("tp"), P(), P("tp"), P("tp", ("sp", "fs")), P("tp", ("sp", "fs")),
    )
    return jax.shard_map(
        functools.partial(run, sizes["sp"], sizes["fs"], sizes["tp"]),
        mesh=mesh, in_specs=placed, out_specs=P("fs", ("sp", "tp"), None), check_vma=False,
    )
```

```python
import functools
import jax
import jax.numpy as jnp
from jax import lax
from jax.experimental import pallas as pl
from jax.experimental.pallas import tpu as pltpu
from jax.sharding import PartitionSpec as P

HEAD_DIM = 128
POOL_GROUPS = 4
BLOCK = 64
EPS = 1e-06
HIGH = lax.Precision.HIGHEST
MESH = pl.DeviceIdType.MESH
BF = jnp.bfloat16
F32 = jnp.float32


def place():
    return lax.axis_index("sp"), lax.axis_index("fs"), lax.axis_index("tp")


def rcopy(src, dst, ssem, rsem, dev):
    return pltpu.make_async_remote_copy(
        src_ref=src, dst_ref=dst, send_sem=ssem, recv_sem=rsem, device_id=dev, device_id_type=MESH
    )


def greet(devs):
    barrier = pltpu.get_barrier_semaphore()
    for cond, dev in devs:
        def tell(dev=dev):
            pl.semaphore_signal(barrier, inc=1, device_id=dev, device_id_type=MESH)
        if cond is None:
            tell()
        else:
            pl.when(cond)(tell)
    pl.semaphore_wait(barrier, sum(1 if cond is None else jnp.where(cond, 1, 0) for cond, _ in devs))


def square(f):
    near = f + 1 - 2 * lax.rem(f, 2)
    return near, lax.rem(f + 2, 4), lax.rem(near + 2, 4)


def project_kernel(
    n_sp, n_fs, n_tp, tok, wq, wf, wi, wo, wp, extra, gain, gmap, pgain, wor, wop, z_ref, e_ref, ow_ref,
    wsrc, xs, ws, acc, x_send, x_recv, f_send, d_send, d_recv, w_send, w_recv, zr_send, zl_send, e_send, e_recv,
):
    s, f, t = place()
    rows, half = tok.shape
    part = rows // 2
    mats = (wq, wf, wi, wo, wp)
    wr, width = wq.shape
    ch = width // n_fs
    for i, w in enumerate(mats):
        for g in range(n_fs):
            wsrc[g, :, i * ch : (i + 1) * ch] = w[:, g * ch : (g + 1) * ch]
    other = (s, f, 1 - t)
    px, py, pd = square(f)
    order = (f, px, py, pd)
    up, down = (s + 1, f, t), (s - 1, f, t)
    has_up, has_down = s < n_sp - 1, s > 0
    greet([(None, other)] + [(None, (s, g, t)) for g in order[1:]] + [(has_up, up), (has_down, down)])

    def cols(c):
        return pl.ds(pl.multiple_of(c * half, half), half)

    def span(a, b):
        return pl.ds(pl.multiple_of((a * n_fs + b) * wr, wr), wr)

    def slot(a, b):
        return ws.at[span(a, b), :]

    def to_up(src, a, b):
        return rcopy(src, slot(a, b), zr_send.at[a, b], w_recv.at[a, b], up)

    def to_down(src, a, b):
        return rcopy(src, slot(a, b), zl_send.at[a, b], w_recv.at[a, b], down)

    sends = []

    def send(c):
        c.start()
        sends.append(c)

    def x_slot(g, h, c):
        return xs.at[g, h * part : (h + 1) * part, cols(c)]

    own = wsrc.at[f]
    pl.when(has_up)(lambda: to_up(own, s, f).start())
    pl.when(has_down)(lambda: to_down(own, s, f).start())
    for i, g in enumerate((pd, px, py)):
        send(rcopy(wsrc.at[g], slot(s, f), w_send.at[i], w_recv.at[s, f], (s, g, t)))
    for i, (p, hs) in enumerate(((px, (0, 1)), (py, (1, 0)))):
        for h in hs:
            send(rcopy(tok.at[h * part : (h + 1) * part, :], x_slot(f, h, t), x_send.at[i, h], x_recv.at[f, h], (s, p, t)))
    for h in range(2):
        send(rcopy(tok.at[h * part : (h + 1) * part, :], x_slot(f, h, t), d_send.at[f, h], d_recv.at[f, h], other))
    for i, g in enumerate(order[1:]):
        send(rcopy(extra.at[g], e_ref.at[f], e_send.at[i], e_recv.at[f], (s, g, t)))
    ws[span(s, f), :] = wsrc[f]
    xs[f, :, cols(t)] = tok[...]
    e_ref[f] = extra[f]
    ow_ref[0:width, :] = wor[...]
    gd = gmap.shape[1]
    for i in range(width // gd):
        at = slice(i * gd, (i + 1) * gd)
        scaled = (gmap[t * (width // gd) + i].astype(F32) * pgain[:, at]).astype(BF)
        folded = jnp.dot(scaled, wop[at, :], preferred_element_type=F32)
        ow_ref[width + i * gd : width + (i + 1) * gd, :] = folded.astype(BF)

    for g in order[1:]:
        to_up(slot(s, g), s, g).wait_recv()
        pl.when(has_up)(lambda: to_up(slot(s, g), s, g).start())
        pl.when(has_down)(lambda: to_down(slot(s, g), s, g).start())

    def landed(g, h):
        here = x_slot(g, h, t)
        rcopy(here, here, d_send.at[g, h], x_recv.at[g, h], other).wait_recv()
        return here

    def hand_on(g, h, here):
        send(rcopy(here, here, d_send.at[g, h], d_recv.at[g, h], other))

    for i, (g, h, onto) in enumerate(((px, 0, py), (py, 1, px))):
        here = landed(g, h)
        send(rcopy(here, here, f_send.at[i], x_recv.at[g, h], (s, onto, t)))
        hand_on(g, h, here)

    def relay(d):
        for g in order:
            a = s - d

            @pl.when(a >= 0)
            def _():
                to_up(slot(a, g), a, g).wait_recv()
                pl.when(has_up)(lambda: to_up(slot(a, g), a, g).start())
            b = s + d

            @pl.when(b < n_sp)
            def _():
                to_down(slot(b, g), b, g).wait_recv()
                pl.when(has_down)(lambda: to_down(slot(b, g), b, g).start())

    def add(a):
        k = pl.ds(pl.multiple_of(a * n_fs * wr, n_fs * wr), n_fs * wr)

        def each(i, _):
            acc[i] += jnp.dot(xs[i, :, k], ws[k, :], preferred_element_type=F32)
            return 0

        lax.fori_loop(0, n_fs, each, 0)

    def multiply(d):
        pl.when(s - d >= 0)(lambda: add(s - d))
        pl.when(s + d < n_sp)(lambda: add(s + d))

    relay(1)
    for g, h in ((px, 1), (py, 0), (pd, 0), (pd, 1)):
        hand_on(g, h, landed(g, h))
    for d in range(2, n_sp - 1):
        relay(d)
    for g in order:
        for h in range(2):
            here = x_slot(g, h, 1 - t)
            rcopy(here, here, d_send.at[g, h], d_recv.at[g, h], other).wait_recv()
    for g in order[1:]:
        rcopy(extra.at[f], e_ref.at[g], e_send.at[0], e_recv.at[g], other).wait_recv()
    for c in sends:
        c.wait_send()

    def norm(j, _):
        tile = 16
        per = rows // tile
        at = (j // per, pl.ds(pl.multiple_of(lax.rem(j, per) * tile, tile), tile))
        feats = xs[at[0], at[1], :].astype(F32)
        scale = lax.rsqrt(jnp.mean(feats * feats, axis=-1, keepdims=True) + EPS)
        xs[at[0], at[1], :] = (feats * scale * gain[...]).astype(BF)
        return 0

    lax.fori_loop(0, n_fs * rows // 16, norm, 0, unroll=2)

    if n_fs * wr % 128 == 0:
        own_k = pl.ds(pl.multiple_of(s * n_fs * wr, n_fs * wr), n_fs * wr)

        def begin(i, _):
            acc[i] = jnp.dot(xs[i, :, own_k], ws[own_k, :], preferred_element_type=F32)
            return 0

        lax.fori_loop(0, n_fs, begin, 0)
        for d in range(1, n_sp - 1):
            multiply(d)
        relay(n_sp - 1)
        multiply(n_sp - 1)

        def finish(i, _):
            z_ref[i] = acc[i].astype(BF)
            return 0
    else:
        relay(n_sp - 1)

        def finish(i, _):
            z_ref[i] = jnp.dot(xs[i], ws[...], preferred_element_type=F32).astype(BF)
            return 0

    lax.fori_loop(0, n_fs, finish, 0)

    for d in range(n_sp):
        for g in order:
            a = s - d

            @pl.when((a >= 0) & has_up)
            def _():
                to_up(slot(a, g), a, g).wait_send()
            b = s + d

            @pl.when((b < n_sp) & has_down)
            def _():
                to_down(slot(b, g), b, g).wait_send()


def dot(a, b, dims):
    return lax.dot_general(a, b, (dims, ((), ())), precision=HIGH, preferred_element_type=F32)


def state_kernel(
    n_sp, group_dim, z, e_all, gap, rec_gain, act, sq_out,
    local, qd, own_st, own_de, st_in, de_in, rim, s_send, s_recv, c_send, c_recv, g_send, g_recv,
):
    s, f, t = place()
    n_fs, rows, _ = z.shape
    ch = HEAD_DIM
    reach = rim.shape[1]
    devs = []
    for d in range(1, n_sp):
        devs.append((s + d < n_sp, (s + d, f, t)))
        devs.append((s - d >= 0, (s - d, f, t)))
    greet(devs)
    edge = rcopy(z.at[:, rows - reach :, 4 * ch :], rim, g_send, g_recv, (s + 1, f, t))
    pl.when(s < n_sp - 1)(edge.start)
    mine = pl.ds(pl.multiple_of(f * ch, ch), ch)
    gap_f = gap[:, mine]
    gain_f = rec_gain[:, mine]
    at = lax.broadcasted_iota(jnp.int32, (BLOCK, BLOCK), 0)
    causal = at >= lax.broadcasted_iota(jnp.int32, (BLOCK, BLOCK), 1)
    lower = causal.astype(F32)

    def one(g, _):
        state = jnp.zeros((ch, ch), F32)
        so_far = jnp.zeros((1, ch), F32)
        e_cols = e_all[g].T
        for n in range(rows // BLOCK):
            here = slice(n * BLOCK, (n + 1) * BLOCK)
            q, fo, v = (z[g, here, i * ch : (i + 1) * ch].astype(F32) for i in range(3))
            q = jax.nn.silu(q)
            k = gap_f * jax.nn.sigmoid(-fo)
            lo = n * BLOCK % 128
            lane = n * BLOCK // 128
            logs = jnp.log1p(-k) + e_cols[lo : lo + BLOCK, lane : lane + 1]
            within = dot(lower, logs, ((1,), (0,)))
            end = within[BLOCK - 1 :]
            q_up = q * jnp.exp(within)
            scores = jnp.where(causal, dot(q_up, k * jnp.exp(-within), ((1,), (1,))), 0.0)
            out = dot(scores, v, ((1,), (0,)))
            if n:
                out = out + dot(q_up, state, ((1,), (1,)))
            local[g, here, :] = out
            qd[g, here, :] = q_up * jnp.exp(so_far)
            state = state * jnp.exp(end) + dot(v.T, k * jnp.exp(end - within), ((1,), (0,)))
            so_far = so_far + end
        own_st[g] = state.astype(BF)
        own_de[g] = jnp.broadcast_to(jnp.exp(so_far), (8, ch))
        return 0

    lax.fori_loop(0, n_fs, one, 0)

    def pair(d):
        dev = (s + d, f, t)
        return (
            rcopy(own_st, st_in.at[d - 1], s_send.at[d - 1], s_recv.at[d - 1], dev),
            rcopy(own_de, de_in.at[d - 1], c_send.at[d - 1], c_recv.at[d - 1], dev),
        )

    for d in range(1, n_sp):
        @pl.when(s + d < n_sp)
        def _():
            for c in pair(d):
                c.start()

        @pl.when(s - d < 0)
        def _():
            st_in[d - 1] = jnp.zeros(st_in.shape[1:], st_in.dtype)
            de_in[d - 1] = jnp.ones(de_in.shape[1:], de_in.dtype)
    pl.when(s == 0)(lambda: rim.__setitem__(Ellipsis, jnp.zeros(rim.shape, rim.dtype)))
    pl.when(s > 0)(edge.wait_recv)
    group = (t * n_fs * ch + f * ch) // group_dim
    spot = s * rows + lax.broadcasted_iota(jnp.int32, (rows, ch), 0)
    window = 2
    for level in range(1, POOL_GROUPS):
        window = jnp.where(group == level, 2 ** (level + 1), window)
    counts = jnp.minimum(spot + 1, window).astype(F32)
    for g in range(n_fs):
        zp = z[g, :, 4 * ch :].astype(F32)
        running = jnp.concatenate([rim[g].astype(F32), zp], axis=0)
        total = None
        for level in range(POOL_GROUPS):
            stride = 2**level
            running = running[stride:] + running[:-stride]
            now = running[running.shape[0] - rows :]
            total = now if level == 0 else jnp.where(group == level, now, total)
        act[1, g * rows : (g + 1) * rows, :] = (total / counts - zp).astype(BF)
    for d in range(1, n_sp):
        @pl.when(s - d >= 0)
        def _():
            for c in pair(d):
                c.wait_recv()

    ones = jnp.ones((8, ch), F32)

    def finish(g, _):
        total = jnp.zeros((ch, ch), F32)
        for d in range(n_sp - 2, -1, -1):
            total = de_in[d, g, 0:1, :] * total + st_in[d, g].astype(F32)
        rec = local[g] + dot(qd[g], total, ((1,), (1,)))
        sums = dot(ones, rec * rec, ((1,), (1,)))
        for i in range(rows // 128):
            sq_out[g, i : i + 1, :] = sums[0:1, i * 128 : (i + 1) * 128]
        gate = jax.nn.silu(z[g, :, 3 * ch : 4 * ch].astype(F32))
        act[0, pl.ds(pl.multiple_of(g * rows, rows), rows), :] = (rec * gain_f * gate).astype(BF)
        return 0

    sq_out[...] = jnp.zeros(sq_out.shape, F32)
    lax.fori_loop(0, n_fs, finish, 0)
    for d in range(1, n_sp):
        @pl.when(s + d < n_sp)
        def _():
            for c in pair(d):
                c.wait_send()
    pl.when(s < n_sp - 1)(edge.wait_send)


def mix_kernel(
    n_sp, n_fs, n_tp, act, sq, ow, final,
    out, acts, sq_all, ow_all, relay_buf, wbuf, part,
    a_send, a_recv, f_send, d_send, d_recv, q_send, q_recv,
    up_send, down_send, o_recv, od_send, od_recv, m_send, m_recv,
):
    s, f, t = place()
    n_half = n_sp // n_tp
    rows = act.shape[1] // n_fs
    half = rows // n_tp
    width, cw = ow.shape[0] // 2, ow.shape[1]
    other = (s, f, 1 - t)
    px, py, pd = square(f)
    up, down = (s + 1, f, t), (s - 1, f, t)
    has_up, has_down = s < n_sp - 1, s > 0
    greet(
        [(None, other)]
        + [(None, (s, g, u)) for g in (px, py, pd) for u in (t, 1 - t)]
        + [(has_up, up), (has_down, down)]
    )

    def to_up(src, a):
        return rcopy(src, relay_buf.at[a], up_send.at[a], o_recv.at[a], up)

    def to_down(src, a):
        return rcopy(src, relay_buf.at[a], down_send.at[a], o_recv.at[a], down)

    def to_other(src, a):
        return rcopy(src, ow_all.at[lax.rem(a, n_half), t], od_send.at[a], od_recv.at[a], other)

    def keep(src, a):
        mine = a // n_half == t

        @pl.when(mine)
        def _():
            ow_all[lax.rem(a, n_half), t] = src[...]

        pl.when(jnp.logical_not(mine))(lambda: to_other(src, a).start())

    sends = []

    def send(c):
        c.start()
        sends.append(c)

    for i, (p, order) in enumerate(((px, (0, 1)), (py, (1, 0)))):
        for h in order:
            send(rcopy(act.at[h], acts.at[t, f, h], a_send.at[i, h], a_recv.at[f, h], (s, p, t)))
    pl.when(has_up)(lambda: to_up(ow, s).start())
    pl.when(has_down)(lambda: to_down(ow, s).start())
    for h in range(2):
        send(rcopy(act.at[h], acts.at[t, f, h], d_send.at[f, h], d_recv.at[f, h], other))
    for i, g in enumerate((px, py, pd)):
        for u in range(n_tp):
            send(rcopy(sq, sq_all.at[t, f], q_send.at[i, u], q_recv.at[t, f], (s, g, u)))
    send(rcopy(sq, sq_all.at[t, f], q_send.at[n_fs - 1, 0], q_recv.at[t, f], other))
    acts[t, f] = act[...]
    sq_all[t, f] = sq[...]
    keep(ow, s)

    def landed(g, h):
        here = acts.at[t, g, h]
        rcopy(here, here, d_send.at[g, h], a_recv.at[g, h], other).wait_recv()
        return here

    def hand_on(g, h, here):
        send(rcopy(here, here, d_send.at[g, h], d_recv.at[g, h], other))

    for i, (g, h, onto) in enumerate(((px, 0, py), (py, 1, px))):
        here = landed(g, h)
        send(rcopy(here, here, f_send.at[i], a_recv.at[g, h], (s, onto, t)))
        hand_on(g, h, here)

    def step(d):
        a = s - d

        @pl.when(a >= 0)
        def _():
            to_up(relay_buf.at[a], a).wait_recv()
            pl.when(has_up)(lambda: to_up(relay_buf.at[a], a).start())
            keep(relay_buf.at[a], a)
        b = s + d

        @pl.when(b < n_sp)
        def _():
            to_down(relay_buf.at[b], b).wait_recv()
            pl.when(has_down)(lambda: to_down(relay_buf.at[b], b).start())
            keep(relay_buf.at[b], b)

    for d in range(1, n_sp):
        step(d)
    for g, h in ((px, 1), (py, 0), (pd, 0), (pd, 1)):
        hand_on(g, h, landed(g, h))
    for i in range(n_half):
        a = t * n_half + i
        here = ow_all.at[i, 1 - t]
        rcopy(here, here, od_send.at[a], od_recv.at[a], other).wait_recv()
    for i in range(n_half):
        for u in range(n_tp):
            for k in range(2):
                wbuf[k, u * width : (u + 1) * width, i * cw : (i + 1) * cw] = ow_all[i, u, k * width : (k + 1) * width, :]
    for g in (px, py, pd):
        for u in range(n_tp):
            here = sq_all.at[u, g]
            rcopy(here, here, q_send.at[0, 0], q_recv.at[u, g], other).wait_recv()
    here = sq_all.at[1 - t, f]
    rcopy(here, here, q_send.at[0, 0], q_recv.at[1 - t, f], other).wait_recv()
    for g in (f, px, py, pd):
        for h in range(2):
            here = acts.at[1 - t, g, h]
            rcopy(here, here, d_send.at[g, h], d_recv.at[g, h], other).wait_recv()

    def piece(g, u):
        return rcopy(part.at[g, u], out.at[f, t], m_send.at[g, u], m_recv.at[f, t], (s, g, u))

    def spread(g):
        for u in range(n_tp):
            c = piece(g, u)
            c.start()
            sends.append(c)

    last = None
    for g in (pd, f, px, py):
        here = pl.ds(pl.multiple_of(g * rows, rows), rows)
        sums = sum(sq_all[u, i, g] for u in range(n_tp) for i in range(n_fs))
        scale = lax.rsqrt(sums / (n_tp * width) + EPS).T
        scale = jnp.concatenate([scale[:, i : i + 1] for i in range(rows // 128)], axis=0)
        left = [
            jnp.concatenate([acts[u, i, h, here, :] for u in range(n_tp) for i in range(n_fs)], axis=1)
            for h in range(2)
        ]
        mixed = (
            jnp.dot(left[0], wbuf[0], preferred_element_type=F32) * scale
            + jnp.dot(left[1], wbuf[1], preferred_element_type=F32)
        ).astype(BF)
        for u in range(n_tp):
            part[g, u] = mixed[u * half : (u + 1) * half]
        if last is not None and last is not f:
            spread(last)
        if last is f:
            c = piece(f, 1 - t)
            c.start()
            sends.append(c)
        last = g
    out[f, t] = part[f, t]
    for i in range(n_half):
        to_other(ow, (1 - t) * n_half + i).wait_send()
    for d in range(n_sp):
        a, b = s - d, s + d

        @pl.when((a >= 0) & has_up)
        def _():
            to_up(ow, a).wait_send()

        @pl.when((b < n_sp) & has_down)
        def _():
            to_down(ow, b).wait_send()
    spread(last)
    for c in sends:
        c.wait_send()
    for g in (px, py, pd):
        for u in range(n_tp):
            here = out.at[g, u]
            rcopy(here, here, m_send.at[g, u], m_recv.at[g, u], other).wait_recv()
    here = out.at[f, 1 - t]
    rcopy(here, here, m_send.at[f, 1 - t], m_recv.at[f, 1 - t], other).wait_recv()
    for u in range(n_tp):
        for i in range(n_half):
            for g in range(n_fs):
                lo = ((u * n_half + i) * n_fs + g) * cw
                final[:, lo : lo + cw] = out[g, u, :, i * cw : (i + 1) * cw]


def vmem(count):
    return [pl.BlockSpec(memory_space=pltpu.VMEM)] * count


def dma(*shape):
    return pltpu.SemaphoreType.DMA(shape) if shape else pltpu.SemaphoreType.DMA


def comm(kernel, outs, scratch, number, name, ins=None, limit=60):
    return pl.pallas_call(
        kernel,
        out_shape=[jax.ShapeDtypeStruct(a, b) if ins is None else pltpu.VMEM(a, b) for a, b in outs],
        **({"out_specs": vmem(len(outs))} if ins is None else {"in_specs": ins, "out_specs": [pl.BlockSpec(memory_space=pltpu.VMEM)] * len(outs)}),
        scratch_shapes=scratch,
        compiler_params=pltpu.CompilerParams(
            collective_id=number, has_side_effects=True, vmem_limit_bytes=limit * 1024 * 1024
        ),
        name=name,
    )


def body(
    n_sp, n_fs, n_tp, tokens, norm_gain, w_query, forget_weight, w_input, w_outgate, w_pool, forget_gap,
    extra_decay, rec_gain, group_weight, pool_gain, recurrent_output_weight, w_out_pool,
):
    s, f, t = place()
    rows, half = tokens.shape[1:]
    width = w_query.shape[1]
    ch = width // n_fs
    n_w = 5
    wr = w_query.shape[0]
    lanes = rows // 128
    extra = jnp.pad(extra_decay[0].T.reshape(n_fs, lanes, 128), ((0, 0), (0, 8 - lanes), (0, 0)))
    cw = w_out_pool.shape[1]
    z, e_all, ow = comm(
        functools.partial(project_kernel, n_sp, n_fs, n_tp),
        [((n_fs, rows, n_w * ch), BF), ((n_fs, 8, 128), F32), ((2 * width, cw), BF)],
        [
            pltpu.VMEM((n_fs, wr, n_w * ch), BF), pltpu.VMEM((n_fs, rows, n_tp * half), BF),
            pltpu.VMEM((n_sp * n_fs * wr, n_w * ch), BF), pltpu.VMEM((n_fs, rows, n_w * ch), F32),
            dma(2, 2), dma(n_fs, 2), dma(2), dma(n_fs, 2), dma(n_fs, 2), dma(n_fs - 1), dma(n_sp, n_fs),
            dma(n_sp, n_fs), dma(n_sp, n_fs), dma(n_fs - 1), dma(n_fs),
        ],
        1, "project",
    )(
        tokens[0], w_query, forget_weight, w_input, w_outgate, w_pool, extra, norm_gain[None],
        group_weight, pool_gain[None], recurrent_output_weight, w_out_pool,
    )
    n_half = n_sp // n_tp
    act, sq = comm(
        functools.partial(state_kernel, n_sp, group_weight.shape[1]),
        [((2, n_fs * rows, ch), BF), ((n_fs, 8, 128), F32)],
        [
            pltpu.VMEM((n_fs, rows, ch), F32), pltpu.VMEM((n_fs, rows, ch), F32),
            pltpu.VMEM((n_fs, ch, ch), BF), pltpu.VMEM((n_fs, 8, ch), F32),
            pltpu.VMEM((n_sp - 1, n_fs, ch, ch), BF), pltpu.VMEM((n_sp - 1, n_fs, 8, ch), F32),
            pltpu.VMEM((n_fs, 2**POOL_GROUPS, ch), BF),
            dma(n_sp - 1), dma(n_sp - 1), dma(n_sp - 1), dma(n_sp - 1), dma(), dma(),
        ],
        2, "state",
    )(z, e_all, forget_gap[None], rec_gain[None])
    out_shape = (n_fs, n_tp, rows // n_tp, n_half * cw)
    (final,) = comm(
        functools.partial(mix_kernel, n_sp, n_fs, n_tp),
        [((rows // n_tp, n_tp * n_half * n_fs * cw), BF)],
        [
            pltpu.VMEM(out_shape, BF), pltpu.VMEM((n_tp, n_fs) + act.shape, BF), pltpu.VMEM((n_tp, n_fs) + sq.shape, F32),
            pltpu.VMEM((n_half, n_tp) + ow.shape, BF), pltpu.VMEM((n_sp,) + ow.shape, BF),
            pltpu.VMEM((2, n_tp * width, n_half * cw), BF), pltpu.VMEM(out_shape, BF),
            dma(2, 2), dma(n_fs, 2), dma(2), dma(n_fs, 2), dma(n_fs, 2), dma(n_fs, n_tp), dma(n_tp, n_fs),
            dma(n_sp), dma(n_sp), dma(n_sp), dma(n_sp), dma(n_sp), dma(n_fs, n_tp), dma(n_fs, n_tp),
        ],
        3, "mix",
    )(act, sq, ow)
    return final[None]


def mm(a, b, dims):
    return lax.dot_general(a, b, (dims, ((), ())), preferred_element_type=F32)


NN, NT, TN = ((1,), (0,)), ((1,), (1,)), ((0,), (0,))


def layer_kernel(
    n_sp, n_fs, n_tp, tok, wq, wf, wi, wo, wp, extra_in, gain_in, gap_in, rec_gain_in, gmap_in, pgain_in, wor, wop_in, final,
    src0, src1, src2, ws0, ws1, ws2, xs, xn, acc0, acc1, acc2, e_src, e_all, local, qd, own_st, own_de,
    t_out, t_in, rim_src, rim, acts, sq_src, sq_all, ow_buf, ow_oth, part, half_way,
    extra, gain, gap, rec_gain, gmap, pgain, wop,
    in_sem, w_in, p_in, x_send, x_recv, xd_send, xd_recv, w_send, w_recv, b_recv, ba_recv, up_send, dn_send, e_send, e_recv,
    t_send, t_recv, g_send, g_recv, a_send, a_recv, ad_send, ad_recv, q_send, q_recv,
    ou_send, on_send, o_recv, od_send, od_recv, m_send, m_recv,
):
    s, f, t = place()
    rows, half = tok.shape
    cut = rows // 2
    wr, width = wq.shape
    ch = width // n_fs
    cw = wor.shape[1]
    n_half = n_sp // n_tp
    out_rows = rows // n_tp
    lanes = rows // 128
    size = 128
    blk = n_fs * wr
    total_k = n_sp * blk
    groups = ((wq, wf, wi), (wp,), (wo,))
    srcs, wss, accs = (src0, src1, src2), (ws0, ws1, ws2), (acc0, acc1, acc2)
    other = (s, f, 1 - t)
    px, py, pd = square(f)
    order = (f, px, py, pd)
    up, down = (s + 1, f, t), (s - 1, f, t)
    has_up, has_down = s < n_sp - 1, s > 0
    is_end = jnp.logical_not(has_up & has_down)

    def when(cond, *copies):
        @pl.when(cond)
        def _():
            for c in copies:
                c.start()

    def sent(ref, sem):
        rcopy(ref, ref, sem, sem, other).wait_send()

    def came(ref, sem):
        rcopy(ref, ref, sem, sem, other).wait_recv()

    def cols(c):
        return pl.ds(pl.multiple_of(c * half, half), half)

    def span(a, b):
        return pl.ds(pl.multiple_of((a * n_fs + b) * wr, wr), wr)

    def slot(c, a, b):
        return wss[c].at[span(a, b), :]

    def block(c, a):
        return wss[c].at[pl.ds(pl.multiple_of(a * blk, blk), blk), :]

    def x_slot(g, h, c):
        return xs.at[g, h * cut : (h + 1) * cut, cols(c)]

    peers = (
        [(None, other)]
        + [(None, (s, g, u)) for g in order[1:] for u in (t, 1 - t)]
        + [(has_up, up), (has_down, down)]
    )
    barrier = pltpu.get_barrier_semaphore()
    for cond, dev in peers:
        def tell(dev=dev):
            pl.semaphore_signal(barrier, inc=1, device_id=dev, device_id_type=MESH)
        if cond is None:
            tell()
        else:
            pl.when(cond)(tell)
    for c in range(3):
        for i, w in enumerate(groups[c]):
            for j, g in enumerate(order):
                lane = pl.ds(pl.multiple_of(g * ch, ch), ch)
                into = wss[c].at[span(s, f), i * ch : (i + 1) * ch] if j == 0 else srcs[c].at[j - 1, :, i * ch : (i + 1) * ch]
                pltpu.make_async_copy(w.at[:, lane], into, w_in.at[c, min(j, 1)]).start()
        if c == 0:
            pltpu.make_async_copy(tok, xs.at[f, :, cols(t)], in_sem.at[0]).start()
            pltpu.make_async_copy(wor, ow_buf.at[s, 0], in_sem.at[1]).start()
    params = ((extra_in, extra), (gain_in, gain), (gmap_in, gmap), (pgain_in, pgain), (wop_in, wop), (gap_in, gap), (rec_gain_in, rec_gain))
    loads = [pltpu.make_async_copy(a, b, p_in.at[i]) for i, (a, b) in enumerate(params)]
    for c in loads:
        c.start()
    pl.semaphore_wait(barrier, sum(1 if cond is None else jnp.where(cond, 1, 0) for cond, _ in peers))

    def took(ref, sem):
        pltpu.make_async_copy(ref, ref, sem).wait()

    def to_up(src, b, a):
        return rcopy(src, slot(0, a, b), up_send.at[0], w_recv.at[a, b], up)

    def to_down(src, b, a):
        return rcopy(src, slot(0, a, b), dn_send.at[0], w_recv.at[a, b], down)

    def both(a, b):
        when(has_up, to_up(slot(0, a, b), b, a))
        when(has_down, to_down(slot(0, a, b), b, a))

    def b_up(c, a):
        return rcopy(block(c, a), block(c, a), up_send.at[c], b_recv.at[c - 1, a], up)

    def b_down(c, a):
        return rcopy(block(c, a), block(c, a), dn_send.at[c], b_recv.at[c - 1, a], down)

    def spread(c):
        for j, g in enumerate(order[1:]):
            rsem = w_recv.at[s, f] if c == 0 else ba_recv.at[c - 1]
            rcopy(srcs[c].at[j], slot(c, s, f), w_send.at[c], rsem, (s, g, t)).start()

    def own_block(c):
        came(wss[c].at[0 : (n_fs - 1) * wr, :], ba_recv.at[c - 1])
        when(has_up, b_up(c, s))
        when(has_down, b_down(c, s))

    low = 2 * s < n_sp

    def relay(c, d, gs=(None,)):
        a, b = s - d, s + d

        def rising(extra):
            for g in gs:
                @pl.when((a >= 0) & has_up & extra)
                def _():
                    hop = to_up(slot(0, a, g), g, a) if c == 0 else b_up(c, a)
                    hop.wait_recv()
                    hop.start()

        def falling():
            for g in gs:
                @pl.when((b < n_sp) & has_down)
                def _():
                    hop = to_down(slot(0, b, g), g, b) if c == 0 else b_down(c, b)
                    hop.wait_recv()
                    hop.start()

        rising(low)
        falling()
        rising(jnp.logical_not(low))

    def arrive(c, d):
        for g in order if c == 0 else (None,):
            a, b = s - d, s + d

            @pl.when((a >= 0) & jnp.logical_not(has_up))
            def _():
                (to_up(slot(0, a, g), g, a) if c == 0 else b_up(c, a)).wait_recv()

            @pl.when((b < n_sp) & jnp.logical_not(has_down))
            def _():
                (to_down(slot(0, b, g), g, b) if c == 0 else b_down(c, b)).wait_recv()

    near = pl.ds(pl.multiple_of(jnp.where(has_down, blk, 0), blk), total_k - blk)
    far = pl.ds(pl.multiple_of(jnp.where(has_down, 0, total_k - blk), blk), blk)

    def gemm(c, p, k, more):
        out = jnp.dot(xn[p, :, k], wss[c][k, :], preferred_element_type=F32)
        accs[c][p] = accs[c][p] + out if more else out

    def main(c, p):
        pl.when(is_end)(lambda: gemm(c, p, near, False))
        pl.when(jnp.logical_not(is_end))(lambda: gemm(c, p, slice(0, total_k), False))

    def each_pair(step):
        def one(p, _):
            step(p)
            return 0

        lax.fori_loop(0, 2, one, 0)

    def last(c):
        arrive(c, n_sp - 1)
        pl.when(is_end)(lambda: each_pair(lambda p: gemm(c, p, far, True)))

    def landed(g, h):
        here = x_slot(g, h, t)
        came(here, x_recv.at[g, h])
        return here

    def hand_on(g, h):
        here = x_slot(g, h, t)
        rcopy(here, here, xd_send, xd_recv.at[g], other).start()

    def norm(j):
        g = order[j]
        came(xs.at[g, :, cols(1 - t)], xd_recv.at[g])
        tile = 16

        def each(i, _):
            at = pl.ds(pl.multiple_of(i * tile, tile), tile)
            feats = xs[g, at, :].astype(F32)
            scale = lax.rsqrt(jnp.mean(feats * feats, axis=-1, keepdims=True) + EPS)
            to = pl.ds(pl.multiple_of((j % 2) * rows + i * tile, tile), tile)
            xn[j // 2, to, :] = (feats * scale * gain[...]).astype(BF)
            return 0

        lax.fori_loop(0, rows // tile, each, 0, unroll=2)

    def ow_up(a, k):
        return rcopy(ow_buf.at[a, k], ow_buf.at[a, k], ou_send, o_recv.at[a, k], up)

    def ow_down(a, k):
        return rcopy(ow_buf.at[a, k], ow_buf.at[a, k], on_send, o_recv.at[a, k], down)

    def ow_share(a, k):
        i = lax.rem(a, n_half)
        when(a // n_half != t, rcopy(ow_buf.at[a, k], ow_oth.at[i, k], od_send, od_recv.at[i, k], other))

    def ow_relay(d, k):
        a, b = s - d, s + d

        @pl.when((a >= 0) & has_up)
        def _():
            ow_up(a, k).wait_recv()
            ow_up(a, k).start()
            ow_share(a, k)

        @pl.when((b < n_sp) & has_down)
        def _():
            ow_down(b, k).wait_recv()
            ow_down(b, k).start()
            ow_share(b, k)

    def ow_take(d, k):
        a, b = s - d, s + d

        @pl.when((a >= 0) & jnp.logical_not(has_up))
        def _():
            ow_up(a, k).wait_recv()
            ow_share(a, k)

        @pl.when((b < n_sp) & jnp.logical_not(has_down))
        def _():
            ow_down(b, k).wait_recv()
            ow_share(b, k)

    took(slot(0, s, f), w_in.at[0, 0])
    both(s, f)
    took(srcs[0], w_in.at[0, 1])
    spread(0)
    took(xs.at[f, :, cols(t)], in_sem.at[0])
    for p, hs in ((px, (0, 1)), (py, (1, 0))):
        for h in hs:
            rcopy(x_slot(f, h, t), x_slot(f, h, t), x_send, x_recv.at[f, h], (s, p, t)).start()
    for h in range(2):
        hand_on(f, h)
    took(ow_buf.at[s, 0], in_sem.at[1])
    when(has_up, ow_up(s, 0))
    when(has_down, ow_down(s, 0))
    for c in loads:
        c.wait()
    for g in range(n_fs):
        e_src[g] = jnp.broadcast_to(extra[g : g + 1, :], e_src.shape[1:])
    for g in order[1:]:
        rcopy(e_src.at[g], e_all.at[f], e_send, e_recv, (s, g, t)).start()
    for c in (1, 2):
        took(slot(c, s, f), w_in.at[c, 0])
        took(srcs[c], w_in.at[c, 1])
        spread(c)
    e_all[f] = e_src[f]
    for g in order[1:]:
        came(slot(0, s, g), w_recv.at[s, g])
        both(s, g)
    gd = gmap.shape[1]
    for i in range(width // gd):
        at = slice(i * gd, (i + 1) * gd)
        scaled = (gmap[t * (width // gd) + i].astype(F32) * pgain[:, at]).astype(BF)
        ow_buf[s, 1, at, :] = jnp.dot(scaled, wop[at, :], preferred_element_type=F32).astype(BF)
    norm(0)
    relay(0, 1, order[:2])
    for g, h, onto in ((px, 0, py), (py, 1, px)):
        here = landed(g, h)
        rcopy(here, here, x_send, x_recv.at[g, h], (s, onto, t)).start()
        hand_on(g, h)
    relay(0, 1, order[2:])
    for d in range(2, n_sp - 1):
        relay(0, d, order[:2])
    for g, h in ((px, 1), (py, 0)):
        landed(g, h)
        hand_on(g, h)
    norm(1)
    for d in range(2, n_sp - 1):
        relay(0, d, order[2:])
    own_block(1)
    pl.when(is_end)(lambda: own_block(2))
    norm(2)
    for d in range(1, n_sp - 1):
        arrive(0, d)
    main(0, 0)
    for h in range(2):
        landed(pd, h)
        hand_on(pd, h)
    norm(3)
    main(0, 1)
    relay(1, 1)

    reach = rim.shape[1]
    edge = rcopy(rim_src, rim, g_send, g_recv, up)

    def send_rim():
        for j in range(n_fs):
            rim_src[j] = acc1[j // 2, (j % 2 + 1) * rows - reach : (j % 2 + 1) * rows, :].astype(BF)
        when(has_up, edge)

    last(0)
    came(e_all.at[0 : n_fs - 1], e_recv)

    mine = pl.ds(pl.multiple_of(f * ch, ch), ch)
    gap_f = gap[:, mine]
    gain_f = rec_gain[:, mine]
    at = lax.broadcasted_iota(jnp.int32, (size, size), 0)
    causal = at >= lax.broadcasted_iota(jnp.int32, (size, size), 1)
    lower = jnp.where(causal, 1.0, 0.0).astype(BF)
    lower = jnp.concatenate([lower, lower], axis=1)

    def scan(j):
        p, base = j // 2, j % 2 * rows
        state = None
        so_far = jnp.zeros((1, ch), F32)
        e_cols = e_all[order[j]].T
        for n in range(rows // size):
            here = slice(n * size, (n + 1) * size)
            there = slice(base + n * size, base + (n + 1) * size)
            v = acc0[p, there, 2 * ch : 3 * ch].astype(BF)
            q = jax.nn.silu(acc0[p, there, 0:ch].astype(BF).astype(F32))
            k = gap_f * jax.nn.sigmoid(-acc0[p, there, ch : 2 * ch].astype(BF).astype(F32))
            logs = jnp.log1p(-k) + e_cols[here, 0:1]
            high = logs.astype(BF)
            low = (logs - high.astype(F32)).astype(BF)
            within = mm(lower, jnp.concatenate([high, low], axis=0), NN)
            mid = within[size // 2 - 1 : size // 2]
            end = within[size - 1 :]
            q = q * jnp.exp(within - mid)
            k = (k * jnp.exp(mid - within)).astype(BF)
            q_up = q.astype(BF)
            scores = jnp.where(causal, mm(q_up, k, NT), 0.0).astype(BF)
            out = mm(scores, v, NN)
            if n:
                out = out + mm(q_up, (state * jnp.exp(mid)).astype(BF), NT)
            local[j, here, :] = out
            qd[j, here, :] = (q * jnp.exp(mid + so_far)).astype(BF)
            fresh = mm(v, k, TN) * jnp.exp(end - mid)
            state = state * jnp.exp(end) + fresh if n else fresh
            so_far = so_far + end
        own_st[j] = state
        own_de[j] = jnp.broadcast_to(jnp.exp(so_far), own_de.shape[1:])

    def carry(g):
        return rcopy(t_out.at[g], t_in.at[g], t_send, t_recv.at[g], up)

    for j in range(n_fs):
        scan(j)

        @pl.when(jnp.logical_not(has_down))
        def _():
            t_in[j] = jnp.zeros(t_in.shape[1:], BF)
            t_out[j] = own_st[j].astype(BF)
            carry(j).start()

    for d in range(2, n_sp - 1):
        relay(1, d)
    pl.when(jnp.logical_not(is_end))(lambda: own_block(2))
    @pl.when(jnp.logical_not(is_end))
    def _():
        each_pair(lambda p: gemm(1, p, slice(0, total_k), False))
        send_rim()

    relay(2, 1)
    def chain():
        for g in range(n_fs):
            carry(g).wait_recv()
            t_out[g] = (own_st[g] + t_in[g].astype(F32) * own_de[g, 0:1, :]).astype(BF)
            carry(g).start()

    group = (t * n_fs * ch + f * ch) // gd
    spot = s * rows + lax.broadcasted_iota(jnp.int32, (rows, ch), 0)
    window = 2
    for level in range(1, POOL_GROUPS):
        window = jnp.where(group == level, 2 ** (level + 1), window)
    share = 1.0 / jnp.minimum(spot + 1, window).astype(F32)

    def rows_of(g):
        return pl.ds(pl.multiple_of(g * rows, rows), rows)

    def pool(j):
        zp = acc1[j // 2, j % 2 * rows : (j % 2 + 1) * rows, :].astype(BF).astype(F32)
        running = jnp.concatenate([rim[j].astype(F32), zp], axis=0)
        total = None
        for level in range(POOL_GROUPS):
            stride = 2**level
            running = running[stride:] + running[:-stride]
            now = running[running.shape[0] - rows :]
            total = now if level == 0 else jnp.where(group == level, now, total)
        acts[1, t, f, rows_of(order[j]), :] = (total * share - zp).astype(BF)

    part_rows = n_fs * rows // 2
    quarter = part_rows // 2

    def a_slot(k, u, g, h, q=None):
        lo, n = (h * part_rows, part_rows) if q is None else (h * part_rows + q * quarter, quarter)
        return acts.at[k, u, g, lo : lo + n, :]

    def a_share(k, g, h):
        here = a_slot(k, t, g, h)
        rcopy(here, here, ad_send, ad_recv.at[k, h], other).start()

    def publish(k):
        for h in range(2):
            here = a_slot(k, t, f, h)
            for p in (px, py):
                rcopy(here, here, a_send, a_recv.at[k, f, h], (s, p, t)).start()
            a_share(k, f, h)

    def a_forward(k, h):
        for g, q, onto in ((px, 0, py), (py, 1, px)):
            came(a_slot(k, t, g, h), a_recv.at[k, g, h])
            here = a_slot(k, t, g, h, q)
            rcopy(here, here, a_send, a_recv.at[k, g, h], (s, onto, t)).start()
            a_share(k, g, h)

    def a_rest(k, h):
        came(a_slot(k, t, pd, h), a_recv.at[k, pd, h])
        a_share(k, pd, h)

    def a_other(k, h):
        came(acts.at[k, 1 - t, :, h * part_rows : (h + 1) * part_rows, :], ad_recv.at[k, h])

    def pool_all():
        pl.when(has_down)(edge.wait_recv)
        for j in range(n_fs):
            pool(j)
        publish(1)

    mid_low = jnp.logical_not(is_end) & low
    mid_high = jnp.logical_not(is_end) & jnp.logical_not(low)
    pl.when(mid_low)(chain)
    for d in range(2, n_sp - 1):
        relay(2, d)
    pl.when(jnp.logical_not(is_end))(lambda: each_pair(lambda p: gemm(2, p, slice(0, total_k), False)))
    pl.when(mid_high)(pool_all)
    pl.when(mid_high)(chain)
    when(has_up, ow_up(s, 1))
    when(has_down, ow_down(s, 1))
    for k in range(2):
        ow_share(s, k)
    ow_relay(1, 0)
    for d in range(1, n_sp - 1):
        arrive(1, d)
    pl.when(is_end)(lambda: each_pair(lambda p: gemm(1, p, near, False)))
    last(1)
    @pl.when(is_end)
    def _():
        send_rim()

        @pl.when(jnp.logical_not(has_down))
        def _():
            rim[...] = jnp.zeros(rim.shape, BF)

    pl.when(jnp.logical_not(mid_high))(pool_all)
    ones = jnp.ones((8, ch), BF)

    def finish(j):
        g = order[j]
        rec = local[j] + mm(qd[j], t_in[j], NT)
        sums = mm(ones, (rec * rec).astype(BF), NT)
        for i in range(lanes):
            sq_src[pl.ds(g * lanes + i, 1), :] = sums[0:1, i * 128 : (i + 1) * 128]
        gate = jax.nn.silu(acc2[j // 2, j % 2 * rows : (j % 2 + 1) * rows, :].astype(BF).astype(F32))
        acts[0, t, f, rows_of(g), :] = (rec * gain_f * gate).astype(BF)

    def finish_all():
        for j in range(n_fs):
            finish(j)
        for u, g in [(1 - t, f)] + [(u, g) for g in order[1:] for u in (t, 1 - t)]:
            rcopy(sq_src, sq_all.at[t * n_fs + f], q_send, q_recv, (s, g, u)).start()
        publish(0)
        sq_all[t * n_fs + f] = sq_src[...]

    pl.when(jnp.logical_not(is_end))(finish_all)
    for d in range(1, n_sp - 1):
        arrive(2, d)
    pl.when(is_end)(lambda: each_pair(lambda p: gemm(2, p, near, False)))
    a_forward(1, 0)
    ow_relay(1, 1)
    a_forward(1, 1)
    last(2)
    @pl.when(has_down & jnp.logical_not(has_up))
    def _():
        for g in range(n_fs):
            carry(g).wait_recv()

    pl.when(is_end)(finish_all)
    for d in range(2, n_sp - 1):
        ow_relay(d, 0)
    for h in range(2):
        a_rest(1, h)
    for d in range(2, n_sp - 1):
        ow_relay(d, 1)
    a_forward(0, 0)
    a_forward(0, 1)
    for d in range(1, n_sp - 1):
        for k in range(2):
            ow_take(d, k)
    came(sq_all.at[0 : n_tp * n_fs - 1], q_recv)
    sums = sum(sq_all[i] for i in range(n_tp * n_fs))
    scale = lax.rsqrt(sums / (n_tp * width) + EPS).T
    half_lanes = n_fs * lanes // 2
    scales = [
        jnp.concatenate([scale[:, h * half_lanes + i : h * half_lanes + i + 1] for i in range(half_lanes)], axis=0)
        for h in range(2)
    ]
    late = s - t * n_half >= n_half - 1

    def spot_of(a, g):
        return pl.ds(pl.multiple_of((a * n_fs + g) * cw, cw), cw)

    def at_part(i, g, u):
        return (i * n_fs + g) * n_tp + u

    def piece(i, g, u):
        return rcopy(part.at[at_part(i, g, u)], final.at[:, spot_of(t * n_half + i, f)], m_send, m_recv, (s, g, u))

    def weight_side(k, a, i, h):
        here = slice(h * part_rows, (h + 1) * part_rows)
        total = None
        for u, w in ((t, ow_buf.at[a, k]), (1 - t, ow_oth.at[i, k])):
            left = jnp.concatenate([acts[k, u, b, here, :] for b in range(n_fs)], axis=1)
            now = jnp.dot(left, w[...], preferred_element_type=F32)
            total = now if total is None else total + now
        return total

    def rec_side(a, i, h):
        half_way[h] = weight_side(0, a, i, h) * scales[h]

    def pool_side(a, i, h):
        mixed = (half_way[h] + weight_side(1, a, i, h)).astype(BF)
        for g in range(h * n_fs // 2, (h + 1) * n_fs // 2):
            for u in range(n_tp):
                lo = (g * n_tp + u) * out_rows - h * part_rows
                part[at_part(i, g, u)] = mixed[lo : lo + out_rows]
                when((g != f) | (u != t), piece(i, g, u))

    def ow_got(j, k):
        i = jnp.where(late, n_half - 1 - j, j)
        if j == n_half - 1:
            ow_take(n_sp - 1, k)
        came(ow_oth.at[i, k], od_recv.at[i, k])
        return t * n_half + i, i

    owns = []
    for j in range(n_half):
        if j == 0:
            for k in range(2):
                a, i = ow_got(0, k)
            for h in range(2):
                a_rest(0, h)
                for k in range(2):
                    a_other(k, h)
                rec_side(a, i, h)
                pool_side(a, i, h)
        else:
            a, i = ow_got(j, 0)
            for h in range(2):
                rec_side(a, i, h)
            a, i = ow_got(j, 1)
            for h in range(2):
                pool_side(a, i, h)
        own = pltpu.make_async_copy(part.at[at_part(i, f, t)], final.at[:, spot_of(a, f)], in_sem.at[min(j, 1)])
        own.start()
        owns.append(own)

    pieces = part.at[0 : n_half * (n_tp * n_fs - 1)]
    came(pieces, m_recv)
    for own in owns:
        own.wait()
    sent(pieces, m_send)
    sent(xs.at[0:3, :, 0:half], x_send)
    sent(xs.at[:, :, 0:half], xd_send)
    sent(e_src.at[0 : n_fs - 1], e_send)
    for c in range(3):
        sent(srcs[c], w_send.at[c])
    sent(acts.at[:, 0, 0:3], a_send)
    sent(acts.at[:, 0], ad_send)
    sent(sq_all.at[0 : n_tp * n_fs - 1], q_send)
    sent(ow_oth, od_send)
    for v in range(n_sp):
        @pl.when(s == v)
        def _():
            if v < n_sp - 1:
                for c in range(3):
                    sent(wss[c].at[0 : (v + 1) * blk, :], up_send.at[c])
                sent(ow_buf.at[0 : v + 1], ou_send)
                sent(rim_src, g_send)
                sent(t_out, t_send)
            if v > 0:
                for c in range(3):
                    sent(wss[c].at[0 : (n_sp - v) * blk, :], dn_send.at[c])
                sent(ow_buf.at[0 : n_sp - v], on_send)


def fused(
    n_sp, n_fs, n_tp, tokens, norm_gain, w_query, forget_weight, w_input, w_outgate, w_pool, forget_gap,
    extra_decay, rec_gain, group_weight, pool_gain, recurrent_output_weight, w_out_pool,
):
    rows, half = tokens.shape[1:]
    wr, width = w_query.shape
    ch = width // n_fs
    cw = w_out_pool.shape[1]
    n_half = n_sp // n_tp
    feats = n_sp * n_fs * wr
    lanes = rows // 128

    def buf(kind, *shape):
        return pltpu.VMEM(shape, kind)

    args = (
        tokens[0], w_query, forget_weight, w_input, w_outgate, w_pool, extra_decay[0].T, norm_gain[None],
        forget_gap[None], rec_gain[None], group_weight, pool_gain[None], recurrent_output_weight, w_out_pool,
    )
    extra, gain, gap, r_gain, gmap, pgain = args[6:12]
    (final,) = comm(
        functools.partial(layer_kernel, n_sp, n_fs, n_tp),
        [((rows // n_tp, n_sp * n_fs * cw), BF)],
        [
            buf(BF, n_fs - 1, wr, 3 * ch), buf(BF, n_fs - 1, wr, ch), buf(BF, n_fs - 1, wr, ch),
            buf(BF, feats, 3 * ch), buf(BF, feats, ch), buf(BF, feats, ch),
            buf(BF, n_fs, rows, n_tp * half), buf(BF, 2, n_fs // 2 * rows, n_tp * half),
            buf(F32, 2, n_fs // 2 * rows, 3 * ch), buf(F32, 2, n_fs // 2 * rows, ch), buf(F32, 2, n_fs // 2 * rows, ch),
            buf(F32, n_fs, 8, rows), buf(F32, n_fs, 8, rows),
            buf(F32, n_fs, rows, ch), buf(BF, n_fs, rows, ch),
            buf(F32, n_fs, ch, ch), buf(F32, n_fs, 8, ch),
            buf(BF, n_fs, ch, ch), buf(BF, n_fs, ch, ch),
            buf(BF, n_fs, 2**POOL_GROUPS, ch), buf(BF, n_fs, 2**POOL_GROUPS, ch),
            buf(BF, 2, n_tp, n_fs, n_fs * rows, ch),
            buf(F32, n_fs * lanes, 128), buf(F32, n_tp * n_fs, n_fs * lanes, 128),
            buf(BF, n_sp, 2, width, cw), buf(BF, n_half, 2, width, cw),
            buf(BF, n_half * n_fs * n_tp, rows // n_tp, cw), buf(F32, 2, n_fs // 2 * rows, cw),
        ]
        + [buf(a.dtype, *a.shape) for a in (extra, gain, gap, r_gain, gmap, pgain, w_out_pool)]
        + [
            dma(2), dma(3, 2), dma(7), dma(), dma(n_fs, 2), dma(), dma(n_fs),
            dma(3), dma(n_sp, n_fs), dma(2, n_sp), dma(2), dma(3), dma(3), dma(), dma(),
            dma(), dma(n_fs), dma(), dma(), dma(), dma(2, n_fs, 2), dma(), dma(2, 2), dma(), dma(),
            dma(), dma(), dma(n_sp, 2), dma(), dma(n_half, 2), dma(), dma(),
        ],
        1, "layer", [pl.BlockSpec(memory_space=pltpu.HBM)] * len(args), 58,
    )(*args)
    return final[None]


def run(n_sp, n_fs, n_tp, *args):
    wr, width = args[2].shape
    whole = n_fs * wr % 128 == 0 and args[-1].shape[1] % 128 == 0 and args[0].shape[1] % 256 == 0
    return (fused if whole and width == n_fs * HEAD_DIM else body)(n_sp, n_fs, n_tp, *args)


def solution(mesh):
    sizes = dict(mesh.shape)
    weight = P(("sp", "fs"), "tp")
    placed = (
        P("fs", "sp", "tp"), P(), weight, weight, weight, weight, weight, P("tp"),
        P("fs", "sp", "tp"), P("tp"), P(), P("tp"), P("tp", ("sp", "fs")), P("tp", ("sp", "fs")),
    )
    return jax.shard_map(
        functools.partial(run, sizes["sp"], sizes["fs"], sizes["tp"]),
        mesh=mesh, in_specs=placed, out_specs=P("fs", ("sp", "tp"), None), check_vma=False,
    )
```

```python
import functools
import jax
import jax.numpy as jnp
from jax import lax
from jax.experimental import pallas as pl
from jax.experimental.pallas import tpu as pltpu
from jax.sharding import PartitionSpec as P

HEAD_DIM = 128
POOL_GROUPS = 4
BLOCK = 64
EPS = 1e-06
HIGH = lax.Precision.HIGHEST
MESH = pl.DeviceIdType.MESH
BF = jnp.bfloat16
F32 = jnp.float32


def place():
    return lax.axis_index("sp"), lax.axis_index("fs"), lax.axis_index("tp")


def rcopy(src, dst, ssem, rsem, dev):
    return pltpu.make_async_remote_copy(
        src_ref=src, dst_ref=dst, send_sem=ssem, recv_sem=rsem, device_id=dev, device_id_type=MESH
    )


def greet(devs):
    barrier = pltpu.get_barrier_semaphore()
    for cond, dev in devs:
        def tell(dev=dev):
            pl.semaphore_signal(barrier, inc=1, device_id=dev, device_id_type=MESH)
        if cond is None:
            tell()
        else:
            pl.when(cond)(tell)
    pl.semaphore_wait(barrier, sum(1 if cond is None else jnp.where(cond, 1, 0) for cond, _ in devs))


def square(f):
    near = f + 1 - 2 * lax.rem(f, 2)
    return near, lax.rem(f + 2, 4), lax.rem(near + 2, 4)


def project_kernel(
    n_sp, n_fs, n_tp, tok, wq, wf, wi, wo, wp, extra, gain, gmap, pgain, wor, wop, z_ref, e_ref, ow_ref,
    wsrc, xs, ws, acc, x_send, x_recv, f_send, d_send, d_recv, w_send, w_recv, zr_send, zl_send, e_send, e_recv,
):
    s, f, t = place()
    rows, half = tok.shape
    part = rows // 2
    mats = (wq, wf, wi, wo, wp)
    wr, width = wq.shape
    ch = width // n_fs
    for i, w in enumerate(mats):
        for g in range(n_fs):
            wsrc[g, :, i * ch : (i + 1) * ch] = w[:, g * ch : (g + 1) * ch]
    other = (s, f, 1 - t)
    px, py, pd = square(f)
    order = (f, px, py, pd)
    up, down = (s + 1, f, t), (s - 1, f, t)
    has_up, has_down = s < n_sp - 1, s > 0
    greet([(None, other)] + [(None, (s, g, t)) for g in order[1:]] + [(has_up, up), (has_down, down)])

    def cols(c):
        return pl.ds(pl.multiple_of(c * half, half), half)

    def span(a, b):
        return pl.ds(pl.multiple_of((a * n_fs + b) * wr, wr), wr)

    def slot(a, b):
        return ws.at[span(a, b), :]

    def to_up(src, a, b):
        return rcopy(src, slot(a, b), zr_send.at[a, b], w_recv.at[a, b], up)

    def to_down(src, a, b):
        return rcopy(src, slot(a, b), zl_send.at[a, b], w_recv.at[a, b], down)

    sends = []

    def send(c):
        c.start()
        sends.append(c)

    def x_slot(g, h, c):
        return xs.at[g, h * part : (h + 1) * part, cols(c)]

    own = wsrc.at[f]
    pl.when(has_up)(lambda: to_up(own, s, f).start())
    pl.when(has_down)(lambda: to_down(own, s, f).start())
    for i, g in enumerate((pd, px, py)):
        send(rcopy(wsrc.at[g], slot(s, f), w_send.at[i], w_recv.at[s, f], (s, g, t)))
    for i, (p, hs) in enumerate(((px, (0, 1)), (py, (1, 0)))):
        for h in hs:
            send(rcopy(tok.at[h * part : (h + 1) * part, :], x_slot(f, h, t), x_send.at[i, h], x_recv.at[f, h], (s, p, t)))
    for h in range(2):
        send(rcopy(tok.at[h * part : (h + 1) * part, :], x_slot(f, h, t), d_send.at[f, h], d_recv.at[f, h], other))
    for i, g in enumerate(order[1:]):
        send(rcopy(extra.at[g], e_ref.at[f], e_send.at[i], e_recv.at[f], (s, g, t)))
    ws[span(s, f), :] = wsrc[f]
    xs[f, :, cols(t)] = tok[...]
    e_ref[f] = extra[f]
    ow_ref[0:width, :] = wor[...]
    gd = gmap.shape[1]
    for i in range(width // gd):
        at = slice(i * gd, (i + 1) * gd)
        scaled = (gmap[t * (width // gd) + i].astype(F32) * pgain[:, at]).astype(BF)
        folded = jnp.dot(scaled, wop[at, :], preferred_element_type=F32)
        ow_ref[width + i * gd : width + (i + 1) * gd, :] = folded.astype(BF)

    for g in order[1:]:
        to_up(slot(s, g), s, g).wait_recv()
        pl.when(has_up)(lambda: to_up(slot(s, g), s, g).start())
        pl.when(has_down)(lambda: to_down(slot(s, g), s, g).start())

    def landed(g, h):
        here = x_slot(g, h, t)
        rcopy(here, here, d_send.at[g, h], x_recv.at[g, h], other).wait_recv()
        return here

    def hand_on(g, h, here):
        send(rcopy(here, here, d_send.at[g, h], d_recv.at[g, h], other))

    for i, (g, h, onto) in enumerate(((px, 0, py), (py, 1, px))):
        here = landed(g, h)
        send(rcopy(here, here, f_send.at[i], x_recv.at[g, h], (s, onto, t)))
        hand_on(g, h, here)

    def relay(d):
        for g in order:
            a = s - d

            @pl.when(a >= 0)
            def _():
                to_up(slot(a, g), a, g).wait_recv()
                pl.when(has_up)(lambda: to_up(slot(a, g), a, g).start())
            b = s + d

            @pl.when(b < n_sp)
            def _():
                to_down(slot(b, g), b, g).wait_recv()
                pl.when(has_down)(lambda: to_down(slot(b, g), b, g).start())

    def add(a):
        k = pl.ds(pl.multiple_of(a * n_fs * wr, n_fs * wr), n_fs * wr)

        def each(i, _):
            acc[i] += jnp.dot(xs[i, :, k], ws[k, :], preferred_element_type=F32)
            return 0

        lax.fori_loop(0, n_fs, each, 0)

    def multiply(d):
        pl.when(s - d >= 0)(lambda: add(s - d))
        pl.when(s + d < n_sp)(lambda: add(s + d))

    relay(1)
    for g, h in ((px, 1), (py, 0), (pd, 0), (pd, 1)):
        hand_on(g, h, landed(g, h))
    for d in range(2, n_sp - 1):
        relay(d)
    for g in order:
        for h in range(2):
            here = x_slot(g, h, 1 - t)
            rcopy(here, here, d_send.at[g, h], d_recv.at[g, h], other).wait_recv()
    for g in order[1:]:
        rcopy(extra.at[f], e_ref.at[g], e_send.at[0], e_recv.at[g], other).wait_recv()
    for c in sends:
        c.wait_send()

    def norm(j, _):
        tile = 16
        per = rows // tile
        at = (j // per, pl.ds(pl.multiple_of(lax.rem(j, per) * tile, tile), tile))
        feats = xs[at[0], at[1], :].astype(F32)
        scale = lax.rsqrt(jnp.mean(feats * feats, axis=-1, keepdims=True) + EPS)
        xs[at[0], at[1], :] = (feats * scale * gain[...]).astype(BF)
        return 0

    lax.fori_loop(0, n_fs * rows // 16, norm, 0, unroll=2)

    if n_fs * wr % 128 == 0:
        own_k = pl.ds(pl.multiple_of(s * n_fs * wr, n_fs * wr), n_fs * wr)

        def begin(i, _):
            acc[i] = jnp.dot(xs[i, :, own_k], ws[own_k, :], preferred_element_type=F32)
            return 0

        lax.fori_loop(0, n_fs, begin, 0)
        for d in range(1, n_sp - 1):
            multiply(d)
        relay(n_sp - 1)
        multiply(n_sp - 1)

        def finish(i, _):
            z_ref[i] = acc[i].astype(BF)
            return 0
    else:
        relay(n_sp - 1)

        def finish(i, _):
            z_ref[i] = jnp.dot(xs[i], ws[...], preferred_element_type=F32).astype(BF)
            return 0

    lax.fori_loop(0, n_fs, finish, 0)

    for d in range(n_sp):
        for g in order:
            a = s - d

            @pl.when((a >= 0) & has_up)
            def _():
                to_up(slot(a, g), a, g).wait_send()
            b = s + d

            @pl.when((b < n_sp) & has_down)
            def _():
                to_down(slot(b, g), b, g).wait_send()


def dot(a, b, dims):
    return lax.dot_general(a, b, (dims, ((), ())), precision=HIGH, preferred_element_type=F32)


def state_kernel(
    n_sp, group_dim, z, e_all, gap, rec_gain, act, sq_out,
    local, qd, own_st, own_de, st_in, de_in, rim, s_send, s_recv, c_send, c_recv, g_send, g_recv,
):
    s, f, t = place()
    n_fs, rows, _ = z.shape
    ch = HEAD_DIM
    reach = rim.shape[1]
    devs = []
    for d in range(1, n_sp):
        devs.append((s + d < n_sp, (s + d, f, t)))
        devs.append((s - d >= 0, (s - d, f, t)))
    greet(devs)
    edge = rcopy(z.at[:, rows - reach :, 4 * ch :], rim, g_send, g_recv, (s + 1, f, t))
    pl.when(s < n_sp - 1)(edge.start)
    mine = pl.ds(pl.multiple_of(f * ch, ch), ch)
    gap_f = gap[:, mine]
    gain_f = rec_gain[:, mine]
    at = lax.broadcasted_iota(jnp.int32, (BLOCK, BLOCK), 0)
    causal = at >= lax.broadcasted_iota(jnp.int32, (BLOCK, BLOCK), 1)
    lower = causal.astype(F32)

    def one(g, _):
        state = jnp.zeros((ch, ch), F32)
        so_far = jnp.zeros((1, ch), F32)
        e_cols = e_all[g].T
        for n in range(rows // BLOCK):
            here = slice(n * BLOCK, (n + 1) * BLOCK)
            q, fo, v = (z[g, here, i * ch : (i + 1) * ch].astype(F32) for i in range(3))
            q = jax.nn.silu(q)
            k = gap_f * jax.nn.sigmoid(-fo)
            lo = n * BLOCK % 128
            lane = n * BLOCK // 128
            logs = jnp.log1p(-k) + e_cols[lo : lo + BLOCK, lane : lane + 1]
            within = dot(lower, logs, ((1,), (0,)))
            end = within[BLOCK - 1 :]
            q_up = q * jnp.exp(within)
            scores = jnp.where(causal, dot(q_up, k * jnp.exp(-within), ((1,), (1,))), 0.0)
            out = dot(scores, v, ((1,), (0,)))
            if n:
                out = out + dot(q_up, state, ((1,), (1,)))
            local[g, here, :] = out
            qd[g, here, :] = q_up * jnp.exp(so_far)
            state = state * jnp.exp(end) + dot(v.T, k * jnp.exp(end - within), ((1,), (0,)))
            so_far = so_far + end
        own_st[g] = state.astype(BF)
        own_de[g] = jnp.broadcast_to(jnp.exp(so_far), (8, ch))
        return 0

    lax.fori_loop(0, n_fs, one, 0)

    def pair(d):
        dev = (s + d, f, t)
        return (
            rcopy(own_st, st_in.at[d - 1], s_send.at[d - 1], s_recv.at[d - 1], dev),
            rcopy(own_de, de_in.at[d - 1], c_send.at[d - 1], c_recv.at[d - 1], dev),
        )

    for d in range(1, n_sp):
        @pl.when(s + d < n_sp)
        def _():
            for c in pair(d):
                c.start()

        @pl.when(s - d < 0)
        def _():
            st_in[d - 1] = jnp.zeros(st_in.shape[1:], st_in.dtype)
            de_in[d - 1] = jnp.ones(de_in.shape[1:], de_in.dtype)
    pl.when(s == 0)(lambda: rim.__setitem__(Ellipsis, jnp.zeros(rim.shape, rim.dtype)))
    pl.when(s > 0)(edge.wait_recv)
    group = (t * n_fs * ch + f * ch) // group_dim
    spot = s * rows + lax.broadcasted_iota(jnp.int32, (rows, ch), 0)
    window = 2
    for level in range(1, POOL_GROUPS):
        window = jnp.where(group == level, 2 ** (level + 1), window)
    counts = jnp.minimum(spot + 1, window).astype(F32)
    for g in range(n_fs):
        zp = z[g, :, 4 * ch :].astype(F32)
        running = jnp.concatenate([rim[g].astype(F32), zp], axis=0)
        total = None
        for level in range(POOL_GROUPS):
            stride = 2**level
            running = running[stride:] + running[:-stride]
            now = running[running.shape[0] - rows :]
            total = now if level == 0 else jnp.where(group == level, now, total)
        act[1, g * rows : (g + 1) * rows, :] = (total / counts - zp).astype(BF)
    for d in range(1, n_sp):
        @pl.when(s - d >= 0)
        def _():
            for c in pair(d):
                c.wait_recv()

    ones = jnp.ones((8, ch), F32)

    def finish(g, _):
        total = jnp.zeros((ch, ch), F32)
        for d in range(n_sp - 2, -1, -1):
            total = de_in[d, g, 0:1, :] * total + st_in[d, g].astype(F32)
        rec = local[g] + dot(qd[g], total, ((1,), (1,)))
        sums = dot(ones, rec * rec, ((1,), (1,)))
        for i in range(rows // 128):
            sq_out[g, i : i + 1, :] = sums[0:1, i * 128 : (i + 1) * 128]
        gate = jax.nn.silu(z[g, :, 3 * ch : 4 * ch].astype(F32))
        act[0, pl.ds(pl.multiple_of(g * rows, rows), rows), :] = (rec * gain_f * gate).astype(BF)
        return 0

    sq_out[...] = jnp.zeros(sq_out.shape, F32)
    lax.fori_loop(0, n_fs, finish, 0)
    for d in range(1, n_sp):
        @pl.when(s + d < n_sp)
        def _():
            for c in pair(d):
                c.wait_send()
    pl.when(s < n_sp - 1)(edge.wait_send)


def mix_kernel(
    n_sp, n_fs, n_tp, act, sq, ow, final,
    out, acts, sq_all, ow_all, relay_buf, wbuf, part,
    a_send, a_recv, f_send, d_send, d_recv, q_send, q_recv,
    up_send, down_send, o_recv, od_send, od_recv, m_send, m_recv,
):
    s, f, t = place()
    n_half = n_sp // n_tp
    rows = act.shape[1] // n_fs
    half = rows // n_tp
    width, cw = ow.shape[0] // 2, ow.shape[1]
    other = (s, f, 1 - t)
    px, py, pd = square(f)
    up, down = (s + 1, f, t), (s - 1, f, t)
    has_up, has_down = s < n_sp - 1, s > 0
    greet(
        [(None, other)]
        + [(None, (s, g, u)) for g in (px, py, pd) for u in (t, 1 - t)]
        + [(has_up, up), (has_down, down)]
    )

    def to_up(src, a):
        return rcopy(src, relay_buf.at[a], up_send.at[a], o_recv.at[a], up)

    def to_down(src, a):
        return rcopy(src, relay_buf.at[a], down_send.at[a], o_recv.at[a], down)

    def to_other(src, a):
        return rcopy(src, ow_all.at[lax.rem(a, n_half), t], od_send.at[a], od_recv.at[a], other)

    def keep(src, a):
        mine = a // n_half == t

        @pl.when(mine)
        def _():
            ow_all[lax.rem(a, n_half), t] = src[...]

        pl.when(jnp.logical_not(mine))(lambda: to_other(src, a).start())

    sends = []

    def send(c):
        c.start()
        sends.append(c)

    for i, (p, order) in enumerate(((px, (0, 1)), (py, (1, 0)))):
        for h in order:
            send(rcopy(act.at[h], acts.at[t, f, h], a_send.at[i, h], a_recv.at[f, h], (s, p, t)))
    pl.when(has_up)(lambda: to_up(ow, s).start())
    pl.when(has_down)(lambda: to_down(ow, s).start())
    for h in range(2):
        send(rcopy(act.at[h], acts.at[t, f, h], d_send.at[f, h], d_recv.at[f, h], other))
    for i, g in enumerate((px, py, pd)):
        for u in range(n_tp):
            send(rcopy(sq, sq_all.at[t, f], q_send.at[i, u], q_recv.at[t, f], (s, g, u)))
    send(rcopy(sq, sq_all.at[t, f], q_send.at[n_fs - 1, 0], q_recv.at[t, f], other))
    acts[t, f] = act[...]
    sq_all[t, f] = sq[...]
    keep(ow, s)

    def landed(g, h):
        here = acts.at[t, g, h]
        rcopy(here, here, d_send.at[g, h], a_recv.at[g, h], other).wait_recv()
        return here

    def hand_on(g, h, here):
        send(rcopy(here, here, d_send.at[g, h], d_recv.at[g, h], other))

    for i, (g, h, onto) in enumerate(((px, 0, py), (py, 1, px))):
        here = landed(g, h)
        send(rcopy(here, here, f_send.at[i], a_recv.at[g, h], (s, onto, t)))
        hand_on(g, h, here)

    def step(d):
        a = s - d

        @pl.when(a >= 0)
        def _():
            to_up(relay_buf.at[a], a).wait_recv()
            pl.when(has_up)(lambda: to_up(relay_buf.at[a], a).start())
            keep(relay_buf.at[a], a)
        b = s + d

        @pl.when(b < n_sp)
        def _():
            to_down(relay_buf.at[b], b).wait_recv()
            pl.when(has_down)(lambda: to_down(relay_buf.at[b], b).start())
            keep(relay_buf.at[b], b)

    for d in range(1, n_sp):
        step(d)
    for g, h in ((px, 1), (py, 0), (pd, 0), (pd, 1)):
        hand_on(g, h, landed(g, h))
    for i in range(n_half):
        a = t * n_half + i
        here = ow_all.at[i, 1 - t]
        rcopy(here, here, od_send.at[a], od_recv.at[a], other).wait_recv()
    for i in range(n_half):
        for u in range(n_tp):
            for k in range(2):
                wbuf[k, u * width : (u + 1) * width, i * cw : (i + 1) * cw] = ow_all[i, u, k * width : (k + 1) * width, :]
    for g in (px, py, pd):
        for u in range(n_tp):
            here = sq_all.at[u, g]
            rcopy(here, here, q_send.at[0, 0], q_recv.at[u, g], other).wait_recv()
    here = sq_all.at[1 - t, f]
    rcopy(here, here, q_send.at[0, 0], q_recv.at[1 - t, f], other).wait_recv()
    for g in (f, px, py, pd):
        for h in range(2):
            here = acts.at[1 - t, g, h]
            rcopy(here, here, d_send.at[g, h], d_recv.at[g, h], other).wait_recv()

    def piece(g, u):
        return rcopy(part.at[g, u], out.at[f, t], m_send.at[g, u], m_recv.at[f, t], (s, g, u))

    def spread(g):
        for u in range(n_tp):
            c = piece(g, u)
            c.start()
            sends.append(c)

    last = None
    for g in (pd, f, px, py):
        here = pl.ds(pl.multiple_of(g * rows, rows), rows)
        sums = sum(sq_all[u, i, g] for u in range(n_tp) for i in range(n_fs))
        scale = lax.rsqrt(sums / (n_tp * width) + EPS).T
        scale = jnp.concatenate([scale[:, i : i + 1] for i in range(rows // 128)], axis=0)
        left = [
            jnp.concatenate([acts[u, i, h, here, :] for u in range(n_tp) for i in range(n_fs)], axis=1)
            for h in range(2)
        ]
        mixed = (
            jnp.dot(left[0], wbuf[0], preferred_element_type=F32) * scale
            + jnp.dot(left[1], wbuf[1], preferred_element_type=F32)
        ).astype(BF)
        for u in range(n_tp):
            part[g, u] = mixed[u * half : (u + 1) * half]
        if last is not None and last is not f:
            spread(last)
        if last is f:
            c = piece(f, 1 - t)
            c.start()
            sends.append(c)
        last = g
    out[f, t] = part[f, t]
    for i in range(n_half):
        to_other(ow, (1 - t) * n_half + i).wait_send()
    for d in range(n_sp):
        a, b = s - d, s + d

        @pl.when((a >= 0) & has_up)
        def _():
            to_up(ow, a).wait_send()

        @pl.when((b < n_sp) & has_down)
        def _():
            to_down(ow, b).wait_send()
    spread(last)
    for c in sends:
        c.wait_send()
    for g in (px, py, pd):
        for u in range(n_tp):
            here = out.at[g, u]
            rcopy(here, here, m_send.at[g, u], m_recv.at[g, u], other).wait_recv()
    here = out.at[f, 1 - t]
    rcopy(here, here, m_send.at[f, 1 - t], m_recv.at[f, 1 - t], other).wait_recv()
    for u in range(n_tp):
        for i in range(n_half):
            for g in range(n_fs):
                lo = ((u * n_half + i) * n_fs + g) * cw
                final[:, lo : lo + cw] = out[g, u, :, i * cw : (i + 1) * cw]


def vmem(count):
    return [pl.BlockSpec(memory_space=pltpu.VMEM)] * count


def dma(*shape):
    return pltpu.SemaphoreType.DMA(shape) if shape else pltpu.SemaphoreType.DMA


def comm(kernel, outs, scratch, number, name, ins=None, limit=60):
    return pl.pallas_call(
        kernel,
        out_shape=[jax.ShapeDtypeStruct(a, b) if ins is None else pltpu.VMEM(a, b) for a, b in outs],
        **({"out_specs": vmem(len(outs))} if ins is None else {"in_specs": ins, "out_specs": [pl.BlockSpec(memory_space=pltpu.VMEM)] * len(outs)}),
        scratch_shapes=scratch,
        compiler_params=pltpu.CompilerParams(
            collective_id=number, has_side_effects=True, vmem_limit_bytes=limit * 1024 * 1024
        ),
        name=name,
    )


def body(
    n_sp, n_fs, n_tp, tokens, norm_gain, w_query, forget_weight, w_input, w_outgate, w_pool, forget_gap,
    extra_decay, rec_gain, group_weight, pool_gain, recurrent_output_weight, w_out_pool,
):
    s, f, t = place()
    rows, half = tokens.shape[1:]
    width = w_query.shape[1]
    ch = width // n_fs
    n_w = 5
    wr = w_query.shape[0]
    lanes = rows // 128
    extra = jnp.pad(extra_decay[0].T.reshape(n_fs, lanes, 128), ((0, 0), (0, 8 - lanes), (0, 0)))
    cw = w_out_pool.shape[1]
    z, e_all, ow = comm(
        functools.partial(project_kernel, n_sp, n_fs, n_tp),
        [((n_fs, rows, n_w * ch), BF), ((n_fs, 8, 128), F32), ((2 * width, cw), BF)],
        [
            pltpu.VMEM((n_fs, wr, n_w * ch), BF), pltpu.VMEM((n_fs, rows, n_tp * half), BF),
            pltpu.VMEM((n_sp * n_fs * wr, n_w * ch), BF), pltpu.VMEM((n_fs, rows, n_w * ch), F32),
            dma(2, 2), dma(n_fs, 2), dma(2), dma(n_fs, 2), dma(n_fs, 2), dma(n_fs - 1), dma(n_sp, n_fs),
            dma(n_sp, n_fs), dma(n_sp, n_fs), dma(n_fs - 1), dma(n_fs),
        ],
        1, "project",
    )(
        tokens[0], w_query, forget_weight, w_input, w_outgate, w_pool, extra, norm_gain[None],
        group_weight, pool_gain[None], recurrent_output_weight, w_out_pool,
    )
    n_half = n_sp // n_tp
    act, sq = comm(
        functools.partial(state_kernel, n_sp, group_weight.shape[1]),
        [((2, n_fs * rows, ch), BF), ((n_fs, 8, 128), F32)],
        [
            pltpu.VMEM((n_fs, rows, ch), F32), pltpu.VMEM((n_fs, rows, ch), F32),
            pltpu.VMEM((n_fs, ch, ch), BF), pltpu.VMEM((n_fs, 8, ch), F32),
            pltpu.VMEM((n_sp - 1, n_fs, ch, ch), BF), pltpu.VMEM((n_sp - 1, n_fs, 8, ch), F32),
            pltpu.VMEM((n_fs, 2**POOL_GROUPS, ch), BF),
            dma(n_sp - 1), dma(n_sp - 1), dma(n_sp - 1), dma(n_sp - 1), dma(), dma(),
        ],
        2, "state",
    )(z, e_all, forget_gap[None], rec_gain[None])
    out_shape = (n_fs, n_tp, rows // n_tp, n_half * cw)
    (final,) = comm(
        functools.partial(mix_kernel, n_sp, n_fs, n_tp),
        [((rows // n_tp, n_tp * n_half * n_fs * cw), BF)],
        [
            pltpu.VMEM(out_shape, BF), pltpu.VMEM((n_tp, n_fs) + act.shape, BF), pltpu.VMEM((n_tp, n_fs) + sq.shape, F32),
            pltpu.VMEM((n_half, n_tp) + ow.shape, BF), pltpu.VMEM((n_sp,) + ow.shape, BF),
            pltpu.VMEM((2, n_tp * width, n_half * cw), BF), pltpu.VMEM(out_shape, BF),
            dma(2, 2), dma(n_fs, 2), dma(2), dma(n_fs, 2), dma(n_fs, 2), dma(n_fs, n_tp), dma(n_tp, n_fs),
            dma(n_sp), dma(n_sp), dma(n_sp), dma(n_sp), dma(n_sp), dma(n_fs, n_tp), dma(n_fs, n_tp),
        ],
        3, "mix",
    )(act, sq, ow)
    return final[None]


def mm(a, b, dims):
    return lax.dot_general(a, b, (dims, ((), ())), preferred_element_type=F32)


NN, NT, TN = ((1,), (0,)), ((1,), (1,)), ((0,), (0,))


def layer_kernel(
    n_sp, n_fs, n_tp, tok, wq, wf, wi, wo, wp, extra_in, gain_in, gap_in, rec_gain_in, gmap_in, pgain_in, wor, wop_in, final,
    src0, src1, src2, src3, ws0, ws1, ws2, ws3, xs, xn, acc0, acc1, acc2, acc3, k_buf, rel, st_buf, lead, e_src, e_all, local, qd, own_st, own_de,
    t_out, t_in, rim_src, rim, acts, sq_src, sq_all, ow_buf, ow_oth, part, half_way,
    extra, gain, gap, rec_gain, gmap, pgain, wop,
    in_sem, w_in, p_in, x_send, x_recv, xd_send, xd_recv, w_send, w_recv, b_recv, ba_recv, up_send, dn_send, e_send, e_recv,
    t_send, t_recv, g_send, g_recv, a_send, a_recv, ad_send, ad_recv, q_send, q_recv,
    ou_send, on_send, o_recv, od_send, od_recv, m_send, m_recv,
):
    s, f, t = place()
    rows, half = tok.shape
    cut = rows // 2
    wr, width = wq.shape
    ch = width // n_fs
    cw = wor.shape[1]
    n_half = n_sp // n_tp
    out_rows = rows // n_tp
    lanes = rows // 128
    size = 128
    blk = n_fs * wr
    total_k = n_sp * blk
    groups = ((wf, wi), (wp,), (wo,), (wq,))
    srcs, wss, accs = (src0, src1, src2, src3), (ws0, ws1, ws2, ws3), (acc0, acc1, acc2, acc3)
    other = (s, f, 1 - t)
    px, py, pd = square(f)
    order = (f, px, py, pd)
    up, down = (s + 1, f, t), (s - 1, f, t)
    has_up, has_down = s < n_sp - 1, s > 0
    is_end = jnp.logical_not(has_up & has_down)

    def when(cond, *copies):
        @pl.when(cond)
        def _():
            for c in copies:
                c.start()

    def sent(ref, sem):
        rcopy(ref, ref, sem, sem, other).wait_send()

    def came(ref, sem):
        rcopy(ref, ref, sem, sem, other).wait_recv()

    def cols(c):
        return pl.ds(pl.multiple_of(c * half, half), half)

    def span(a, b):
        return pl.ds(pl.multiple_of((a * n_fs + b) * wr, wr), wr)

    def slot(c, a, b):
        return wss[c].at[span(a, b), :]

    def block(c, a):
        return wss[c].at[pl.ds(pl.multiple_of(a * blk, blk), blk), :]

    def x_slot(g, h, c):
        return xs.at[g, h * cut : (h + 1) * cut, cols(c)]

    peers = (
        [(None, other)]
        + [(None, (s, g, u)) for g in order[1:] for u in (t, 1 - t)]
        + [(has_up, (s + 1, f, u)) for u in (t, 1 - t)]
        + [(has_down, (s - 1, f, u)) for u in (t, 1 - t)]
    )
    barrier = pltpu.get_barrier_semaphore()
    for cond, dev in peers:
        def tell(dev=dev):
            pl.semaphore_signal(barrier, inc=1, device_id=dev, device_id_type=MESH)
        if cond is None:
            tell()
        else:
            pl.when(cond)(tell)
    for c in (1, 0, 3, 2):
        for i, w in enumerate(groups[c]):
            for j, g in enumerate(order):
                lane = pl.ds(pl.multiple_of(g * ch, ch), ch)
                into = wss[c].at[span(s, f), i * ch : (i + 1) * ch] if j == 0 else srcs[c].at[j - 1, :, i * ch : (i + 1) * ch]
                pltpu.make_async_copy(w.at[:, lane], into, w_in.at[c, min(j, 1)]).start()
        if c == 0:
            pltpu.make_async_copy(tok, xs.at[f, :, cols(t)], in_sem.at[0]).start()
            pltpu.make_async_copy(wor, ow_buf.at[s, 0], in_sem.at[1]).start()
    params = ((extra_in, extra), (gain_in, gain), (gmap_in, gmap), (pgain_in, pgain), (wop_in, wop), (gap_in, gap), (rec_gain_in, rec_gain))
    loads = [pltpu.make_async_copy(a, b, p_in.at[i]) for i, (a, b) in enumerate(params)]
    for c in loads:
        c.start()
    pl.semaphore_wait(barrier, sum(1 if cond is None else jnp.where(cond, 1, 0) for cond, _ in peers))

    def took(ref, sem):
        pltpu.make_async_copy(ref, ref, sem).wait()

    def to_up(src, b, a):
        return rcopy(src, slot(0, a, b), up_send.at[0], w_recv.at[a, b], up)

    def to_down(src, b, a):
        return rcopy(src, slot(0, a, b), dn_send.at[0], w_recv.at[a, b], down)

    def both(a, b):
        when(has_up, to_up(slot(0, a, b), b, a))
        when(has_down, to_down(slot(0, a, b), b, a))

    def b_up(c, a):
        return rcopy(block(c, a), block(c, a), up_send.at[c], b_recv.at[c - 1, a], up)

    def b_down(c, a):
        return rcopy(block(c, a), block(c, a), dn_send.at[c], b_recv.at[c - 1, a], down)

    def spread(c):
        for j, g in enumerate(order[1:]):
            rsem = w_recv.at[s, f] if c == 0 else ba_recv.at[c - 1]
            rcopy(srcs[c].at[j], slot(c, s, f), w_send.at[c], rsem, (s, g, t)).start()

    def chunk(c, g, dev):
        here = slot(c, s, g)
        return rcopy(here, here, (up_send if dev is up else dn_send).at[c], b_recv.at[c - 1, s], dev)

    def own_wait(c):
        came(wss[c].at[0 : (n_fs - 1) * wr, :], ba_recv.at[c - 1])

    def own_up(c, cond=True):
        when(has_up & cond, *(chunk(c, g, up) for g in order[1:]))

    def own_down(c, cond=True):
        when(has_down & cond, *(chunk(c, g, down) for g in order[1:]))

    low = 2 * s < n_sp
    inner = jnp.logical_not(is_end)
    mid_low = inner & low
    mid_high = inner & jnp.logical_not(low)

    def relay(c, d, gs=(None,)):
        a, b = s - d, s + d

        def rising(extra):
            for g in gs:
                @pl.when((a >= 0) & has_up & extra)
                def _():
                    hop = to_up(slot(0, a, g), g, a) if c == 0 else b_up(c, a)
                    hop.wait_recv()
                    hop.start()

        def falling():
            for g in gs:
                @pl.when((b < n_sp) & has_down)
                def _():
                    hop = to_down(slot(0, b, g), g, b) if c == 0 else b_down(c, b)
                    hop.wait_recv()
                    hop.start()

        rising(low)
        falling()
        rising(jnp.logical_not(low))

    def arrive(c, d):
        for g in order if c == 0 else (None,):
            a, b = s - d, s + d

            @pl.when((a >= 0) & jnp.logical_not(has_up))
            def _():
                (to_up(slot(0, a, g), g, a) if c == 0 else b_up(c, a)).wait_recv()

            @pl.when((b < n_sp) & jnp.logical_not(has_down))
            def _():
                (to_down(slot(0, b, g), g, b) if c == 0 else b_down(c, b)).wait_recv()

    near = pl.ds(pl.multiple_of(jnp.where(has_down, blk, 0), blk), total_k - blk)
    far = pl.ds(pl.multiple_of(jnp.where(has_down, 0, total_k - blk), blk), blk)

    def gemm(c, p, k, more):
        out = jnp.dot(xn[p, :, k], wss[c][k, :], preferred_element_type=F32)
        accs[c][p] = accs[c][p] + out if more else out

    def main(c, p):
        pl.when(is_end)(lambda: gemm(c, p, near, False))
        pl.when(jnp.logical_not(is_end))(lambda: gemm(c, p, slice(0, total_k), False))

    def each_pair(step):
        def one(p, _):
            step(p)
            return 0

        lax.fori_loop(0, 2, one, 0)

    def last(c):
        arrive(c, n_sp - 1)
        pl.when(is_end)(lambda: each_pair(lambda p: gemm(c, p, far, True)))

    def landed(g, h):
        here = x_slot(g, h, t)
        came(here, x_recv.at[g, h])
        return here

    def hand_on(g, h):
        here = x_slot(g, h, t)
        rcopy(here, here, xd_send, xd_recv.at[g], other).start()

    def norm(j):
        g = order[j]
        came(xs.at[g, :, cols(1 - t)], xd_recv.at[g])
        tile = 16

        def each(i, _):
            at = pl.ds(pl.multiple_of(i * tile, tile), tile)
            feats = xs[g, at, :].astype(F32)
            scale = lax.rsqrt(jnp.mean(feats * feats, axis=-1, keepdims=True) + EPS)
            to = pl.ds(pl.multiple_of((j % 2) * rows + i * tile, tile), tile)
            xn[j // 2, to, :] = (feats * scale * gain[...]).astype(BF)
            return 0

        lax.fori_loop(0, rows // tile, each, 0, unroll=2)

    def ow_up(a, k):
        return rcopy(ow_buf.at[a, k], ow_buf.at[a, k], ou_send, o_recv.at[a, k], up)

    def ow_down(a, k):
        return rcopy(ow_buf.at[a, k], ow_buf.at[a, k], on_send, o_recv.at[a, k], down)

    def ow_share(a, k):
        i = lax.rem(a, n_half)
        when(a // n_half != t, rcopy(ow_buf.at[a, k], ow_oth.at[i, k], od_send, od_recv.at[i, k], other))

    def ow_start(a, k, rise, cond=True):
        to, has, edge_at = (s + 1, has_up, n_sp - 1) if rise else (s - 1, has_down, 0)
        ssem = ou_send if rise else on_send
        across = (to == edge_at) & (a // n_half != t)
        i = lax.rem(a, n_half)
        when(has & cond & jnp.logical_not(across), (ow_up if rise else ow_down)(a, k))
        when(has & cond & across, rcopy(ow_buf.at[a, k], ow_oth.at[i, k], ssem, od_recv.at[i, k], (to, f, 1 - t)))

    def ow_rise(d, k, cond=True):
        a = s - d

        @pl.when((a >= 0) & has_up & cond)
        def _():
            ow_up(a, k).wait_recv()
            ow_start(a, k, True)
            ow_share(a, k)

    def ow_fall(d, k, cond=True):
        b = s + d

        @pl.when((b < n_sp) & has_down & cond)
        def _():
            ow_down(b, k).wait_recv()
            ow_start(b, k, False)
            ow_share(b, k)

    def ow_relay(d, k):
        ow_rise(d, k)
        ow_fall(d, k)

    def ow_take(d, k):
        a, b = s - d, s + d
        pl.when((a >= 0) & jnp.logical_not(has_up) & (a // n_half == t))(ow_up(a, k).wait_recv)
        pl.when((b < n_sp) & jnp.logical_not(has_down) & (b // n_half == t))(ow_down(b, k).wait_recv)

    took(slot(1, s, f), w_in.at[1, 0])
    when(has_up, chunk(1, f, up))
    when(has_down, chunk(1, f, down))
    took(srcs[1], w_in.at[1, 1])
    spread(1)
    took(slot(0, s, f), w_in.at[0, 0])
    both(s, f)
    took(srcs[0], w_in.at[0, 1])
    spread(0)
    for c in (3, 2):
        took(slot(c, s, f), w_in.at[c, 0])
        when(has_up, chunk(c, f, up))
        when(has_down, chunk(c, f, down))
    took(xs.at[f, :, cols(t)], in_sem.at[0])
    for p, hs in ((px, (0, 1)), (py, (1, 0))):
        for h in hs:
            rcopy(x_slot(f, h, t), x_slot(f, h, t), x_send, x_recv.at[f, h], (s, p, t)).start()
    for h in range(2):
        hand_on(f, h)
    for c in loads:
        c.wait()
    for g in range(n_fs):
        e_src[g] = jnp.broadcast_to(extra[g : g + 1, :], e_src.shape[1:])
    for g in order[1:]:
        rcopy(e_src.at[g], e_all.at[f], e_send, e_recv, (s, g, t)).start()
    for c in (3, 2):
        took(srcs[c], w_in.at[c, 1])
        spread(c)
    e_all[f] = e_src[f]
    own_wait(1)
    own_up(1)
    own_down(1)
    for g in order[1:]:
        came(slot(0, s, g), w_recv.at[s, g])
        both(s, g)
    gd = gmap.shape[1]
    for i in range(width // gd):
        at = slice(i * gd, (i + 1) * gd)
        scaled = (gmap[t * (width // gd) + i].astype(F32) * pgain[:, at]).astype(BF)
        ow_buf[s, 1, at, :] = jnp.dot(scaled, wop[at, :], preferred_element_type=F32).astype(BF)
    norm(0)
    relay(1, 1)
    relay(0, 1, order[:2])
    for g, h, onto in ((px, 0, py), (py, 1, px)):
        here = landed(g, h)
        rcopy(here, here, x_send, x_recv.at[g, h], (s, onto, t)).start()
        hand_on(g, h)
    for d in range(2, n_sp - 1):
        relay(1, d)
    relay(0, 1, order[2:])
    for g, h in ((px, 1), (py, 0)):
        landed(g, h)
        hand_on(g, h)
    for d in range(2, n_sp - 1):
        relay(0, d, order[:2])
    norm(1)
    for c in (3, 2):
        own_wait(c)
        own_up(c, is_end)
        own_down(c, is_end)
    took(ow_buf.at[s, 0], in_sem.at[1])
    for k in range(2):
        ow_start(s, k, True, is_end)
        ow_start(s, k, False, is_end)
        ow_share(s, k)
    norm(2)
    for d in range(1, n_sp):
        arrive(1, d)
    gemm(1, 0, slice(0, total_k), False)
    for d in range(2, n_sp - 1):
        relay(0, d, order[2:])
    own_up(3, inner)
    own_down(3, inner)
    for h in range(2):
        landed(pd, h)
        hand_on(pd, h)
    norm(3)
    gemm(1, 1, slice(0, total_k), False)

    reach = rim.shape[1]
    edge = rcopy(rim_src, rim, g_send, g_recv, up)

    def send_rim():
        for j in range(n_fs):
            rim_src[j] = acc1[j // 2, (j % 2 + 1) * rows - reach : (j % 2 + 1) * rows, :].astype(BF)
        when(has_up, edge)

    send_rim()
    relay(3, 1)
    for d in range(1, n_sp - 1):
        arrive(0, d)
    each_pair(lambda p: main(0, p))
    def chain():
        for g in range(n_fs):
            carry(g).wait_recv()
            t_out[g] = (own_st[g] + t_in[g].astype(F32) * own_de[g, 0:1, :]).astype(BF)
            carry(g).start()

    group = (t * n_fs * ch + f * ch) // gd
    spot = s * rows + lax.broadcasted_iota(jnp.int32, (rows, ch), 0)
    window = 2
    for level in range(1, POOL_GROUPS):
        window = jnp.where(group == level, 2 ** (level + 1), window)
    share = 1.0 / jnp.minimum(spot + 1, window).astype(F32)

    def rows_of(g):
        return pl.ds(pl.multiple_of(g * rows, rows), rows)

    def pool(j):
        zp = acc1[j // 2, j % 2 * rows : (j % 2 + 1) * rows, :].astype(BF).astype(F32)
        running = jnp.concatenate([rim[j].astype(F32), zp], axis=0)
        total = None
        for level in range(POOL_GROUPS):
            stride = 2**level
            running = running[stride:] + running[:-stride]
            now = running[running.shape[0] - rows :]
            total = now if level == 0 else jnp.where(group == level, now, total)
        acts[1, t, f, rows_of(order[j]), :] = (total * share - zp).astype(BF)

    part_rows = n_fs * rows // 2
    quarter = part_rows // 2

    def a_slot(k, u, g, h, q=None):
        lo, n = (h * part_rows, part_rows) if q is None else (h * part_rows + q * quarter, quarter)
        return acts.at[k, u, g, lo : lo + n, :]

    def a_share(k, g, h):
        here = a_slot(k, t, g, h)
        rcopy(here, here, ad_send, ad_recv.at[k, h], other).start()

    def publish(k):
        for h in range(2):
            here = a_slot(k, t, f, h)
            for p in (px, py):
                rcopy(here, here, a_send, a_recv.at[k, f, h], (s, p, t)).start()
            a_share(k, f, h)

    def a_forward(k, h):
        for g, q, onto in ((px, 0, py), (py, 1, px)):
            came(a_slot(k, t, g, h), a_recv.at[k, g, h])
            here = a_slot(k, t, g, h, q)
            rcopy(here, here, a_send, a_recv.at[k, g, h], (s, onto, t)).start()
            a_share(k, g, h)

    def a_rest(k, h):
        came(a_slot(k, t, pd, h), a_recv.at[k, pd, h])
        a_share(k, pd, h)

    def a_other(k, h):
        came(acts.at[k, 1 - t, :, h * part_rows : (h + 1) * part_rows, :], ad_recv.at[k, h])

    def pool_all():
        pl.when(has_down)(edge.wait_recv)
        for j in range(n_fs):
            pool(j)
        publish(1)

    @pl.when(jnp.logical_not(has_down))
    def _():
        rim[...] = jnp.zeros(rim.shape, BF)

    pool_all()
    last(0)
    came(e_all.at[0 : n_fs - 1], e_recv)

    mine = pl.ds(pl.multiple_of(f * ch, ch), ch)
    gap_f = gap[:, mine]
    gain_f = rec_gain[:, mine]
    at = lax.broadcasted_iota(jnp.int32, (size, size), 0)
    causal = at >= lax.broadcasted_iota(jnp.int32, (size, size), 1)
    lower = jnp.where(causal, 1.0, 0.0).astype(BF)
    lower = jnp.concatenate([lower, lower], axis=1)

    steps = rows // size

    def spots(j, n):
        lo = j % 2 * rows + n * size
        return slice(n * size, (n + 1) * size), slice(lo, lo + size)

    def states(j):
        state = None
        so_far = jnp.zeros((1, ch), F32)
        e_cols = e_all[order[j]].T
        for n in range(steps):
            here, there = spots(j, n)
            v = acc0[j // 2, there, ch : 2 * ch].astype(BF)
            k = gap_f * jax.nn.sigmoid(-acc0[j // 2, there, 0:ch].astype(BF).astype(F32))
            logs = jnp.log1p(-k) + e_cols[here, 0:1]
            high = logs.astype(BF)
            low = (logs - high.astype(F32)).astype(BF)
            within = mm(lower, jnp.concatenate([high, low], axis=0), NN)
            mid = within[size // 2 - 1 : size // 2]
            end = within[size - 1 :]
            k = (k * jnp.exp(mid - within)).astype(BF)
            k_buf[j, here, :] = k
            rel[j, here, :] = within - mid
            lead[j, n] = jnp.broadcast_to(jnp.exp(mid + so_far), lead.shape[2:])
            fresh = mm(v, k, TN) * jnp.exp(end - mid)
            if n:
                st_buf[j, n - 1] = (state * jnp.exp(mid)).astype(BF)
            state = state * jnp.exp(end) + fresh if n else fresh
            so_far = so_far + end
        own_st[j] = state
        own_de[j] = jnp.broadcast_to(jnp.exp(so_far), own_de.shape[1:])

    def reads(j):
        for n in range(steps):
            here, there = spots(j, n)
            v = acc0[j // 2, there, ch : 2 * ch].astype(BF)
            q = jax.nn.silu(acc3[j // 2, there, :].astype(BF).astype(F32)) * jnp.exp(rel[j, here, :])
            q_up = q.astype(BF)
            scores = jnp.where(causal, mm(q_up, k_buf[j, here, :], NT), 0.0).astype(BF)
            out = mm(scores, v, NN)
            if n:
                out = out + mm(q_up, st_buf[j, n - 1], NT)
            local[j, here, :] = out
            qd[j, here, :] = (q * lead[j, n, 0:1, :]).astype(BF)

    def carry(g):
        return rcopy(t_out.at[g], t_in.at[g], t_send, t_recv.at[g], up)

    for j in range(n_fs):
        states(j)

        @pl.when(jnp.logical_not(has_down))
        def _():
            t_in[j] = jnp.zeros(t_in.shape[1:], BF)
            t_out[j] = own_st[j].astype(BF)
            carry(j).start()

    for d in range(2, n_sp - 1):
        relay(3, d)
    own_up(2, inner)
    own_down(2, inner)
    for d in range(1, n_sp - 1):
        arrive(3, d)
    each_pair(lambda p: main(3, p))
    last(3)
    for j in range(n_fs):
        reads(j)
    relay(2, 1)
    pl.when(mid_low)(chain)
    for d in range(2, n_sp - 1):
        relay(2, d)
    for k in range(2):
        ow_start(s, k, False, inner)
    a_forward(1, 0)
    pl.when(mid_high)(chain)
    for k in range(2):
        ow_start(s, k, True, inner)
        ow_rise(1, k, mid_low)
        ow_fall(1, k, mid_high)
    pl.when(inner)(lambda: each_pair(lambda p: gemm(2, p, slice(0, total_k), False)))
    a_forward(1, 1)
    ones = jnp.ones((8, ch), BF)

    def finish(j):
        g = order[j]
        rec = local[j] + mm(qd[j], t_in[j], NT)
        sums = mm(ones, (rec * rec).astype(BF), NT)
        for i in range(lanes):
            sq_src[pl.ds(g * lanes + i, 1), :] = sums[0:1, i * 128 : (i + 1) * 128]
        gate = jax.nn.silu(acc2[j // 2, j % 2 * rows : (j % 2 + 1) * rows, :].astype(BF).astype(F32))
        acts[0, t, f, rows_of(g), :] = (rec * gain_f * gate).astype(BF)

    def finish_all():
        for j in range(n_fs):
            finish(j)
        for u, g in [(1 - t, f)] + [(u, g) for g in order[1:] for u in (t, 1 - t)]:
            rcopy(sq_src, sq_all.at[t * n_fs + f], q_send, q_recv, (s, g, u)).start()
        publish(0)
        sq_all[t * n_fs + f] = sq_src[...]

    pl.when(inner)(finish_all)
    for k in range(2):
        ow_rise(1, k, mid_high)
    pl.when(inner)(lambda: a_forward(0, 0))
    for k in range(2):
        ow_fall(1, k, mid_low)
    pl.when(inner)(lambda: a_forward(0, 1))
    for d in range(1, n_sp - 1):
        arrive(2, d)
    pl.when(is_end)(lambda: each_pair(lambda p: gemm(2, p, near, False)))
    last(2)
    @pl.when(has_down & jnp.logical_not(has_up))
    def _():
        for g in range(n_fs):
            carry(g).wait_recv()

    pl.when(is_end)(finish_all)
    for d in range(2, n_sp - 1):
        ow_relay(d, 0)
    for h in range(2):
        a_rest(1, h)
    for d in range(2, n_sp - 1):
        ow_relay(d, 1)
    pl.when(is_end)(lambda: a_forward(0, 0))
    pl.when(is_end)(lambda: a_forward(0, 1))
    for d in range(1, n_sp - 1):
        for k in range(2):
            ow_take(d, k)
    came(sq_all.at[0 : n_tp * n_fs - 1], q_recv)
    sums = sum(sq_all[i] for i in range(n_tp * n_fs))
    scale = lax.rsqrt(sums / (n_tp * width) + EPS).T
    half_lanes = n_fs * lanes // 2
    scales = [
        jnp.concatenate([scale[:, h * half_lanes + i : h * half_lanes + i + 1] for i in range(half_lanes)], axis=0)
        for h in range(2)
    ]
    late = s - t * n_half >= n_half - 1

    def spot_of(a, g):
        return pl.ds(pl.multiple_of((a * n_fs + g) * cw, cw), cw)

    def at_part(i, g, u):
        return (i * n_fs + g) * n_tp + u

    def piece(i, g, u):
        return rcopy(part.at[at_part(i, g, u)], final.at[:, spot_of(t * n_half + i, f)], m_send, m_recv, (s, g, u))

    def weight_side(k, a, i, h):
        here = slice(h * part_rows, (h + 1) * part_rows)
        total = None
        for u, w in ((t, ow_buf.at[a, k]), (1 - t, ow_oth.at[i, k])):
            left = jnp.concatenate([acts[k, u, b, here, :] for b in range(n_fs)], axis=1)
            now = jnp.dot(left, w[...], preferred_element_type=F32)
            total = now if total is None else total + now
        return total

    def rec_side(a, i, h):
        half_way[h] = weight_side(0, a, i, h) * scales[h]

    def pool_side(a, i, h):
        mixed = (half_way[h] + weight_side(1, a, i, h)).astype(BF)
        for g in range(h * n_fs // 2, (h + 1) * n_fs // 2):
            for u in range(n_tp):
                lo = (g * n_tp + u) * out_rows - h * part_rows
                part[at_part(i, g, u)] = mixed[lo : lo + out_rows]
                when((g != f) | (u != t), piece(i, g, u))

    def ow_got(j, k):
        i = jnp.where(late, n_half - 1 - j, j)
        if j == n_half - 1:
            ow_take(n_sp - 1, k)
        came(ow_oth.at[i, k], od_recv.at[i, k])
        return t * n_half + i, i

    owns = []
    for j in range(n_half):
        if j == 0:
            for k in range(2):
                a, i = ow_got(0, k)
            for h in range(2):
                a_rest(0, h)
                for k in range(2):
                    a_other(k, h)
                rec_side(a, i, h)
                pool_side(a, i, h)
        else:
            a, i = ow_got(j, 0)
            for h in range(2):
                rec_side(a, i, h)
            a, i = ow_got(j, 1)
            for h in range(2):
                pool_side(a, i, h)
        own = pltpu.make_async_copy(part.at[at_part(i, f, t)], final.at[:, spot_of(a, f)], in_sem.at[min(j, 1)])
        own.start()
        owns.append(own)

    pieces = part.at[0 : n_half * (n_tp * n_fs - 1)]
    came(pieces, m_recv)
    for own in owns:
        own.wait()
    sent(pieces, m_send)
    sent(xs.at[0:3, :, 0:half], x_send)
    sent(xs.at[:, :, 0:half], xd_send)
    sent(e_src.at[0 : n_fs - 1], e_send)
    for c in range(4):
        sent(srcs[c], w_send.at[c])
    sent(acts.at[:, 0, 0:3], a_send)
    sent(acts.at[:, 0], ad_send)
    sent(sq_all.at[0 : n_tp * n_fs - 1], q_send)
    pl.when(jnp.logical_not(is_end))(lambda: sent(ow_oth, od_send))
    pl.when(is_end & (s // n_half != t))(lambda: sent(ow_oth.at[0], od_send))
    for v in range(n_sp):
        @pl.when(s == v)
        def _():
            if v < n_sp - 1:
                for c in range(4):
                    sent(wss[c].at[0 : (v + 1) * blk, :], up_send.at[c])
                sent(ow_buf.at[0 : v + 1], ou_send)
                sent(rim_src, g_send)
                sent(t_out, t_send)
            if v > 0:
                for c in range(4):
                    sent(wss[c].at[0 : (n_sp - v) * blk, :], dn_send.at[c])
                sent(ow_buf.at[0 : n_sp - v], on_send)


def fused(
    n_sp, n_fs, n_tp, tokens, norm_gain, w_query, forget_weight, w_input, w_outgate, w_pool, forget_gap,
    extra_decay, rec_gain, group_weight, pool_gain, recurrent_output_weight, w_out_pool,
):
    rows, half = tokens.shape[1:]
    wr, width = w_query.shape
    ch = width // n_fs
    cw = w_out_pool.shape[1]
    n_half = n_sp // n_tp
    feats = n_sp * n_fs * wr
    lanes = rows // 128

    def buf(kind, *shape):
        return pltpu.VMEM(shape, kind)

    args = (
        tokens[0], w_query, forget_weight, w_input, w_outgate, w_pool, extra_decay[0].T, norm_gain[None],
        forget_gap[None], rec_gain[None], group_weight, pool_gain[None], recurrent_output_weight, w_out_pool,
    )
    extra, gain, gap, r_gain, gmap, pgain = args[6:12]
    (final,) = comm(
        functools.partial(layer_kernel, n_sp, n_fs, n_tp),
        [((rows // n_tp, n_sp * n_fs * cw), BF)],
        [
            buf(BF, n_fs - 1, wr, 2 * ch), buf(BF, n_fs - 1, wr, ch), buf(BF, n_fs - 1, wr, ch), buf(BF, n_fs - 1, wr, ch),
            buf(BF, feats, 2 * ch), buf(BF, feats, ch), buf(BF, feats, ch), buf(BF, feats, ch),
            buf(BF, n_fs, rows, n_tp * half), buf(BF, 2, n_fs // 2 * rows, n_tp * half),
            buf(F32, 2, n_fs // 2 * rows, 2 * ch), buf(F32, 2, n_fs // 2 * rows, ch), buf(F32, 2, n_fs // 2 * rows, ch),
            buf(F32, 2, n_fs // 2 * rows, ch), buf(BF, n_fs, rows, ch), buf(F32, n_fs, rows, ch),
            buf(BF, n_fs, rows // 128, ch, ch), buf(F32, n_fs, rows // 128, 8, ch),
            buf(F32, n_fs, 8, rows), buf(F32, n_fs, 8, rows),
            buf(F32, n_fs, rows, ch), buf(BF, n_fs, rows, ch),
            buf(F32, n_fs, ch, ch), buf(F32, n_fs, 8, ch),
            buf(BF, n_fs, ch, ch), buf(BF, n_fs, ch, ch),
            buf(BF, n_fs, 2**POOL_GROUPS, ch), buf(BF, n_fs, 2**POOL_GROUPS, ch),
            buf(BF, 2, n_tp, n_fs, n_fs * rows, ch),
            buf(F32, n_fs * lanes, 128), buf(F32, n_tp * n_fs, n_fs * lanes, 128),
            buf(BF, n_sp, 2, width, cw), buf(BF, n_half, 2, width, cw),
            buf(BF, n_half * n_fs * n_tp, rows // n_tp, cw), buf(F32, 2, n_fs // 2 * rows, cw),
        ]
        + [buf(a.dtype, *a.shape) for a in (extra, gain, gap, r_gain, gmap, pgain, w_out_pool)]
        + [
            dma(2), dma(4, 2), dma(7), dma(), dma(n_fs, 2), dma(), dma(n_fs),
            dma(4), dma(n_sp, n_fs), dma(3, n_sp), dma(3), dma(4), dma(4), dma(), dma(),
            dma(), dma(n_fs), dma(), dma(), dma(), dma(2, n_fs, 2), dma(), dma(2, 2), dma(), dma(),
            dma(), dma(), dma(n_sp, 2), dma(), dma(n_half, 2), dma(), dma(),
        ],
        1, "layer", [pl.BlockSpec(memory_space=pltpu.HBM)] * len(args), 58,
    )(*args)
    return final[None]


def run(n_sp, n_fs, n_tp, *args):
    wr, width = args[2].shape
    whole = n_fs * wr % 128 == 0 and args[-1].shape[1] % 128 == 0 and args[0].shape[1] % 256 == 0
    return (fused if whole and width == n_fs * HEAD_DIM else body)(n_sp, n_fs, n_tp, *args)


def solution(mesh):
    sizes = dict(mesh.shape)
    weight = P(("sp", "fs"), "tp")
    placed = (
        P("fs", "sp", "tp"), P(), weight, weight, weight, weight, weight, P("tp"),
        P("fs", "sp", "tp"), P("tp"), P(), P("tp"), P("tp", ("sp", "fs")), P("tp", ("sp", "fs")),
    )
    return jax.shard_map(
        functools.partial(run, sizes["sp"], sizes["fs"], sizes["tp"]),
        mesh=mesh, in_specs=placed, out_specs=P("fs", ("sp", "tp"), None), check_vma=False,
    )
```

```python
import functools
import jax
import jax.numpy as jnp
from jax import lax
from jax.experimental import pallas as pl
from jax.experimental.pallas import tpu as pltpu
from jax.sharding import PartitionSpec as P

HEAD_DIM = 128
POOL_GROUPS = 4
BLOCK = 64
EPS = 1e-06
HIGH = lax.Precision.HIGHEST
MESH = pl.DeviceIdType.MESH
BF = jnp.bfloat16
F32 = jnp.float32


def place():
    return lax.axis_index("sp"), lax.axis_index("fs"), lax.axis_index("tp")


def rcopy(src, dst, ssem, rsem, dev):
    return pltpu.make_async_remote_copy(
        src_ref=src, dst_ref=dst, send_sem=ssem, recv_sem=rsem, device_id=dev, device_id_type=MESH
    )


def greet(devs):
    barrier = pltpu.get_barrier_semaphore()
    for cond, dev in devs:
        def tell(dev=dev):
            pl.semaphore_signal(barrier, inc=1, device_id=dev, device_id_type=MESH)
        if cond is None:
            tell()
        else:
            pl.when(cond)(tell)
    pl.semaphore_wait(barrier, sum(1 if cond is None else jnp.where(cond, 1, 0) for cond, _ in devs))


def square(f):
    near = f + 1 - 2 * lax.rem(f, 2)
    return near, lax.rem(f + 2, 4), lax.rem(near + 2, 4)


def project_kernel(
    n_sp, n_fs, n_tp, tok, wq, wf, wi, wo, wp, extra, gain, gmap, pgain, wor, wop, z_ref, e_ref, ow_ref,
    wsrc, xs, ws, acc, x_send, x_recv, f_send, d_send, d_recv, w_send, w_recv, zr_send, zl_send, e_send, e_recv,
):
    s, f, t = place()
    rows, half = tok.shape
    part = rows // 2
    mats = (wq, wf, wi, wo, wp)
    wr, width = wq.shape
    ch = width // n_fs
    for i, w in enumerate(mats):
        for g in range(n_fs):
            wsrc[g, :, i * ch : (i + 1) * ch] = w[:, g * ch : (g + 1) * ch]
    other = (s, f, 1 - t)
    px, py, pd = square(f)
    order = (f, px, py, pd)
    up, down = (s + 1, f, t), (s - 1, f, t)
    has_up, has_down = s < n_sp - 1, s > 0
    greet([(None, other)] + [(None, (s, g, t)) for g in order[1:]] + [(has_up, up), (has_down, down)])

    def cols(c):
        return pl.ds(pl.multiple_of(c * half, half), half)

    def span(a, b):
        return pl.ds(pl.multiple_of((a * n_fs + b) * wr, wr), wr)

    def slot(a, b):
        return ws.at[span(a, b), :]

    def to_up(src, a, b):
        return rcopy(src, slot(a, b), zr_send.at[a, b], w_recv.at[a, b], up)

    def to_down(src, a, b):
        return rcopy(src, slot(a, b), zl_send.at[a, b], w_recv.at[a, b], down)

    sends = []

    def send(c):
        c.start()
        sends.append(c)

    def x_slot(g, h, c):
        return xs.at[g, h * part : (h + 1) * part, cols(c)]

    own = wsrc.at[f]
    pl.when(has_up)(lambda: to_up(own, s, f).start())
    pl.when(has_down)(lambda: to_down(own, s, f).start())
    for i, g in enumerate((pd, px, py)):
        send(rcopy(wsrc.at[g], slot(s, f), w_send.at[i], w_recv.at[s, f], (s, g, t)))
    for i, (p, hs) in enumerate(((px, (0, 1)), (py, (1, 0)))):
        for h in hs:
            send(rcopy(tok.at[h * part : (h + 1) * part, :], x_slot(f, h, t), x_send.at[i, h], x_recv.at[f, h], (s, p, t)))
    for h in range(2):
        send(rcopy(tok.at[h * part : (h + 1) * part, :], x_slot(f, h, t), d_send.at[f, h], d_recv.at[f, h], other))
    for i, g in enumerate(order[1:]):
        send(rcopy(extra.at[g], e_ref.at[f], e_send.at[i], e_recv.at[f], (s, g, t)))
    ws[span(s, f), :] = wsrc[f]
    xs[f, :, cols(t)] = tok[...]
    e_ref[f] = extra[f]
    ow_ref[0:width, :] = wor[...]
    gd = gmap.shape[1]
    for i in range(width // gd):
        at = slice(i * gd, (i + 1) * gd)
        scaled = (gmap[t * (width // gd) + i].astype(F32) * pgain[:, at]).astype(BF)
        folded = jnp.dot(scaled, wop[at, :], preferred_element_type=F32)
        ow_ref[width + i * gd : width + (i + 1) * gd, :] = folded.astype(BF)

    for g in order[1:]:
        to_up(slot(s, g), s, g).wait_recv()
        pl.when(has_up)(lambda: to_up(slot(s, g), s, g).start())
        pl.when(has_down)(lambda: to_down(slot(s, g), s, g).start())

    def landed(g, h):
        here = x_slot(g, h, t)
        rcopy(here, here, d_send.at[g, h], x_recv.at[g, h], other).wait_recv()
        return here

    def hand_on(g, h, here):
        send(rcopy(here, here, d_send.at[g, h], d_recv.at[g, h], other))

    for i, (g, h, onto) in enumerate(((px, 0, py), (py, 1, px))):
        here = landed(g, h)
        send(rcopy(here, here, f_send.at[i], x_recv.at[g, h], (s, onto, t)))
        hand_on(g, h, here)

    def relay(d):
        for g in order:
            a = s - d

            @pl.when(a >= 0)
            def _():
                to_up(slot(a, g), a, g).wait_recv()
                pl.when(has_up)(lambda: to_up(slot(a, g), a, g).start())
            b = s + d

            @pl.when(b < n_sp)
            def _():
                to_down(slot(b, g), b, g).wait_recv()
                pl.when(has_down)(lambda: to_down(slot(b, g), b, g).start())

    def add(a):
        k = pl.ds(pl.multiple_of(a * n_fs * wr, n_fs * wr), n_fs * wr)

        def each(i, _):
            acc[i] += jnp.dot(xs[i, :, k], ws[k, :], preferred_element_type=F32)
            return 0

        lax.fori_loop(0, n_fs, each, 0)

    def multiply(d):
        pl.when(s - d >= 0)(lambda: add(s - d))
        pl.when(s + d < n_sp)(lambda: add(s + d))

    relay(1)
    for g, h in ((px, 1), (py, 0), (pd, 0), (pd, 1)):
        hand_on(g, h, landed(g, h))
    for d in range(2, n_sp - 1):
        relay(d)
    for g in order:
        for h in range(2):
            here = x_slot(g, h, 1 - t)
            rcopy(here, here, d_send.at[g, h], d_recv.at[g, h], other).wait_recv()
    for g in order[1:]:
        rcopy(extra.at[f], e_ref.at[g], e_send.at[0], e_recv.at[g], other).wait_recv()
    for c in sends:
        c.wait_send()

    def norm(j, _):
        tile = 16
        per = rows // tile
        at = (j // per, pl.ds(pl.multiple_of(lax.rem(j, per) * tile, tile), tile))
        feats = xs[at[0], at[1], :].astype(F32)
        scale = lax.rsqrt(jnp.mean(feats * feats, axis=-1, keepdims=True) + EPS)
        xs[at[0], at[1], :] = (feats * scale * gain[...]).astype(BF)
        return 0

    lax.fori_loop(0, n_fs * rows // 16, norm, 0, unroll=2)

    if n_fs * wr % 128 == 0:
        own_k = pl.ds(pl.multiple_of(s * n_fs * wr, n_fs * wr), n_fs * wr)

        def begin(i, _):
            acc[i] = jnp.dot(xs[i, :, own_k], ws[own_k, :], preferred_element_type=F32)
            return 0

        lax.fori_loop(0, n_fs, begin, 0)
        for d in range(1, n_sp - 1):
            multiply(d)
        relay(n_sp - 1)
        multiply(n_sp - 1)

        def finish(i, _):
            z_ref[i] = acc[i].astype(BF)
            return 0
    else:
        relay(n_sp - 1)

        def finish(i, _):
            z_ref[i] = jnp.dot(xs[i], ws[...], preferred_element_type=F32).astype(BF)
            return 0

    lax.fori_loop(0, n_fs, finish, 0)

    for d in range(n_sp):
        for g in order:
            a = s - d

            @pl.when((a >= 0) & has_up)
            def _():
                to_up(slot(a, g), a, g).wait_send()
            b = s + d

            @pl.when((b < n_sp) & has_down)
            def _():
                to_down(slot(b, g), b, g).wait_send()


def dot(a, b, dims):
    return lax.dot_general(a, b, (dims, ((), ())), precision=HIGH, preferred_element_type=F32)


def state_kernel(
    n_sp, group_dim, z, e_all, gap, rec_gain, act, sq_out,
    local, qd, own_st, own_de, st_in, de_in, rim, s_send, s_recv, c_send, c_recv, g_send, g_recv,
):
    s, f, t = place()
    n_fs, rows, _ = z.shape
    ch = HEAD_DIM
    reach = rim.shape[1]
    devs = []
    for d in range(1, n_sp):
        devs.append((s + d < n_sp, (s + d, f, t)))
        devs.append((s - d >= 0, (s - d, f, t)))
    greet(devs)
    edge = rcopy(z.at[:, rows - reach :, 4 * ch :], rim, g_send, g_recv, (s + 1, f, t))
    pl.when(s < n_sp - 1)(edge.start)
    mine = pl.ds(pl.multiple_of(f * ch, ch), ch)
    gap_f = gap[:, mine]
    gain_f = rec_gain[:, mine]
    at = lax.broadcasted_iota(jnp.int32, (BLOCK, BLOCK), 0)
    causal = at >= lax.broadcasted_iota(jnp.int32, (BLOCK, BLOCK), 1)
    lower = causal.astype(F32)

    def one(g, _):
        state = jnp.zeros((ch, ch), F32)
        so_far = jnp.zeros((1, ch), F32)
        e_cols = e_all[g].T
        for n in range(rows // BLOCK):
            here = slice(n * BLOCK, (n + 1) * BLOCK)
            q, fo, v = (z[g, here, i * ch : (i + 1) * ch].astype(F32) for i in range(3))
            q = jax.nn.silu(q)
            k = gap_f * jax.nn.sigmoid(-fo)
            lo = n * BLOCK % 128
            lane = n * BLOCK // 128
            logs = jnp.log1p(-k) + e_cols[lo : lo + BLOCK, lane : lane + 1]
            within = dot(lower, logs, ((1,), (0,)))
            end = within[BLOCK - 1 :]
            q_up = q * jnp.exp(within)
            scores = jnp.where(causal, dot(q_up, k * jnp.exp(-within), ((1,), (1,))), 0.0)
            out = dot(scores, v, ((1,), (0,)))
            if n:
                out = out + dot(q_up, state, ((1,), (1,)))
            local[g, here, :] = out
            qd[g, here, :] = q_up * jnp.exp(so_far)
            state = state * jnp.exp(end) + dot(v.T, k * jnp.exp(end - within), ((1,), (0,)))
            so_far = so_far + end
        own_st[g] = state.astype(BF)
        own_de[g] = jnp.broadcast_to(jnp.exp(so_far), (8, ch))
        return 0

    lax.fori_loop(0, n_fs, one, 0)

    def pair(d):
        dev = (s + d, f, t)
        return (
            rcopy(own_st, st_in.at[d - 1], s_send.at[d - 1], s_recv.at[d - 1], dev),
            rcopy(own_de, de_in.at[d - 1], c_send.at[d - 1], c_recv.at[d - 1], dev),
        )

    for d in range(1, n_sp):
        @pl.when(s + d < n_sp)
        def _():
            for c in pair(d):
                c.start()

        @pl.when(s - d < 0)
        def _():
            st_in[d - 1] = jnp.zeros(st_in.shape[1:], st_in.dtype)
            de_in[d - 1] = jnp.ones(de_in.shape[1:], de_in.dtype)
    pl.when(s == 0)(lambda: rim.__setitem__(Ellipsis, jnp.zeros(rim.shape, rim.dtype)))
    pl.when(s > 0)(edge.wait_recv)
    group = (t * n_fs * ch + f * ch) // group_dim
    spot = s * rows + lax.broadcasted_iota(jnp.int32, (rows, ch), 0)
    window = 2
    for level in range(1, POOL_GROUPS):
        window = jnp.where(group == level, 2 ** (level + 1), window)
    counts = jnp.minimum(spot + 1, window).astype(F32)
    for g in range(n_fs):
        zp = z[g, :, 4 * ch :].astype(F32)
        running = jnp.concatenate([rim[g].astype(F32), zp], axis=0)
        total = None
        for level in range(POOL_GROUPS):
            stride = 2**level
            running = running[stride:] + running[:-stride]
            now = running[running.shape[0] - rows :]
            total = now if level == 0 else jnp.where(group == level, now, total)
        act[1, g * rows : (g + 1) * rows, :] = (total / counts - zp).astype(BF)
    for d in range(1, n_sp):
        @pl.when(s - d >= 0)
        def _():
            for c in pair(d):
                c.wait_recv()

    ones = jnp.ones((8, ch), F32)

    def finish(g, _):
        total = jnp.zeros((ch, ch), F32)
        for d in range(n_sp - 2, -1, -1):
            total = de_in[d, g, 0:1, :] * total + st_in[d, g].astype(F32)
        rec = local[g] + dot(qd[g], total, ((1,), (1,)))
        sums = dot(ones, rec * rec, ((1,), (1,)))
        for i in range(rows // 128):
            sq_out[g, i : i + 1, :] = sums[0:1, i * 128 : (i + 1) * 128]
        gate = jax.nn.silu(z[g, :, 3 * ch : 4 * ch].astype(F32))
        act[0, pl.ds(pl.multiple_of(g * rows, rows), rows), :] = (rec * gain_f * gate).astype(BF)
        return 0

    sq_out[...] = jnp.zeros(sq_out.shape, F32)
    lax.fori_loop(0, n_fs, finish, 0)
    for d in range(1, n_sp):
        @pl.when(s + d < n_sp)
        def _():
            for c in pair(d):
                c.wait_send()
    pl.when(s < n_sp - 1)(edge.wait_send)


def mix_kernel(
    n_sp, n_fs, n_tp, act, sq, ow, final,
    out, acts, sq_all, ow_all, relay_buf, wbuf, part,
    a_send, a_recv, f_send, d_send, d_recv, q_send, q_recv,
    up_send, down_send, o_recv, od_send, od_recv, m_send, m_recv,
):
    s, f, t = place()
    n_half = n_sp // n_tp
    rows = act.shape[1] // n_fs
    half = rows // n_tp
    width, cw = ow.shape[0] // 2, ow.shape[1]
    other = (s, f, 1 - t)
    px, py, pd = square(f)
    up, down = (s + 1, f, t), (s - 1, f, t)
    has_up, has_down = s < n_sp - 1, s > 0
    greet(
        [(None, other)]
        + [(None, (s, g, u)) for g in (px, py, pd) for u in (t, 1 - t)]
        + [(has_up, up), (has_down, down)]
    )

    def to_up(src, a):
        return rcopy(src, relay_buf.at[a], up_send.at[a], o_recv.at[a], up)

    def to_down(src, a):
        return rcopy(src, relay_buf.at[a], down_send.at[a], o_recv.at[a], down)

    def to_other(src, a):
        return rcopy(src, ow_all.at[lax.rem(a, n_half), t], od_send.at[a], od_recv.at[a], other)

    def keep(src, a):
        mine = a // n_half == t

        @pl.when(mine)
        def _():
            ow_all[lax.rem(a, n_half), t] = src[...]

        pl.when(jnp.logical_not(mine))(lambda: to_other(src, a).start())

    sends = []

    def send(c):
        c.start()
        sends.append(c)

    for i, (p, order) in enumerate(((px, (0, 1)), (py, (1, 0)))):
        for h in order:
            send(rcopy(act.at[h], acts.at[t, f, h], a_send.at[i, h], a_recv.at[f, h], (s, p, t)))
    pl.when(has_up)(lambda: to_up(ow, s).start())
    pl.when(has_down)(lambda: to_down(ow, s).start())
    for h in range(2):
        send(rcopy(act.at[h], acts.at[t, f, h], d_send.at[f, h], d_recv.at[f, h], other))
    for i, g in enumerate((px, py, pd)):
        for u in range(n_tp):
            send(rcopy(sq, sq_all.at[t, f], q_send.at[i, u], q_recv.at[t, f], (s, g, u)))
    send(rcopy(sq, sq_all.at[t, f], q_send.at[n_fs - 1, 0], q_recv.at[t, f], other))
    acts[t, f] = act[...]
    sq_all[t, f] = sq[...]
    keep(ow, s)

    def landed(g, h):
        here = acts.at[t, g, h]
        rcopy(here, here, d_send.at[g, h], a_recv.at[g, h], other).wait_recv()
        return here

    def hand_on(g, h, here):
        send(rcopy(here, here, d_send.at[g, h], d_recv.at[g, h], other))

    for i, (g, h, onto) in enumerate(((px, 0, py), (py, 1, px))):
        here = landed(g, h)
        send(rcopy(here, here, f_send.at[i], a_recv.at[g, h], (s, onto, t)))
        hand_on(g, h, here)

    def step(d):
        a = s - d

        @pl.when(a >= 0)
        def _():
            to_up(relay_buf.at[a], a).wait_recv()
            pl.when(has_up)(lambda: to_up(relay_buf.at[a], a).start())
            keep(relay_buf.at[a], a)
        b = s + d

        @pl.when(b < n_sp)
        def _():
            to_down(relay_buf.at[b], b).wait_recv()
            pl.when(has_down)(lambda: to_down(relay_buf.at[b], b).start())
            keep(relay_buf.at[b], b)

    for d in range(1, n_sp):
        step(d)
    for g, h in ((px, 1), (py, 0), (pd, 0), (pd, 1)):
        hand_on(g, h, landed(g, h))
    for i in range(n_half):
        a = t * n_half + i
        here = ow_all.at[i, 1 - t]
        rcopy(here, here, od_send.at[a], od_recv.at[a], other).wait_recv()
    for i in range(n_half):
        for u in range(n_tp):
            for k in range(2):
                wbuf[k, u * width : (u + 1) * width, i * cw : (i + 1) * cw] = ow_all[i, u, k * width : (k + 1) * width, :]
    for g in (px, py, pd):
        for u in range(n_tp):
            here = sq_all.at[u, g]
            rcopy(here, here, q_send.at[0, 0], q_recv.at[u, g], other).wait_recv()
    here = sq_all.at[1 - t, f]
    rcopy(here, here, q_send.at[0, 0], q_recv.at[1 - t, f], other).wait_recv()
    for g in (f, px, py, pd):
        for h in range(2):
            here = acts.at[1 - t, g, h]
            rcopy(here, here, d_send.at[g, h], d_recv.at[g, h], other).wait_recv()

    def piece(g, u):
        return rcopy(part.at[g, u], out.at[f, t], m_send.at[g, u], m_recv.at[f, t], (s, g, u))

    def spread(g):
        for u in range(n_tp):
            c = piece(g, u)
            c.start()
            sends.append(c)

    last = None
    for g in (pd, f, px, py):
        here = pl.ds(pl.multiple_of(g * rows, rows), rows)
        sums = sum(sq_all[u, i, g] for u in range(n_tp) for i in range(n_fs))
        scale = lax.rsqrt(sums / (n_tp * width) + EPS).T
        scale = jnp.concatenate([scale[:, i : i + 1] for i in range(rows // 128)], axis=0)
        left = [
            jnp.concatenate([acts[u, i, h, here, :] for u in range(n_tp) for i in range(n_fs)], axis=1)
            for h in range(2)
        ]
        mixed = (
            jnp.dot(left[0], wbuf[0], preferred_element_type=F32) * scale
            + jnp.dot(left[1], wbuf[1], preferred_element_type=F32)
        ).astype(BF)
        for u in range(n_tp):
            part[g, u] = mixed[u * half : (u + 1) * half]
        if last is not None and last is not f:
            spread(last)
        if last is f:
            c = piece(f, 1 - t)
            c.start()
            sends.append(c)
        last = g
    out[f, t] = part[f, t]
    for i in range(n_half):
        to_other(ow, (1 - t) * n_half + i).wait_send()
    for d in range(n_sp):
        a, b = s - d, s + d

        @pl.when((a >= 0) & has_up)
        def _():
            to_up(ow, a).wait_send()

        @pl.when((b < n_sp) & has_down)
        def _():
            to_down(ow, b).wait_send()
    spread(last)
    for c in sends:
        c.wait_send()
    for g in (px, py, pd):
        for u in range(n_tp):
            here = out.at[g, u]
            rcopy(here, here, m_send.at[g, u], m_recv.at[g, u], other).wait_recv()
    here = out.at[f, 1 - t]
    rcopy(here, here, m_send.at[f, 1 - t], m_recv.at[f, 1 - t], other).wait_recv()
    for u in range(n_tp):
        for i in range(n_half):
            for g in range(n_fs):
                lo = ((u * n_half + i) * n_fs + g) * cw
                final[:, lo : lo + cw] = out[g, u, :, i * cw : (i + 1) * cw]


def vmem(count):
    return [pl.BlockSpec(memory_space=pltpu.VMEM)] * count


def dma(*shape):
    return pltpu.SemaphoreType.DMA(shape) if shape else pltpu.SemaphoreType.DMA


def comm(kernel, outs, scratch, number, name, ins=None, limit=60):
    return pl.pallas_call(
        kernel,
        out_shape=[jax.ShapeDtypeStruct(a, b) if ins is None else pltpu.VMEM(a, b) for a, b in outs],
        **({"out_specs": vmem(len(outs))} if ins is None else {"in_specs": ins, "out_specs": [pl.BlockSpec(memory_space=pltpu.VMEM)] * len(outs)}),
        scratch_shapes=scratch,
        compiler_params=pltpu.CompilerParams(
            collective_id=number, has_side_effects=True, vmem_limit_bytes=limit * 1024 * 1024
        ),
        name=name,
    )


def body(
    n_sp, n_fs, n_tp, tokens, norm_gain, w_query, forget_weight, w_input, w_outgate, w_pool, forget_gap,
    extra_decay, rec_gain, group_weight, pool_gain, recurrent_output_weight, w_out_pool,
):
    s, f, t = place()
    rows, half = tokens.shape[1:]
    width = w_query.shape[1]
    ch = width // n_fs
    n_w = 5
    wr = w_query.shape[0]
    lanes = rows // 128
    extra = jnp.pad(extra_decay[0].T.reshape(n_fs, lanes, 128), ((0, 0), (0, 8 - lanes), (0, 0)))
    cw = w_out_pool.shape[1]
    z, e_all, ow = comm(
        functools.partial(project_kernel, n_sp, n_fs, n_tp),
        [((n_fs, rows, n_w * ch), BF), ((n_fs, 8, 128), F32), ((2 * width, cw), BF)],
        [
            pltpu.VMEM((n_fs, wr, n_w * ch), BF), pltpu.VMEM((n_fs, rows, n_tp * half), BF),
            pltpu.VMEM((n_sp * n_fs * wr, n_w * ch), BF), pltpu.VMEM((n_fs, rows, n_w * ch), F32),
            dma(2, 2), dma(n_fs, 2), dma(2), dma(n_fs, 2), dma(n_fs, 2), dma(n_fs - 1), dma(n_sp, n_fs),
            dma(n_sp, n_fs), dma(n_sp, n_fs), dma(n_fs - 1), dma(n_fs),
        ],
        1, "project",
    )(
        tokens[0], w_query, forget_weight, w_input, w_outgate, w_pool, extra, norm_gain[None],
        group_weight, pool_gain[None], recurrent_output_weight, w_out_pool,
    )
    n_half = n_sp // n_tp
    act, sq = comm(
        functools.partial(state_kernel, n_sp, group_weight.shape[1]),
        [((2, n_fs * rows, ch), BF), ((n_fs, 8, 128), F32)],
        [
            pltpu.VMEM((n_fs, rows, ch), F32), pltpu.VMEM((n_fs, rows, ch), F32),
            pltpu.VMEM((n_fs, ch, ch), BF), pltpu.VMEM((n_fs, 8, ch), F32),
            pltpu.VMEM((n_sp - 1, n_fs, ch, ch), BF), pltpu.VMEM((n_sp - 1, n_fs, 8, ch), F32),
            pltpu.VMEM((n_fs, 2**POOL_GROUPS, ch), BF),
            dma(n_sp - 1), dma(n_sp - 1), dma(n_sp - 1), dma(n_sp - 1), dma(), dma(),
        ],
        2, "state",
    )(z, e_all, forget_gap[None], rec_gain[None])
    out_shape = (n_fs, n_tp, rows // n_tp, n_half * cw)
    (final,) = comm(
        functools.partial(mix_kernel, n_sp, n_fs, n_tp),
        [((rows // n_tp, n_tp * n_half * n_fs * cw), BF)],
        [
            pltpu.VMEM(out_shape, BF), pltpu.VMEM((n_tp, n_fs) + act.shape, BF), pltpu.VMEM((n_tp, n_fs) + sq.shape, F32),
            pltpu.VMEM((n_half, n_tp) + ow.shape, BF), pltpu.VMEM((n_sp,) + ow.shape, BF),
            pltpu.VMEM((2, n_tp * width, n_half * cw), BF), pltpu.VMEM(out_shape, BF),
            dma(2, 2), dma(n_fs, 2), dma(2), dma(n_fs, 2), dma(n_fs, 2), dma(n_fs, n_tp), dma(n_tp, n_fs),
            dma(n_sp), dma(n_sp), dma(n_sp), dma(n_sp), dma(n_sp), dma(n_fs, n_tp), dma(n_fs, n_tp),
        ],
        3, "mix",
    )(act, sq, ow)
    return final[None]


def mm(a, b, dims):
    return lax.dot_general(a, b, (dims, ((), ())), preferred_element_type=F32)


NN, NT, TN = ((1,), (0,)), ((1,), (1,)), ((0,), (0,))


def layer_kernel(
    n_sp, n_fs, n_tp, tok, wq, wf, wi, wo, wp, extra_in, gain_in, gap_in, rec_gain_in, gmap_in, pgain_in, wor, wop_in, final,
    src0, src1, src2, src3, ws0, ws1, ws2, ws3, xs, xn, acc0, acc1, acc2, acc3, k_buf, rel, st_buf, lead, e_src, e_all, local, qd, own_st, own_de,
    t_out, t_in, rim_src, rim, acts, sq_src, sq_all, ow_buf, ow_oth, part, half_way,
    extra, gain, gap, rec_gain, gmap, pgain, wop,
    in_sem, w_in, p_in, x_send, x_recv, xd_send, xd_recv, w_send, w_recv, b_recv, ba_recv, up_send, dn_send, e_send, e_recv,
    t_send, t_recv, g_send, g_recv, a_send, a_recv, ad_send, ad_recv, q_send, q_recv,
    ou_send, on_send, o_recv, od_send, od_recv, m_send, m_recv, ready,
):
    s, f, t = place()
    rows, half = tok.shape
    cut = rows // 2
    wr, width = wq.shape
    ch = width // n_fs
    cw = wor.shape[1]
    n_half = n_sp // n_tp
    out_rows = rows // n_tp
    lanes = rows // 128
    size = 128
    blk = n_fs * wr
    total_k = n_sp * blk
    groups = ((wf, wi), (wp,), (wo,), (wq,))
    srcs, wss, accs = (src0, src1, src2, src3), (ws0, ws1, ws2, ws3), (acc0, acc1, acc2, acc3)
    other = (s, f, 1 - t)
    px, py, pd = square(f)
    order = (f, px, py, pd)
    up, down = (s + 1, f, t), (s - 1, f, t)
    has_up, has_down = s < n_sp - 1, s > 0
    is_end = jnp.logical_not(has_up & has_down)

    def when(cond, *copies):
        @pl.when(cond)
        def _():
            for c in copies:
                c.start()

    def sent(ref, sem):
        rcopy(ref, ref, sem, sem, other).wait_send()

    def came(ref, sem):
        rcopy(ref, ref, sem, sem, other).wait_recv()

    def cols(c):
        return pl.ds(pl.multiple_of(c * half, half), half)

    def span(a, b):
        return pl.ds(pl.multiple_of((a * n_fs + b) * wr, wr), wr)

    def slot(c, a, b):
        return wss[c].at[span(a, b), :]

    def block(c, a):
        return wss[c].at[pl.ds(pl.multiple_of(a * blk, blk), blk), :]

    def x_slot(g, h, c):
        return xs.at[g, h * cut : (h + 1) * cut, cols(c)]

    peers = (
        [(None, other)]
        + [(None, (s, px, t)), (None, (s, py, t))]
        + [(has_up, up), (has_down, down)]
    )
    barrier = pltpu.get_barrier_semaphore()
    for cond, dev in peers:
        def tell(dev=dev):
            pl.semaphore_signal(barrier, inc=1, device_id=dev, device_id_type=MESH)
        if cond is None:
            tell()
        else:
            pl.when(cond)(tell)
    for c in (1, 0, 3, 2):
        for i, w in enumerate(groups[c]):
            for j, g in enumerate(order):
                lane = pl.ds(pl.multiple_of(g * ch, ch), ch)
                into = wss[c].at[span(s, f), i * ch : (i + 1) * ch] if j == 0 else srcs[c].at[j - 1, :, i * ch : (i + 1) * ch]
                pltpu.make_async_copy(w.at[:, lane], into, w_in.at[c, min(j, 1)]).start()
        if c == 0:
            pltpu.make_async_copy(tok, xs.at[f, :, cols(t)], in_sem.at[0]).start()
            pltpu.make_async_copy(wor, ow_buf.at[s, 0], in_sem.at[1]).start()
    params = ((extra_in, extra), (gain_in, gain), (gmap_in, gmap), (pgain_in, pgain), (wop_in, wop), (gap_in, gap), (rec_gain_in, rec_gain))
    loads = [pltpu.make_async_copy(a, b, p_in.at[i]) for i, (a, b) in enumerate(params)]
    for c in loads:
        c.start()
    pl.semaphore_wait(barrier, sum(1 if cond is None else jnp.where(cond, 1, 0) for cond, _ in peers))

    def took(ref, sem):
        pltpu.make_async_copy(ref, ref, sem).wait()

    def to_up(src, b, a):
        return rcopy(src, slot(0, a, b), up_send.at[0], w_recv.at[a, b], up)

    def to_down(src, b, a):
        return rcopy(src, slot(0, a, b), dn_send.at[0], w_recv.at[a, b], down)

    def both(a, b):
        when(has_up, to_up(slot(0, a, b), b, a))
        when(has_down, to_down(slot(0, a, b), b, a))

    def b_up(c, a):
        return rcopy(block(c, a), block(c, a), up_send.at[c], b_recv.at[c - 1, a], up)

    def b_down(c, a):
        return rcopy(block(c, a), block(c, a), dn_send.at[c], b_recv.at[c - 1, a], down)

    def spread(c, some=(0, 1, 2)):
        for j in some:
            g = order[1 + j]
            rsem = w_recv.at[s, f] if c == 0 else ba_recv.at[c - 1]
            rcopy(srcs[c].at[j], slot(c, s, f), w_send.at[c], rsem, (s, g, t)).start()

    def chunk(c, g, dev):
        here = slot(c, s, g)
        return rcopy(here, here, (up_send if dev is up else dn_send).at[c], b_recv.at[c - 1, s], dev)

    def own_wait(c):
        came(wss[c].at[0 : (n_fs - 1) * wr, :], ba_recv.at[c - 1])

    def own_up(c, cond=True):
        when(has_up & cond, *(chunk(c, g, up) for g in order[1:]))

    def own_down(c, cond=True):
        when(has_down & cond, *(chunk(c, g, down) for g in order[1:]))

    low = 2 * s < n_sp
    inner = jnp.logical_not(is_end)
    mid_low = inner & low
    mid_high = inner & jnp.logical_not(low)

    def relay(c, d, gs=(None,), inward=True, outward=True):
        a, b = s - d, s + d

        def rising(extra):
            for g in gs:
                @pl.when((a >= 0) & has_up & extra)
                def _():
                    hop = to_up(slot(0, a, g), g, a) if c == 0 else b_up(c, a)
                    hop.wait_recv()
                    hop.start()

        def falling(extra):
            for g in gs:
                @pl.when((b < n_sp) & has_down & extra)
                def _():
                    hop = to_down(slot(0, b, g), g, b) if c == 0 else b_down(c, b)
                    hop.wait_recv()
                    hop.start()

        if inward:
            rising(low)
            falling(jnp.logical_not(low))
        if outward:
            falling(low)
            rising(jnp.logical_not(low))

    def arrive(c, d):
        for g in order if c == 0 else (None,):
            a, b = s - d, s + d

            @pl.when((a >= 0) & jnp.logical_not(has_up))
            def _():
                (to_up(slot(0, a, g), g, a) if c == 0 else b_up(c, a)).wait_recv()

            @pl.when((b < n_sp) & jnp.logical_not(has_down))
            def _():
                (to_down(slot(0, b, g), g, b) if c == 0 else b_down(c, b)).wait_recv()

    near = pl.ds(pl.multiple_of(jnp.where(has_down, blk, 0), blk), total_k - blk)
    far = pl.ds(pl.multiple_of(jnp.where(has_down, 0, total_k - blk), blk), blk)

    def gemm(c, p, k, more):
        out = jnp.dot(xn[p, :, k], wss[c][k, :], preferred_element_type=F32)
        accs[c][p] = accs[c][p] + out if more else out

    def main(c, p):
        pl.when(is_end)(lambda: gemm(c, p, near, False))
        pl.when(jnp.logical_not(is_end))(lambda: gemm(c, p, slice(0, total_k), False))

    def each_pair(step):
        def one(p, _):
            step(p)
            return 0

        lax.fori_loop(0, 2, one, 0)

    def last(c):
        arrive(c, n_sp - 1)
        pl.when(is_end)(lambda: each_pair(lambda p: gemm(c, p, far, True)))

    def landed(g, h):
        here = x_slot(g, h, t)
        came(here, x_recv.at[g, h])
        return here

    def hand_on(g, h):
        here = x_slot(g, h, t)
        rcopy(here, here, xd_send, xd_recv.at[g], other).start()

    def norm(j):
        g = order[j]
        came(xs.at[g, :, cols(1 - t)], xd_recv.at[g])
        tile = 16

        def each(i, _):
            at = pl.ds(pl.multiple_of(i * tile, tile), tile)
            feats = xs[g, at, :].astype(F32)
            scale = lax.rsqrt(jnp.mean(feats * feats, axis=-1, keepdims=True) + EPS)
            to = pl.ds(pl.multiple_of((j % 2) * rows + i * tile, tile), tile)
            xn[j // 2, to, :] = (feats * scale * gain[...]).astype(BF)
            return 0

        lax.fori_loop(0, rows // tile, each, 0, unroll=2)

    def ow_up(a, k):
        return rcopy(ow_buf.at[a, k], ow_buf.at[a, k], ou_send, o_recv.at[a, k], up)

    def ow_down(a, k):
        return rcopy(ow_buf.at[a, k], ow_buf.at[a, k], on_send, o_recv.at[a, k], down)

    def ow_share(a, k):
        i = lax.rem(a, n_half)
        when(a // n_half != t, rcopy(ow_buf.at[a, k], ow_oth.at[i, k], od_send, od_recv.at[i, k], other))

    def ow_start(a, k, rise, cond=True):
        to, has, edge_at = (s + 1, has_up, n_sp - 1) if rise else (s - 1, has_down, 0)
        ssem = ou_send if rise else on_send
        across = (to == edge_at) & (a // n_half != t)
        i = lax.rem(a, n_half)
        when(has & cond & jnp.logical_not(across), (ow_up if rise else ow_down)(a, k))
        when(has & cond & across, rcopy(ow_buf.at[a, k], ow_oth.at[i, k], ssem, od_recv.at[i, k], (to, f, 1 - t)))

    def ow_rise(d, k, cond=True):
        a = s - d

        @pl.when((a >= 0) & has_up & cond)
        def _():
            ow_up(a, k).wait_recv()
            ow_start(a, k, True)
            ow_share(a, k)

    def ow_fall(d, k, cond=True):
        b = s + d

        @pl.when((b < n_sp) & has_down & cond)
        def _():
            ow_down(b, k).wait_recv()
            ow_start(b, k, False)
            ow_share(b, k)

    def ow_relay(d, k):
        ow_rise(d, k)
        ow_fall(d, k)

    def ow_take(d, k):
        a, b = s - d, s + d
        pl.when((a >= 0) & jnp.logical_not(has_up) & (a // n_half == t))(ow_up(a, k).wait_recv)
        pl.when((b < n_sp) & jnp.logical_not(has_down) & (b // n_half == t))(ow_down(b, k).wait_recv)

    pl.semaphore_signal(ready, inc=1, device_id=(s, px, t), device_id_type=MESH)
    took(slot(1, s, f), w_in.at[1, 0])
    when(has_up, chunk(1, f, up))
    when(has_down, chunk(1, f, down))
    took(srcs[1], w_in.at[1, 1])
    spread(1, (0, 1))
    took(slot(0, s, f), w_in.at[0, 0])
    both(s, f)
    took(srcs[0], w_in.at[0, 1])
    spread(0, (0, 1))
    for c in (3, 2):
        took(slot(c, s, f), w_in.at[c, 0])
        when(has_up, chunk(c, f, up))
        when(has_down, chunk(c, f, down))
    pl.semaphore_wait(ready, 1)
    spread(1, (2,))
    spread(0, (2,))
    took(xs.at[f, :, cols(t)], in_sem.at[0])
    for p, hs in ((px, (0, 1)), (py, (1, 0))):
        for h in hs:
            rcopy(x_slot(f, h, t), x_slot(f, h, t), x_send, x_recv.at[f, h], (s, p, t)).start()
    for h in range(2):
        hand_on(f, h)
    for c in loads:
        c.wait()
    for g in range(n_fs):
        e_src[g] = jnp.broadcast_to(extra[g : g + 1, :], e_src.shape[1:])
    for g in order[1:]:
        rcopy(e_src.at[g], e_all.at[f], e_send, e_recv, (s, g, t)).start()
    for c in (3, 2):
        took(srcs[c], w_in.at[c, 1])
        spread(c)
    e_all[f] = e_src[f]
    own_wait(1)
    own_up(1)
    own_down(1)
    for g in order[1:]:
        came(slot(0, s, g), w_recv.at[s, g])
        both(s, g)
    gd = gmap.shape[1]
    for i in range(width // gd):
        at = slice(i * gd, (i + 1) * gd)
        scaled = (gmap[t * (width // gd) + i].astype(F32) * pgain[:, at]).astype(BF)
        ow_buf[s, 1, at, :] = jnp.dot(scaled, wop[at, :], preferred_element_type=F32).astype(BF)
    norm(0)
    relay(1, 1)
    relay(0, 1, order[:2])
    for g, h, onto in ((px, 0, py), (py, 1, px)):
        here = landed(g, h)
        rcopy(here, here, x_send, x_recv.at[g, h], (s, onto, t)).start()
        hand_on(g, h)
    for d in range(2, n_sp - 1):
        relay(1, d)
    relay(0, 1, order[2:])
    for g, h in ((px, 1), (py, 0)):
        landed(g, h)
        hand_on(g, h)
    for d in range(2, n_sp - 1):
        relay(0, d, order[:2])
    norm(1)
    for c in (3, 2):
        own_wait(c)
        own_up(c, is_end)
        own_down(c, is_end)
    took(ow_buf.at[s, 0], in_sem.at[1])
    for k in range(2):
        ow_start(s, k, True, is_end)
        ow_start(s, k, False, is_end)
        ow_share(s, k)
    norm(2)
    for d in range(1, n_sp):
        arrive(1, d)
    gemm(1, 0, slice(0, total_k), False)
    for d in range(2, n_sp - 1):
        relay(0, d, order[2:])
    own_up(3, inner)
    own_down(3, inner)
    for h in range(2):
        landed(pd, h)
        hand_on(pd, h)
    norm(3)
    gemm(1, 1, slice(0, total_k), False)

    reach = rim.shape[1]
    edge = rcopy(rim_src, rim, g_send, g_recv, up)

    def send_rim():
        for j in range(n_fs):
            rim_src[j] = acc1[j // 2, (j % 2 + 1) * rows - reach : (j % 2 + 1) * rows, :].astype(BF)
        when(has_up, edge)

    send_rim()
    relay(3, 1)
    own_up(2, mid_low)
    own_down(2, mid_high)
    for d in range(1, n_sp - 1):
        arrive(0, d)
    each_pair(lambda p: main(0, p))
    def chain():
        for g in range(n_fs):
            carry(g).wait_recv()
            t_out[g] = (own_st[g] + t_in[g].astype(F32) * own_de[g, 0:1, :]).astype(BF)
            carry(g).start()

    group = (t * n_fs * ch + f * ch) // gd
    spot = s * rows + lax.broadcasted_iota(jnp.int32, (rows, ch), 0)
    window = 2
    for level in range(1, POOL_GROUPS):
        window = jnp.where(group == level, 2 ** (level + 1), window)
    share = 1.0 / jnp.minimum(spot + 1, window).astype(F32)

    def rows_of(g):
        return pl.ds(pl.multiple_of(g * rows, rows), rows)

    def pool(j):
        zp = acc1[j // 2, j % 2 * rows : (j % 2 + 1) * rows, :].astype(BF).astype(F32)
        running = jnp.concatenate([rim[j].astype(F32), zp], axis=0)
        total = None
        for level in range(POOL_GROUPS):
            stride = 2**level
            running = running[stride:] + running[:-stride]
            now = running[running.shape[0] - rows :]
            total = now if level == 0 else jnp.where(group == level, now, total)
        acts[1, t, f, rows_of(order[j]), :] = (total * share - zp).astype(BF)

    part_rows = n_fs * rows // 2
    quarter = part_rows // 2

    def a_slot(k, u, g, h, q=None):
        lo, n = (h * part_rows, part_rows) if q is None else (h * part_rows + q * quarter, quarter)
        return acts.at[k, u, g, lo : lo + n, :]

    def a_share(k, g, h):
        here = a_slot(k, t, g, h)
        rcopy(here, here, ad_send, ad_recv.at[k, h], other).start()

    def publish(k):
        for h in range(2):
            here = a_slot(k, t, f, h)
            for p in (px, py):
                rcopy(here, here, a_send, a_recv.at[k, f, h], (s, p, t)).start()
            a_share(k, f, h)

    def a_forward(k, h):
        for g, q, onto in ((px, 0, py), (py, 1, px)):
            came(a_slot(k, t, g, h), a_recv.at[k, g, h])
            here = a_slot(k, t, g, h, q)
            rcopy(here, here, a_send, a_recv.at[k, g, h], (s, onto, t)).start()
            a_share(k, g, h)

    def a_rest(k, h):
        came(a_slot(k, t, pd, h), a_recv.at[k, pd, h])
        a_share(k, pd, h)

    def a_other(k, h):
        came(acts.at[k, 1 - t, :, h * part_rows : (h + 1) * part_rows, :], ad_recv.at[k, h])

    def pool_all():
        pl.when(has_down)(edge.wait_recv)
        for j in range(n_fs):
            pool(j)
        publish(1)

    @pl.when(jnp.logical_not(has_down))
    def _():
        rim[...] = jnp.zeros(rim.shape, BF)

    pool_all()
    last(0)
    came(e_all.at[0 : n_fs - 1], e_recv)

    mine = pl.ds(pl.multiple_of(f * ch, ch), ch)
    gap_f = gap[:, mine]
    gain_f = rec_gain[:, mine]
    at = lax.broadcasted_iota(jnp.int32, (size, size), 0)
    causal = at >= lax.broadcasted_iota(jnp.int32, (size, size), 1)
    lower = jnp.where(causal, 1.0, 0.0).astype(BF)
    lower = jnp.concatenate([lower, lower], axis=1)

    steps = rows // size

    def spots(j, n):
        lo = j % 2 * rows + n * size
        return slice(n * size, (n + 1) * size), slice(lo, lo + size)

    def states(j):
        state = None
        so_far = jnp.zeros((1, ch), F32)
        e_cols = e_all[order[j]].T
        for n in range(steps):
            here, there = spots(j, n)
            v = acc0[j // 2, there, ch : 2 * ch].astype(BF)
            k = gap_f * jax.nn.sigmoid(-acc0[j // 2, there, 0:ch].astype(BF).astype(F32))
            logs = jnp.log1p(-k) + e_cols[here, 0:1]
            high = logs.astype(BF)
            low = (logs - high.astype(F32)).astype(BF)
            within = mm(lower, jnp.concatenate([high, low], axis=0), NN)
            mid = within[size // 2 - 1 : size // 2]
            end = within[size - 1 :]
            k = (k * jnp.exp(mid - within)).astype(BF)
            k_buf[j, here, :] = k
            rel[j, here, :] = within - mid
            lead[j, n] = jnp.broadcast_to(jnp.exp(mid + so_far), lead.shape[2:])
            fresh = mm(v, k, TN) * jnp.exp(end - mid)
            if n:
                st_buf[j, n - 1] = (state * jnp.exp(mid)).astype(BF)
            state = state * jnp.exp(end) + fresh if n else fresh
            so_far = so_far + end
        own_st[j] = state
        own_de[j] = jnp.broadcast_to(jnp.exp(so_far), own_de.shape[1:])

    def reads(j):
        for n in range(steps):
            here, there = spots(j, n)
            v = acc0[j // 2, there, ch : 2 * ch].astype(BF)
            q = jax.nn.silu(acc3[j // 2, there, :].astype(BF).astype(F32)) * jnp.exp(rel[j, here, :])
            q_up = q.astype(BF)
            scores = jnp.where(causal, mm(q_up, k_buf[j, here, :], NT), 0.0).astype(BF)
            out = mm(scores, v, NN)
            if n:
                out = out + mm(q_up, st_buf[j, n - 1], NT)
            local[j, here, :] = out
            qd[j, here, :] = (q * lead[j, n, 0:1, :]).astype(BF)

    def carry(g):
        return rcopy(t_out.at[g], t_in.at[g], t_send, t_recv.at[g], up)

    for j in range(n_fs):
        states(j)

        @pl.when(jnp.logical_not(has_down))
        def _():
            t_in[j] = jnp.zeros(t_in.shape[1:], BF)
            t_out[j] = own_st[j].astype(BF)
            carry(j).start()

    for d in range(2, n_sp - 1):
        relay(3, d)
    own_up(2, mid_high)
    own_down(2, mid_low)
    relay(2, 1, outward=False)
    for d in range(1, n_sp - 1):
        arrive(3, d)
    each_pair(lambda p: main(3, p))
    last(3)
    for j in range(n_fs):
        reads(j)
    pl.when(mid_low)(chain)
    relay(2, 1, inward=False)
    for d in range(2, n_sp - 1):
        relay(2, d)
    for k in range(2):
        ow_start(s, k, False, inner)
    a_forward(1, 0)
    pl.when(mid_high)(chain)
    for k in range(2):
        ow_start(s, k, True, inner)
        ow_rise(1, k, mid_low)
        ow_fall(1, k, mid_high)
    pl.when(inner)(lambda: each_pair(lambda p: gemm(2, p, slice(0, total_k), False)))
    a_forward(1, 1)
    ones = jnp.ones((8, ch), BF)

    def finish(j):
        g = order[j]
        rec = local[j] + mm(qd[j], t_in[j], NT)
        sums = mm(ones, (rec * rec).astype(BF), NT)
        for i in range(lanes):
            sq_src[pl.ds(g * lanes + i, 1), :] = sums[0:1, i * 128 : (i + 1) * 128]
        gate = jax.nn.silu(acc2[j // 2, j % 2 * rows : (j % 2 + 1) * rows, :].astype(BF).astype(F32))
        acts[0, t, f, rows_of(g), :] = (rec * gain_f * gate).astype(BF)

    def finish_all():
        for j in range(n_fs):
            finish(j)
        for u, g in [(1 - t, f)] + [(u, g) for g in order[1:] for u in (t, 1 - t)]:
            rcopy(sq_src, sq_all.at[t * n_fs + f], q_send, q_recv, (s, g, u)).start()
        publish(0)
        sq_all[t * n_fs + f] = sq_src[...]

    pl.when(inner)(finish_all)
    for k in range(2):
        ow_rise(1, k, mid_high)
    pl.when(inner)(lambda: a_forward(0, 0))
    for k in range(2):
        ow_fall(1, k, mid_low)
    pl.when(inner)(lambda: a_forward(0, 1))
    for d in range(1, n_sp - 1):
        arrive(2, d)
    pl.when(is_end)(lambda: each_pair(lambda p: gemm(2, p, near, False)))
    last(2)
    @pl.when(has_down & jnp.logical_not(has_up))
    def _():
        for g in range(n_fs):
            carry(g).wait_recv()

    pl.when(is_end)(finish_all)
    for d in range(2, n_sp - 1):
        ow_relay(d, 0)
    for h in range(2):
        a_rest(1, h)
    for d in range(2, n_sp - 1):
        ow_relay(d, 1)
    pl.when(is_end)(lambda: a_forward(0, 0))
    pl.when(is_end)(lambda: a_forward(0, 1))
    for d in range(1, n_sp - 1):
        for k in range(2):
            ow_take(d, k)
    came(sq_all.at[0 : n_tp * n_fs - 1], q_recv)
    sums = sum(sq_all[i] for i in range(n_tp * n_fs))
    scale = lax.rsqrt(sums / (n_tp * width) + EPS).T
    half_lanes = n_fs * lanes // 2
    scales = [
        jnp.concatenate([scale[:, h * half_lanes + i : h * half_lanes + i + 1] for i in range(half_lanes)], axis=0)
        for h in range(2)
    ]
    late = s - t * n_half >= n_half - 1

    def spot_of(a, g):
        return pl.ds(pl.multiple_of((a * n_fs + g) * cw, cw), cw)

    def at_part(i, g, u):
        return (i * n_fs + g) * n_tp + u

    def piece(i, g, u):
        return rcopy(part.at[at_part(i, g, u)], final.at[:, spot_of(t * n_half + i, f)], m_send, m_recv, (s, g, u))

    def weight_side(k, a, i, h):
        here = slice(h * part_rows, (h + 1) * part_rows)
        total = None
        for u, w in ((t, ow_buf.at[a, k]), (1 - t, ow_oth.at[i, k])):
            left = jnp.concatenate([acts[k, u, b, here, :] for b in range(n_fs)], axis=1)
            now = jnp.dot(left, w[...], preferred_element_type=F32)
            total = now if total is None else total + now
        return total

    def rec_side(a, i, h):
        half_way[h] = weight_side(0, a, i, h) * scales[h]

    def pool_side(a, i, h):
        mixed = (half_way[h] + weight_side(1, a, i, h)).astype(BF)
        for g in range(h * n_fs // 2, (h + 1) * n_fs // 2):
            for u in range(n_tp):
                lo = (g * n_tp + u) * out_rows - h * part_rows
                part[at_part(i, g, u)] = mixed[lo : lo + out_rows]
                when((g != f) | (u != t), piece(i, g, u))

    def ow_got(j, k):
        i = jnp.where(late, n_half - 1 - j, j)
        if j == n_half - 1:
            ow_take(n_sp - 1, k)
        came(ow_oth.at[i, k], od_recv.at[i, k])
        return t * n_half + i, i

    owns = []
    for j in range(n_half):
        if j == 0:
            for k in range(2):
                a, i = ow_got(0, k)
            for h in range(2):
                a_rest(0, h)
                for k in range(2):
                    a_other(k, h)
                rec_side(a, i, h)
                pool_side(a, i, h)
        else:
            a, i = ow_got(j, 0)
            for h in range(2):
                rec_side(a, i, h)
            a, i = ow_got(j, 1)
            for h in range(2):
                pool_side(a, i, h)
        own = pltpu.make_async_copy(part.at[at_part(i, f, t)], final.at[:, spot_of(a, f)], in_sem.at[min(j, 1)])
        own.start()
        owns.append(own)

    pieces = part.at[0 : n_half * (n_tp * n_fs - 1)]
    came(pieces, m_recv)
    for own in owns:
        own.wait()
    sent(pieces, m_send)
    sent(xs.at[0:3, :, 0:half], x_send)
    sent(xs.at[:, :, 0:half], xd_send)
    sent(e_src.at[0 : n_fs - 1], e_send)
    for c in range(4):
        sent(srcs[c], w_send.at[c])
    sent(acts.at[:, 0, 0:3], a_send)
    sent(acts.at[:, 0], ad_send)
    sent(sq_all.at[0 : n_tp * n_fs - 1], q_send)
    pl.when(jnp.logical_not(is_end))(lambda: sent(ow_oth, od_send))
    pl.when(is_end & (s // n_half != t))(lambda: sent(ow_oth.at[0], od_send))
    for v in range(n_sp):
        @pl.when(s == v)
        def _():
            if v < n_sp - 1:
                for c in range(4):
                    sent(wss[c].at[0 : (v + 1) * blk, :], up_send.at[c])
                sent(ow_buf.at[0 : v + 1], ou_send)
                sent(rim_src, g_send)
                sent(t_out, t_send)
            if v > 0:
                for c in range(4):
                    sent(wss[c].at[0 : (n_sp - v) * blk, :], dn_send.at[c])
                sent(ow_buf.at[0 : n_sp - v], on_send)


def fused(
    n_sp, n_fs, n_tp, tokens, norm_gain, w_query, forget_weight, w_input, w_outgate, w_pool, forget_gap,
    extra_decay, rec_gain, group_weight, pool_gain, recurrent_output_weight, w_out_pool,
):
    rows, half = tokens.shape[1:]
    wr, width = w_query.shape
    ch = width // n_fs
    cw = w_out_pool.shape[1]
    n_half = n_sp // n_tp
    feats = n_sp * n_fs * wr
    lanes = rows // 128

    def buf(kind, *shape):
        return pltpu.VMEM(shape, kind)

    args = (
        tokens[0], w_query, forget_weight, w_input, w_outgate, w_pool, extra_decay[0].T, norm_gain[None],
        forget_gap[None], rec_gain[None], group_weight, pool_gain[None], recurrent_output_weight, w_out_pool,
    )
    extra, gain, gap, r_gain, gmap, pgain = args[6:12]
    (final,) = comm(
        functools.partial(layer_kernel, n_sp, n_fs, n_tp),
        [((rows // n_tp, n_sp * n_fs * cw), BF)],
        [
            buf(BF, n_fs - 1, wr, 2 * ch), buf(BF, n_fs - 1, wr, ch), buf(BF, n_fs - 1, wr, ch), buf(BF, n_fs - 1, wr, ch),
            buf(BF, feats, 2 * ch), buf(BF, feats, ch), buf(BF, feats, ch), buf(BF, feats, ch),
            buf(BF, n_fs, rows, n_tp * half), buf(BF, 2, n_fs // 2 * rows, n_tp * half),
            buf(F32, 2, n_fs // 2 * rows, 2 * ch), buf(F32, 2, n_fs // 2 * rows, ch), buf(F32, 2, n_fs // 2 * rows, ch),
            buf(F32, 2, n_fs // 2 * rows, ch), buf(BF, n_fs, rows, ch), buf(F32, n_fs, rows, ch),
            buf(BF, n_fs, rows // 128, ch, ch), buf(F32, n_fs, rows // 128, 8, ch),
            buf(F32, n_fs, 8, rows), buf(F32, n_fs, 8, rows),
            buf(F32, n_fs, rows, ch), buf(BF, n_fs, rows, ch),
            buf(F32, n_fs, ch, ch), buf(F32, n_fs, 8, ch),
            buf(BF, n_fs, ch, ch), buf(BF, n_fs, ch, ch),
            buf(BF, n_fs, 2**POOL_GROUPS, ch), buf(BF, n_fs, 2**POOL_GROUPS, ch),
            buf(BF, 2, n_tp, n_fs, n_fs * rows, ch),
            buf(F32, n_fs * lanes, 128), buf(F32, n_tp * n_fs, n_fs * lanes, 128),
            buf(BF, n_sp, 2, width, cw), buf(BF, n_half, 2, width, cw),
            buf(BF, n_half * n_fs * n_tp, rows // n_tp, cw), buf(F32, 2, n_fs // 2 * rows, cw),
        ]
        + [buf(a.dtype, *a.shape) for a in (extra, gain, gap, r_gain, gmap, pgain, w_out_pool)]
        + [
            dma(2), dma(4, 2), dma(7), dma(), dma(n_fs, 2), dma(), dma(n_fs),
            dma(4), dma(n_sp, n_fs), dma(3, n_sp), dma(3), dma(4), dma(4), dma(), dma(),
            dma(), dma(n_fs), dma(), dma(), dma(), dma(2, n_fs, 2), dma(), dma(2, 2), dma(), dma(),
            dma(), dma(), dma(n_sp, 2), dma(), dma(n_half, 2), dma(), dma(),
            pltpu.SemaphoreType.REGULAR,
        ],
        1, "layer", [pl.BlockSpec(memory_space=pltpu.HBM)] * len(args), 58,
    )(*args)
    return final[None]


def run(n_sp, n_fs, n_tp, *args):
    wr, width = args[2].shape
    whole = n_fs * wr % 128 == 0 and args[-1].shape[1] % 128 == 0 and args[0].shape[1] % 256 == 0
    return (fused if whole and width == n_fs * HEAD_DIM else body)(n_sp, n_fs, n_tp, *args)


def solution(mesh):
    sizes = dict(mesh.shape)
    weight = P(("sp", "fs"), "tp")
    placed = (
        P("fs", "sp", "tp"), P(), weight, weight, weight, weight, weight, P("tp"),
        P("fs", "sp", "tp"), P("tp"), P(), P("tp"), P("tp", ("sp", "fs")), P("tp", ("sp", "fs")),
    )
    return jax.shard_map(
        functools.partial(run, sizes["sp"], sizes["fs"], sizes["tp"]),
        mesh=mesh, in_specs=placed, out_specs=P("fs", ("sp", "tp"), None), check_vma=False,
    )
```

```python
import functools
import jax
import jax.numpy as jnp
from jax import lax
from jax.experimental import pallas as pl
from jax.experimental.pallas import tpu as pltpu
from jax.sharding import PartitionSpec as P

HEAD_DIM = 128
POOL_GROUPS = 4
BLOCK = 64
EPS = 1e-06
HIGH = lax.Precision.HIGHEST
MESH = pl.DeviceIdType.MESH
BF = jnp.bfloat16
F32 = jnp.float32


def place():
    return lax.axis_index("sp"), lax.axis_index("fs"), lax.axis_index("tp")


def rcopy(src, dst, ssem, rsem, dev):
    return pltpu.make_async_remote_copy(
        src_ref=src, dst_ref=dst, send_sem=ssem, recv_sem=rsem, device_id=dev, device_id_type=MESH
    )


def greet(devs):
    barrier = pltpu.get_barrier_semaphore()
    for cond, dev in devs:
        def tell(dev=dev):
            pl.semaphore_signal(barrier, inc=1, device_id=dev, device_id_type=MESH)
        if cond is None:
            tell()
        else:
            pl.when(cond)(tell)
    pl.semaphore_wait(barrier, sum(1 if cond is None else jnp.where(cond, 1, 0) for cond, _ in devs))


def square(f):
    near = f + 1 - 2 * lax.rem(f, 2)
    return near, lax.rem(f + 2, 4), lax.rem(near + 2, 4)


def project_kernel(
    n_sp, n_fs, n_tp, tok, wq, wf, wi, wo, wp, extra, gain, gmap, pgain, wor, wop, z_ref, e_ref, ow_ref,
    wsrc, xs, ws, acc, x_send, x_recv, f_send, d_send, d_recv, w_send, w_recv, zr_send, zl_send, e_send, e_recv,
):
    s, f, t = place()
    rows, half = tok.shape
    part = rows // 2
    mats = (wq, wf, wi, wo, wp)
    wr, width = wq.shape
    ch = width // n_fs
    for i, w in enumerate(mats):
        for g in range(n_fs):
            wsrc[g, :, i * ch : (i + 1) * ch] = w[:, g * ch : (g + 1) * ch]
    other = (s, f, 1 - t)
    px, py, pd = square(f)
    order = (f, px, py, pd)
    up, down = (s + 1, f, t), (s - 1, f, t)
    has_up, has_down = s < n_sp - 1, s > 0
    greet([(None, other)] + [(None, (s, g, t)) for g in order[1:]] + [(has_up, up), (has_down, down)])

    def cols(c):
        return pl.ds(pl.multiple_of(c * half, half), half)

    def span(a, b):
        return pl.ds(pl.multiple_of((a * n_fs + b) * wr, wr), wr)

    def slot(a, b):
        return ws.at[span(a, b), :]

    def to_up(src, a, b):
        return rcopy(src, slot(a, b), zr_send.at[a, b], w_recv.at[a, b], up)

    def to_down(src, a, b):
        return rcopy(src, slot(a, b), zl_send.at[a, b], w_recv.at[a, b], down)

    sends = []

    def send(c):
        c.start()
        sends.append(c)

    def x_slot(g, h, c):
        return xs.at[g, h * part : (h + 1) * part, cols(c)]

    own = wsrc.at[f]
    pl.when(has_up)(lambda: to_up(own, s, f).start())
    pl.when(has_down)(lambda: to_down(own, s, f).start())
    for i, g in enumerate((pd, px, py)):
        send(rcopy(wsrc.at[g], slot(s, f), w_send.at[i], w_recv.at[s, f], (s, g, t)))
    for i, (p, hs) in enumerate(((px, (0, 1)), (py, (1, 0)))):
        for h in hs:
            send(rcopy(tok.at[h * part : (h + 1) * part, :], x_slot(f, h, t), x_send.at[i, h], x_recv.at[f, h], (s, p, t)))
    for h in range(2):
        send(rcopy(tok.at[h * part : (h + 1) * part, :], x_slot(f, h, t), d_send.at[f, h], d_recv.at[f, h], other))
    for i, g in enumerate(order[1:]):
        send(rcopy(extra.at[g], e_ref.at[f], e_send.at[i], e_recv.at[f], (s, g, t)))
    ws[span(s, f), :] = wsrc[f]
    xs[f, :, cols(t)] = tok[...]
    e_ref[f] = extra[f]
    ow_ref[0:width, :] = wor[...]
    gd = gmap.shape[1]
    for i in range(width // gd):
        at = slice(i * gd, (i + 1) * gd)
        scaled = (gmap[t * (width // gd) + i].astype(F32) * pgain[:, at]).astype(BF)
        folded = jnp.dot(scaled, wop[at, :], preferred_element_type=F32)
        ow_ref[width + i * gd : width + (i + 1) * gd, :] = folded.astype(BF)

    for g in order[1:]:
        to_up(slot(s, g), s, g).wait_recv()
        pl.when(has_up)(lambda: to_up(slot(s, g), s, g).start())
        pl.when(has_down)(lambda: to_down(slot(s, g), s, g).start())

    def landed(g, h):
        here = x_slot(g, h, t)
        rcopy(here, here, d_send.at[g, h], x_recv.at[g, h], other).wait_recv()
        return here

    def hand_on(g, h, here):
        send(rcopy(here, here, d_send.at[g, h], d_recv.at[g, h], other))

    for i, (g, h, onto) in enumerate(((px, 0, py), (py, 1, px))):
        here = landed(g, h)
        send(rcopy(here, here, f_send.at[i], x_recv.at[g, h], (s, onto, t)))
        hand_on(g, h, here)

    def relay(d):
        for g in order:
            a = s - d

            @pl.when(a >= 0)
            def _():
                to_up(slot(a, g), a, g).wait_recv()
                pl.when(has_up)(lambda: to_up(slot(a, g), a, g).start())
            b = s + d

            @pl.when(b < n_sp)
            def _():
                to_down(slot(b, g), b, g).wait_recv()
                pl.when(has_down)(lambda: to_down(slot(b, g), b, g).start())

    def add(a):
        k = pl.ds(pl.multiple_of(a * n_fs * wr, n_fs * wr), n_fs * wr)

        def each(i, _):
            acc[i] += jnp.dot(xs[i, :, k], ws[k, :], preferred_element_type=F32)
            return 0

        lax.fori_loop(0, n_fs, each, 0)

    def multiply(d):
        pl.when(s - d >= 0)(lambda: add(s - d))
        pl.when(s + d < n_sp)(lambda: add(s + d))

    relay(1)
    for g, h in ((px, 1), (py, 0), (pd, 0), (pd, 1)):
        hand_on(g, h, landed(g, h))
    for d in range(2, n_sp - 1):
        relay(d)
    for g in order:
        for h in range(2):
            here = x_slot(g, h, 1 - t)
            rcopy(here, here, d_send.at[g, h], d_recv.at[g, h], other).wait_recv()
    for g in order[1:]:
        rcopy(extra.at[f], e_ref.at[g], e_send.at[0], e_recv.at[g], other).wait_recv()
    for c in sends:
        c.wait_send()

    def norm(j, _):
        tile = 16
        per = rows // tile
        at = (j // per, pl.ds(pl.multiple_of(lax.rem(j, per) * tile, tile), tile))
        feats = xs[at[0], at[1], :].astype(F32)
        scale = lax.rsqrt(jnp.mean(feats * feats, axis=-1, keepdims=True) + EPS)
        xs[at[0], at[1], :] = (feats * scale * gain[...]).astype(BF)
        return 0

    lax.fori_loop(0, n_fs * rows // 16, norm, 0, unroll=2)

    if n_fs * wr % 128 == 0:
        own_k = pl.ds(pl.multiple_of(s * n_fs * wr, n_fs * wr), n_fs * wr)

        def begin(i, _):
            acc[i] = jnp.dot(xs[i, :, own_k], ws[own_k, :], preferred_element_type=F32)
            return 0

        lax.fori_loop(0, n_fs, begin, 0)
        for d in range(1, n_sp - 1):
            multiply(d)
        relay(n_sp - 1)
        multiply(n_sp - 1)

        def finish(i, _):
            z_ref[i] = acc[i].astype(BF)
            return 0
    else:
        relay(n_sp - 1)

        def finish(i, _):
            z_ref[i] = jnp.dot(xs[i], ws[...], preferred_element_type=F32).astype(BF)
            return 0

    lax.fori_loop(0, n_fs, finish, 0)

    for d in range(n_sp):
        for g in order:
            a = s - d

            @pl.when((a >= 0) & has_up)
            def _():
                to_up(slot(a, g), a, g).wait_send()
            b = s + d

            @pl.when((b < n_sp) & has_down)
            def _():
                to_down(slot(b, g), b, g).wait_send()


def dot(a, b, dims):
    return lax.dot_general(a, b, (dims, ((), ())), precision=HIGH, preferred_element_type=F32)


def state_kernel(
    n_sp, group_dim, z, e_all, gap, rec_gain, act, sq_out,
    local, qd, own_st, own_de, st_in, de_in, rim, s_send, s_recv, c_send, c_recv, g_send, g_recv,
):
    s, f, t = place()
    n_fs, rows, _ = z.shape
    ch = HEAD_DIM
    reach = rim.shape[1]
    devs = []
    for d in range(1, n_sp):
        devs.append((s + d < n_sp, (s + d, f, t)))
        devs.append((s - d >= 0, (s - d, f, t)))
    greet(devs)
    edge = rcopy(z.at[:, rows - reach :, 4 * ch :], rim, g_send, g_recv, (s + 1, f, t))
    pl.when(s < n_sp - 1)(edge.start)
    mine = pl.ds(pl.multiple_of(f * ch, ch), ch)
    gap_f = gap[:, mine]
    gain_f = rec_gain[:, mine]
    at = lax.broadcasted_iota(jnp.int32, (BLOCK, BLOCK), 0)
    causal = at >= lax.broadcasted_iota(jnp.int32, (BLOCK, BLOCK), 1)
    lower = causal.astype(F32)

    def one(g, _):
        state = jnp.zeros((ch, ch), F32)
        so_far = jnp.zeros((1, ch), F32)
        e_cols = e_all[g].T
        for n in range(rows // BLOCK):
            here = slice(n * BLOCK, (n + 1) * BLOCK)
            q, fo, v = (z[g, here, i * ch : (i + 1) * ch].astype(F32) for i in range(3))
            q = jax.nn.silu(q)
            k = gap_f * jax.nn.sigmoid(-fo)
            lo = n * BLOCK % 128
            lane = n * BLOCK // 128
            logs = jnp.log1p(-k) + e_cols[lo : lo + BLOCK, lane : lane + 1]
            within = dot(lower, logs, ((1,), (0,)))
            end = within[BLOCK - 1 :]
            q_up = q * jnp.exp(within)
            scores = jnp.where(causal, dot(q_up, k * jnp.exp(-within), ((1,), (1,))), 0.0)
            out = dot(scores, v, ((1,), (0,)))
            if n:
                out = out + dot(q_up, state, ((1,), (1,)))
            local[g, here, :] = out
            qd[g, here, :] = q_up * jnp.exp(so_far)
            state = state * jnp.exp(end) + dot(v.T, k * jnp.exp(end - within), ((1,), (0,)))
            so_far = so_far + end
        own_st[g] = state.astype(BF)
        own_de[g] = jnp.broadcast_to(jnp.exp(so_far), (8, ch))
        return 0

    lax.fori_loop(0, n_fs, one, 0)

    def pair(d):
        dev = (s + d, f, t)
        return (
            rcopy(own_st, st_in.at[d - 1], s_send.at[d - 1], s_recv.at[d - 1], dev),
            rcopy(own_de, de_in.at[d - 1], c_send.at[d - 1], c_recv.at[d - 1], dev),
        )

    for d in range(1, n_sp):
        @pl.when(s + d < n_sp)
        def _():
            for c in pair(d):
                c.start()

        @pl.when(s - d < 0)
        def _():
            st_in[d - 1] = jnp.zeros(st_in.shape[1:], st_in.dtype)
            de_in[d - 1] = jnp.ones(de_in.shape[1:], de_in.dtype)
    pl.when(s == 0)(lambda: rim.__setitem__(Ellipsis, jnp.zeros(rim.shape, rim.dtype)))
    pl.when(s > 0)(edge.wait_recv)
    group = (t * n_fs * ch + f * ch) // group_dim
    spot = s * rows + lax.broadcasted_iota(jnp.int32, (rows, ch), 0)
    window = 2
    for level in range(1, POOL_GROUPS):
        window = jnp.where(group == level, 2 ** (level + 1), window)
    counts = jnp.minimum(spot + 1, window).astype(F32)
    for g in range(n_fs):
        zp = z[g, :, 4 * ch :].astype(F32)
        running = jnp.concatenate([rim[g].astype(F32), zp], axis=0)
        total = None
        for level in range(POOL_GROUPS):
            stride = 2**level
            running = running[stride:] + running[:-stride]
            now = running[running.shape[0] - rows :]
            total = now if level == 0 else jnp.where(group == level, now, total)
        act[1, g * rows : (g + 1) * rows, :] = (total / counts - zp).astype(BF)
    for d in range(1, n_sp):
        @pl.when(s - d >= 0)
        def _():
            for c in pair(d):
                c.wait_recv()

    ones = jnp.ones((8, ch), F32)

    def finish(g, _):
        total = jnp.zeros((ch, ch), F32)
        for d in range(n_sp - 2, -1, -1):
            total = de_in[d, g, 0:1, :] * total + st_in[d, g].astype(F32)
        rec = local[g] + dot(qd[g], total, ((1,), (1,)))
        sums = dot(ones, rec * rec, ((1,), (1,)))
        for i in range(rows // 128):
            sq_out[g, i : i + 1, :] = sums[0:1, i * 128 : (i + 1) * 128]
        gate = jax.nn.silu(z[g, :, 3 * ch : 4 * ch].astype(F32))
        act[0, pl.ds(pl.multiple_of(g * rows, rows), rows), :] = (rec * gain_f * gate).astype(BF)
        return 0

    sq_out[...] = jnp.zeros(sq_out.shape, F32)
    lax.fori_loop(0, n_fs, finish, 0)
    for d in range(1, n_sp):
        @pl.when(s + d < n_sp)
        def _():
            for c in pair(d):
                c.wait_send()
    pl.when(s < n_sp - 1)(edge.wait_send)


def mix_kernel(
    n_sp, n_fs, n_tp, act, sq, ow, final,
    out, acts, sq_all, ow_all, relay_buf, wbuf, part,
    a_send, a_recv, f_send, d_send, d_recv, q_send, q_recv,
    up_send, down_send, o_recv, od_send, od_recv, m_send, m_recv,
):
    s, f, t = place()
    n_half = n_sp // n_tp
    rows = act.shape[1] // n_fs
    half = rows // n_tp
    width, cw = ow.shape[0] // 2, ow.shape[1]
    other = (s, f, 1 - t)
    px, py, pd = square(f)
    up, down = (s + 1, f, t), (s - 1, f, t)
    has_up, has_down = s < n_sp - 1, s > 0
    greet(
        [(None, other)]
        + [(None, (s, g, u)) for g in (px, py, pd) for u in (t, 1 - t)]
        + [(has_up, up), (has_down, down)]
    )

    def to_up(src, a):
        return rcopy(src, relay_buf.at[a], up_send.at[a], o_recv.at[a], up)

    def to_down(src, a):
        return rcopy(src, relay_buf.at[a], down_send.at[a], o_recv.at[a], down)

    def to_other(src, a):
        return rcopy(src, ow_all.at[lax.rem(a, n_half), t], od_send.at[a], od_recv.at[a], other)

    def keep(src, a):
        mine = a // n_half == t

        @pl.when(mine)
        def _():
            ow_all[lax.rem(a, n_half), t] = src[...]

        pl.when(jnp.logical_not(mine))(lambda: to_other(src, a).start())

    sends = []

    def send(c):
        c.start()
        sends.append(c)

    for i, (p, order) in enumerate(((px, (0, 1)), (py, (1, 0)))):
        for h in order:
            send(rcopy(act.at[h], acts.at[t, f, h], a_send.at[i, h], a_recv.at[f, h], (s, p, t)))
    pl.when(has_up)(lambda: to_up(ow, s).start())
    pl.when(has_down)(lambda: to_down(ow, s).start())
    for h in range(2):
        send(rcopy(act.at[h], acts.at[t, f, h], d_send.at[f, h], d_recv.at[f, h], other))
    for i, g in enumerate((px, py, pd)):
        for u in range(n_tp):
            send(rcopy(sq, sq_all.at[t, f], q_send.at[i, u], q_recv.at[t, f], (s, g, u)))
    send(rcopy(sq, sq_all.at[t, f], q_send.at[n_fs - 1, 0], q_recv.at[t, f], other))
    acts[t, f] = act[...]
    sq_all[t, f] = sq[...]
    keep(ow, s)

    def landed(g, h):
        here = acts.at[t, g, h]
        rcopy(here, here, d_send.at[g, h], a_recv.at[g, h], other).wait_recv()
        return here

    def hand_on(g, h, here):
        send(rcopy(here, here, d_send.at[g, h], d_recv.at[g, h], other))

    for i, (g, h, onto) in enumerate(((px, 0, py), (py, 1, px))):
        here = landed(g, h)
        send(rcopy(here, here, f_send.at[i], a_recv.at[g, h], (s, onto, t)))
        hand_on(g, h, here)

    def step(d):
        a = s - d

        @pl.when(a >= 0)
        def _():
            to_up(relay_buf.at[a], a).wait_recv()
            pl.when(has_up)(lambda: to_up(relay_buf.at[a], a).start())
            keep(relay_buf.at[a], a)
        b = s + d

        @pl.when(b < n_sp)
        def _():
            to_down(relay_buf.at[b], b).wait_recv()
            pl.when(has_down)(lambda: to_down(relay_buf.at[b], b).start())
            keep(relay_buf.at[b], b)

    for d in range(1, n_sp):
        step(d)
    for g, h in ((px, 1), (py, 0), (pd, 0), (pd, 1)):
        hand_on(g, h, landed(g, h))
    for i in range(n_half):
        a = t * n_half + i
        here = ow_all.at[i, 1 - t]
        rcopy(here, here, od_send.at[a], od_recv.at[a], other).wait_recv()
    for i in range(n_half):
        for u in range(n_tp):
            for k in range(2):
                wbuf[k, u * width : (u + 1) * width, i * cw : (i + 1) * cw] = ow_all[i, u, k * width : (k + 1) * width, :]
    for g in (px, py, pd):
        for u in range(n_tp):
            here = sq_all.at[u, g]
            rcopy(here, here, q_send.at[0, 0], q_recv.at[u, g], other).wait_recv()
    here = sq_all.at[1 - t, f]
    rcopy(here, here, q_send.at[0, 0], q_recv.at[1 - t, f], other).wait_recv()
    for g in (f, px, py, pd):
        for h in range(2):
            here = acts.at[1 - t, g, h]
            rcopy(here, here, d_send.at[g, h], d_recv.at[g, h], other).wait_recv()

    def piece(g, u):
        return rcopy(part.at[g, u], out.at[f, t], m_send.at[g, u], m_recv.at[f, t], (s, g, u))

    def spread(g):
        for u in range(n_tp):
            c = piece(g, u)
            c.start()
            sends.append(c)

    last = None
    for g in (pd, f, px, py):
        here = pl.ds(pl.multiple_of(g * rows, rows), rows)
        sums = sum(sq_all[u, i, g] for u in range(n_tp) for i in range(n_fs))
        scale = lax.rsqrt(sums / (n_tp * width) + EPS).T
        scale = jnp.concatenate([scale[:, i : i + 1] for i in range(rows // 128)], axis=0)
        left = [
            jnp.concatenate([acts[u, i, h, here, :] for u in range(n_tp) for i in range(n_fs)], axis=1)
            for h in range(2)
        ]
        mixed = (
            jnp.dot(left[0], wbuf[0], preferred_element_type=F32) * scale
            + jnp.dot(left[1], wbuf[1], preferred_element_type=F32)
        ).astype(BF)
        for u in range(n_tp):
            part[g, u] = mixed[u * half : (u + 1) * half]
        if last is not None and last is not f:
            spread(last)
        if last is f:
            c = piece(f, 1 - t)
            c.start()
            sends.append(c)
        last = g
    out[f, t] = part[f, t]
    for i in range(n_half):
        to_other(ow, (1 - t) * n_half + i).wait_send()
    for d in range(n_sp):
        a, b = s - d, s + d

        @pl.when((a >= 0) & has_up)
        def _():
            to_up(ow, a).wait_send()

        @pl.when((b < n_sp) & has_down)
        def _():
            to_down(ow, b).wait_send()
    spread(last)
    for c in sends:
        c.wait_send()
    for g in (px, py, pd):
        for u in range(n_tp):
            here = out.at[g, u]
            rcopy(here, here, m_send.at[g, u], m_recv.at[g, u], other).wait_recv()
    here = out.at[f, 1 - t]
    rcopy(here, here, m_send.at[f, 1 - t], m_recv.at[f, 1 - t], other).wait_recv()
    for u in range(n_tp):
        for i in range(n_half):
            for g in range(n_fs):
                lo = ((u * n_half + i) * n_fs + g) * cw
                final[:, lo : lo + cw] = out[g, u, :, i * cw : (i + 1) * cw]


def vmem(count):
    return [pl.BlockSpec(memory_space=pltpu.VMEM)] * count


def dma(*shape):
    return pltpu.SemaphoreType.DMA(shape) if shape else pltpu.SemaphoreType.DMA


def comm(kernel, outs, scratch, number, name, ins=None, limit=60):
    return pl.pallas_call(
        kernel,
        out_shape=[jax.ShapeDtypeStruct(a, b) if ins is None else pltpu.VMEM(a, b) for a, b in outs],
        **({"out_specs": vmem(len(outs))} if ins is None else {"in_specs": ins, "out_specs": [pl.BlockSpec(memory_space=pltpu.VMEM)] * len(outs)}),
        scratch_shapes=scratch,
        compiler_params=pltpu.CompilerParams(
            collective_id=number, has_side_effects=True, vmem_limit_bytes=limit * 1024 * 1024
        ),
        name=name,
    )


def body(
    n_sp, n_fs, n_tp, tokens, norm_gain, w_query, forget_weight, w_input, w_outgate, w_pool, forget_gap,
    extra_decay, rec_gain, group_weight, pool_gain, recurrent_output_weight, w_out_pool,
):
    s, f, t = place()
    rows, half = tokens.shape[1:]
    width = w_query.shape[1]
    ch = width // n_fs
    n_w = 5
    wr = w_query.shape[0]
    lanes = rows // 128
    extra = jnp.pad(extra_decay[0].T.reshape(n_fs, lanes, 128), ((0, 0), (0, 8 - lanes), (0, 0)))
    cw = w_out_pool.shape[1]
    z, e_all, ow = comm(
        functools.partial(project_kernel, n_sp, n_fs, n_tp),
        [((n_fs, rows, n_w * ch), BF), ((n_fs, 8, 128), F32), ((2 * width, cw), BF)],
        [
            pltpu.VMEM((n_fs, wr, n_w * ch), BF), pltpu.VMEM((n_fs, rows, n_tp * half), BF),
            pltpu.VMEM((n_sp * n_fs * wr, n_w * ch), BF), pltpu.VMEM((n_fs, rows, n_w * ch), F32),
            dma(2, 2), dma(n_fs, 2), dma(2), dma(n_fs, 2), dma(n_fs, 2), dma(n_fs - 1), dma(n_sp, n_fs),
            dma(n_sp, n_fs), dma(n_sp, n_fs), dma(n_fs - 1), dma(n_fs),
        ],
        1, "project",
    )(
        tokens[0], w_query, forget_weight, w_input, w_outgate, w_pool, extra, norm_gain[None],
        group_weight, pool_gain[None], recurrent_output_weight, w_out_pool,
    )
    n_half = n_sp // n_tp
    act, sq = comm(
        functools.partial(state_kernel, n_sp, group_weight.shape[1]),
        [((2, n_fs * rows, ch), BF), ((n_fs, 8, 128), F32)],
        [
            pltpu.VMEM((n_fs, rows, ch), F32), pltpu.VMEM((n_fs, rows, ch), F32),
            pltpu.VMEM((n_fs, ch, ch), BF), pltpu.VMEM((n_fs, 8, ch), F32),
            pltpu.VMEM((n_sp - 1, n_fs, ch, ch), BF), pltpu.VMEM((n_sp - 1, n_fs, 8, ch), F32),
            pltpu.VMEM((n_fs, 2**POOL_GROUPS, ch), BF),
            dma(n_sp - 1), dma(n_sp - 1), dma(n_sp - 1), dma(n_sp - 1), dma(), dma(),
        ],
        2, "state",
    )(z, e_all, forget_gap[None], rec_gain[None])
    out_shape = (n_fs, n_tp, rows // n_tp, n_half * cw)
    (final,) = comm(
        functools.partial(mix_kernel, n_sp, n_fs, n_tp),
        [((rows // n_tp, n_tp * n_half * n_fs * cw), BF)],
        [
            pltpu.VMEM(out_shape, BF), pltpu.VMEM((n_tp, n_fs) + act.shape, BF), pltpu.VMEM((n_tp, n_fs) + sq.shape, F32),
            pltpu.VMEM((n_half, n_tp) + ow.shape, BF), pltpu.VMEM((n_sp,) + ow.shape, BF),
            pltpu.VMEM((2, n_tp * width, n_half * cw), BF), pltpu.VMEM(out_shape, BF),
            dma(2, 2), dma(n_fs, 2), dma(2), dma(n_fs, 2), dma(n_fs, 2), dma(n_fs, n_tp), dma(n_tp, n_fs),
            dma(n_sp), dma(n_sp), dma(n_sp), dma(n_sp), dma(n_sp), dma(n_fs, n_tp), dma(n_fs, n_tp),
        ],
        3, "mix",
    )(act, sq, ow)
    return final[None]


def mm(a, b, dims):
    return lax.dot_general(a, b, (dims, ((), ())), preferred_element_type=F32)


NN, NT, TN = ((1,), (0,)), ((1,), (1,)), ((0,), (0,))


def layer_kernel(
    n_sp, n_fs, n_tp, tok, wq, wf, wi, wo, wp, extra_in, gain_in, gap_in, rec_gain_in, gmap_in, pgain_in, wor, wop_in, final,
    src0, src1, src2, src3, ws0, ws1, ws2, ws3, xs, xn, acc0, acc1, acc2, acc3, k_buf, rel, st_buf, lead, e_src, e_all, local, qd, own_st, own_de,
    t_out, t_in, rim_src, rim, acts, sq_src, sq_all, ow_buf, ow_oth, part, half_way,
    extra, gain, gap, rec_gain, gmap, pgain, wop,
    in_sem, w_in, p_in, x_send, x_recv, xd_send, xd_recv, w_send, w_recv, b_recv, ba_recv, up_send, dn_send, e_send, e_recv,
    t_send, t_recv, g_send, g_recv, a_send, a_recv, ad_send, ad_recv, q_send, q_recv,
    ou_send, on_send, o_recv, od_send, od_recv, m_send, m_recv, ready,
):
    s, f, t = place()
    rows, half = tok.shape
    cut = rows // 2
    wr, width = wq.shape
    ch = width // n_fs
    cw = wor.shape[1]
    n_half = n_sp // n_tp
    out_rows = rows // n_tp
    lanes = rows // 128
    size = 128
    blk = n_fs * wr
    total_k = n_sp * blk
    groups = ((wf, wi), (wp,), (wo,), (wq,))
    srcs, wss, accs = (src0, src1, src2, src3), (ws0, ws1, ws2, ws3), (acc0, acc1, acc2, acc3)
    other = (s, f, 1 - t)
    px, py, pd = square(f)
    order = (f, px, py, pd)
    up, down = (s + 1, f, t), (s - 1, f, t)
    has_up, has_down = s < n_sp - 1, s > 0
    is_end = jnp.logical_not(has_up & has_down)

    def when(cond, *copies):
        @pl.when(cond)
        def _():
            for c in copies:
                c.start()

    def sent(ref, sem):
        rcopy(ref, ref, sem, sem, other).wait_send()

    def came(ref, sem):
        rcopy(ref, ref, sem, sem, other).wait_recv()

    def cols(c):
        return pl.ds(pl.multiple_of(c * half, half), half)

    def span(a, b):
        return pl.ds(pl.multiple_of((a * n_fs + b) * wr, wr), wr)

    def slot(c, a, b):
        return wss[c].at[span(a, b), :]

    def block(c, a):
        return wss[c].at[pl.ds(pl.multiple_of(a * blk, blk), blk), :]

    def x_slot(g, h, c):
        return xs.at[g, h * cut : (h + 1) * cut, cols(c)]

    peers = (
        [(None, other)]
        + [(None, (s, px, t)), (None, (s, py, t))]
        + [(has_up, up), (has_down, down)]
    )
    barrier = pltpu.get_barrier_semaphore()
    for cond, dev in peers:
        def tell(dev=dev):
            pl.semaphore_signal(barrier, inc=1, device_id=dev, device_id_type=MESH)
        if cond is None:
            tell()
        else:
            pl.when(cond)(tell)
    for c in (1, 0, 3, 2):
        for i, w in enumerate(groups[c]):
            for j, g in enumerate(order):
                lane = pl.ds(pl.multiple_of(g * ch, ch), ch)
                into = wss[c].at[span(s, f), i * ch : (i + 1) * ch] if j == 0 else srcs[c].at[j - 1, :, i * ch : (i + 1) * ch]
                pltpu.make_async_copy(w.at[:, lane], into, w_in.at[c, min(j, 1)]).start()
        if c == 0:
            pltpu.make_async_copy(tok, xs.at[f, :, cols(t)], in_sem.at[0]).start()
            pltpu.make_async_copy(wor, ow_buf.at[s, 0], in_sem.at[1]).start()
    params = ((extra_in, extra), (gain_in, gain), (gmap_in, gmap), (pgain_in, pgain), (wop_in, wop), (gap_in, gap), (rec_gain_in, rec_gain))
    loads = [pltpu.make_async_copy(a, b, p_in.at[i]) for i, (a, b) in enumerate(params)]
    for c in loads:
        c.start()
    pl.semaphore_wait(barrier, sum(1 if cond is None else jnp.where(cond, 1, 0) for cond, _ in peers))

    def took(ref, sem):
        pltpu.make_async_copy(ref, ref, sem).wait()

    def to_up(src, b, a):
        return rcopy(src, slot(0, a, b), up_send.at[0], w_recv.at[a, b], up)

    def to_down(src, b, a):
        return rcopy(src, slot(0, a, b), dn_send.at[0], w_recv.at[a, b], down)

    def both(a, b):
        when(has_up, to_up(slot(0, a, b), b, a))
        when(has_down, to_down(slot(0, a, b), b, a))

    def b_up(c, a):
        return rcopy(block(c, a), block(c, a), up_send.at[c], b_recv.at[c - 1, a], up)

    def b_down(c, a):
        return rcopy(block(c, a), block(c, a), dn_send.at[c], b_recv.at[c - 1, a], down)

    def spread(c, some=(0, 1, 2)):
        for j in some:
            g = order[1 + j]
            rsem = w_recv.at[s, f] if c == 0 else ba_recv.at[c - 1]
            rcopy(srcs[c].at[j], slot(c, s, f), w_send.at[c], rsem, (s, g, t)).start()

    def chunk(c, g, dev):
        here = slot(c, s, g)
        return rcopy(here, here, (up_send if dev is up else dn_send).at[c], b_recv.at[c - 1, s], dev)

    def own_wait(c):
        came(wss[c].at[0 : (n_fs - 1) * wr, :], ba_recv.at[c - 1])

    def own_up(c, cond=True):
        when(has_up & cond, *(chunk(c, g, up) for g in order[1:]))

    def own_down(c, cond=True):
        when(has_down & cond, *(chunk(c, g, down) for g in order[1:]))

    low = 2 * s < n_sp
    inner = jnp.logical_not(is_end)
    mid_low = inner & low
    mid_high = inner & jnp.logical_not(low)

    def relay(c, d, gs=(None,), inward=True, outward=True):
        a, b = s - d, s + d

        def rising(extra):
            for g in gs:
                @pl.when((a >= 0) & has_up & extra)
                def _():
                    hop = to_up(slot(0, a, g), g, a) if c == 0 else b_up(c, a)
                    hop.wait_recv()
                    hop.start()

        def falling(extra):
            for g in gs:
                @pl.when((b < n_sp) & has_down & extra)
                def _():
                    hop = to_down(slot(0, b, g), g, b) if c == 0 else b_down(c, b)
                    hop.wait_recv()
                    hop.start()

        if inward:
            rising(low)
            falling(jnp.logical_not(low))
        if outward:
            falling(low)
            rising(jnp.logical_not(low))

    def arrive(c, d):
        for g in order if c == 0 else (None,):
            a, b = s - d, s + d

            @pl.when((a >= 0) & jnp.logical_not(has_up))
            def _():
                (to_up(slot(0, a, g), g, a) if c == 0 else b_up(c, a)).wait_recv()

            @pl.when((b < n_sp) & jnp.logical_not(has_down))
            def _():
                (to_down(slot(0, b, g), g, b) if c == 0 else b_down(c, b)).wait_recv()

    near = pl.ds(pl.multiple_of(jnp.where(has_down, blk, 0), blk), total_k - blk)
    far = pl.ds(pl.multiple_of(jnp.where(has_down, 0, total_k - blk), blk), blk)

    def gemm(c, p, k, more):
        out = jnp.dot(xn[p, :, k], wss[c][k, :], preferred_element_type=F32)
        accs[c][p] = accs[c][p] + out if more else out

    def main(c, p):
        pl.when(is_end)(lambda: gemm(c, p, near, False))
        pl.when(jnp.logical_not(is_end))(lambda: gemm(c, p, slice(0, total_k), False))

    def each_pair(step):
        def one(p, _):
            step(p)
            return 0

        lax.fori_loop(0, 2, one, 0)

    def last(c):
        arrive(c, n_sp - 1)
        pl.when(is_end)(lambda: each_pair(lambda p: gemm(c, p, far, True)))

    def landed(g, h):
        here = x_slot(g, h, t)
        came(here, x_recv.at[g, h])
        return here

    def hand_on(g, h):
        here = x_slot(g, h, t)
        rcopy(here, here, xd_send, xd_recv.at[g], other).start()

    def norm(j):
        g = order[j]
        came(xs.at[g, :, cols(1 - t)], xd_recv.at[g])
        tile = 16

        def each(i, _):
            at = pl.ds(pl.multiple_of(i * tile, tile), tile)
            feats = xs[g, at, :].astype(F32)
            scale = lax.rsqrt(jnp.mean(feats * feats, axis=-1, keepdims=True) + EPS)
            to = pl.ds(pl.multiple_of((j % 2) * rows + i * tile, tile), tile)
            xn[j // 2, to, :] = (feats * scale * gain[...]).astype(BF)
            return 0

        lax.fori_loop(0, rows // tile, each, 0, unroll=2)

    def cut_of(ref, a, k):
        mid = width // 2
        return ref.at[a, k // 3] if k in (0, 3) else ref.at[a, 1, (k - 1) * mid : k * mid, :]

    def ow_up(a, k):
        return rcopy(cut_of(ow_buf, a, k), cut_of(ow_buf, a, k), ou_send, o_recv.at[a, k], up)

    def ow_down(a, k):
        return rcopy(cut_of(ow_buf, a, k), cut_of(ow_buf, a, k), on_send, o_recv.at[a, k], down)

    def ow_share(a, k):
        i = lax.rem(a, n_half)
        when(a // n_half != t, rcopy(cut_of(ow_buf, a, k), cut_of(ow_oth, i, k), od_send, od_recv.at[i, k], other))

    def ow_start(a, k, rise, cond=True):
        to, has, edge_at = (s + 1, has_up, n_sp - 1) if rise else (s - 1, has_down, 0)
        ssem = ou_send if rise else on_send
        across = (to == edge_at) & (a // n_half != t)
        i = lax.rem(a, n_half)
        when(has & cond & jnp.logical_not(across), (ow_up if rise else ow_down)(a, k))
        when(has & cond & across, rcopy(cut_of(ow_buf, a, k), cut_of(ow_oth, i, k), ssem, od_recv.at[i, k], (to, f, 1 - t)))

    def ow_rise(d, k, cond=True):
        a = s - d

        @pl.when((a >= 0) & has_up & cond)
        def _():
            ow_up(a, k).wait_recv()
            ow_start(a, k, True)
            ow_share(a, k)

    def ow_fall(d, k, cond=True):
        b = s + d

        @pl.when((b < n_sp) & has_down & cond)
        def _():
            ow_down(b, k).wait_recv()
            ow_start(b, k, False)
            ow_share(b, k)

    def ow_relay(d, k):
        ow_rise(d, k)
        ow_fall(d, k)

    def ow_take(d, k):
        a, b = s - d, s + d
        pl.when((a >= 0) & jnp.logical_not(has_up) & (a // n_half == t))(ow_up(a, k).wait_recv)
        pl.when((b < n_sp) & jnp.logical_not(has_down) & (b // n_half == t))(ow_down(b, k).wait_recv)

    pl.semaphore_signal(ready, inc=1, device_id=(s, px, t), device_id_type=MESH)
    took(slot(1, s, f), w_in.at[1, 0])
    when(has_up, chunk(1, f, up))
    when(has_down, chunk(1, f, down))
    took(srcs[1], w_in.at[1, 1])
    spread(1, (0, 1))
    took(slot(0, s, f), w_in.at[0, 0])
    both(s, f)
    took(srcs[0], w_in.at[0, 1])
    spread(0, (0, 1))
    for c in (3, 2):
        took(slot(c, s, f), w_in.at[c, 0])
        when(has_up, chunk(c, f, up))
        when(has_down, chunk(c, f, down))
    pl.semaphore_wait(ready, 1)
    spread(1, (2,))
    spread(0, (2,))
    took(xs.at[f, :, cols(t)], in_sem.at[0])
    for p, hs in ((px, (0, 1)), (py, (1, 0))):
        for h in hs:
            rcopy(x_slot(f, h, t), x_slot(f, h, t), x_send, x_recv.at[f, h], (s, p, t)).start()
    for h in range(2):
        hand_on(f, h)
    for c in loads:
        c.wait()
    for g in range(n_fs):
        e_src[g] = jnp.broadcast_to(extra[g : g + 1, :], e_src.shape[1:])
    for g in order[1:]:
        rcopy(e_src.at[g], e_all.at[f], e_send, e_recv, (s, g, t)).start()
    for c in (3, 2):
        took(srcs[c], w_in.at[c, 1])
        spread(c)
    e_all[f] = e_src[f]
    own_wait(1)
    own_up(1)
    own_down(1)
    for g in order[1:]:
        came(slot(0, s, g), w_recv.at[s, g])
        both(s, g)
    gd = gmap.shape[1]
    for i in range(width // gd):
        at = slice(i * gd, (i + 1) * gd)
        scaled = (gmap[t * (width // gd) + i].astype(F32) * pgain[:, at]).astype(BF)
        ow_buf[s, 1, at, :] = jnp.dot(scaled, wop[at, :], preferred_element_type=F32).astype(BF)
    norm(0)
    relay(1, 1)
    relay(0, 1, order[:2])
    for g, h, onto in ((px, 0, py), (py, 1, px)):
        here = landed(g, h)
        rcopy(here, here, x_send, x_recv.at[g, h], (s, onto, t)).start()
        hand_on(g, h)
    for d in range(2, n_sp - 1):
        relay(1, d)
    relay(0, 1, order[2:])
    for g, h in ((px, 1), (py, 0)):
        landed(g, h)
        hand_on(g, h)
    for d in range(2, n_sp - 1):
        relay(0, d, order[:2])
    norm(1)
    for c in (3, 2):
        own_wait(c)
        own_up(c, is_end)
        own_down(c, is_end)
    took(ow_buf.at[s, 0], in_sem.at[1])
    for k in range(3):
        ow_start(s, k, True, is_end)
        ow_start(s, k, False, is_end)
        ow_share(s, k)
    norm(2)
    for d in range(1, n_sp):
        arrive(1, d)
    gemm(1, 0, slice(0, total_k), False)
    for d in range(2, n_sp - 1):
        relay(0, d, order[2:])
    own_up(3, inner)
    own_down(3, inner)
    for h in range(2):
        landed(pd, h)
        hand_on(pd, h)
    norm(3)
    gemm(1, 1, slice(0, total_k), False)

    reach = rim.shape[1]
    edge = rcopy(rim_src, rim, g_send, g_recv, up)

    def send_rim():
        for j in range(n_fs):
            rim_src[j] = acc1[j // 2, (j % 2 + 1) * rows - reach : (j % 2 + 1) * rows, :].astype(BF)
        when(has_up, edge)

    send_rim()
    relay(3, 1)
    own_up(2, mid_low)
    own_down(2, mid_high)
    for d in range(1, n_sp - 1):
        arrive(0, d)
    each_pair(lambda p: main(0, p))
    def chain():
        for g in range(n_fs):
            carry(g).wait_recv()
            t_out[g] = (own_st[g] + t_in[g].astype(F32) * own_de[g, 0:1, :]).astype(BF)
            carry(g).start()

    group = (t * n_fs * ch + f * ch) // gd
    spot = s * rows + lax.broadcasted_iota(jnp.int32, (rows, ch), 0)
    window = 2
    for level in range(1, POOL_GROUPS):
        window = jnp.where(group == level, 2 ** (level + 1), window)
    share = 1.0 / jnp.minimum(spot + 1, window).astype(F32)

    def rows_of(g):
        return pl.ds(pl.multiple_of(g * rows, rows), rows)

    def pool(j):
        zp = acc1[j // 2, j % 2 * rows : (j % 2 + 1) * rows, :].astype(BF).astype(F32)
        running = jnp.concatenate([rim[j].astype(F32), zp], axis=0)
        total = None
        for level in range(POOL_GROUPS):
            stride = 2**level
            running = running[stride:] + running[:-stride]
            now = running[running.shape[0] - rows :]
            total = now if level == 0 else jnp.where(group == level, now, total)
        acts[1, t, f, rows_of(order[j]), :] = (total * share - zp).astype(BF)

    part_rows = n_fs * rows // 2
    quarter = part_rows // 2

    def a_slot(k, u, g, h, q=None):
        lo, n = (h * part_rows, part_rows) if q is None else (h * part_rows + q * quarter, quarter)
        return acts.at[k, u, g, lo : lo + n, :]

    def a_share(k, g, h):
        here = a_slot(k, t, g, h)
        rcopy(here, here, ad_send, ad_recv.at[k, h], other).start()

    def publish(k):
        for h in range(2):
            here = a_slot(k, t, f, h)
            for p in (px, py):
                rcopy(here, here, a_send, a_recv.at[k, f, h], (s, p, t)).start()
            a_share(k, f, h)

    def a_forward(k, h):
        for g, q, onto in ((px, 0, py), (py, 1, px)):
            came(a_slot(k, t, g, h), a_recv.at[k, g, h])
            here = a_slot(k, t, g, h, q)
            rcopy(here, here, a_send, a_recv.at[k, g, h], (s, onto, t)).start()
            a_share(k, g, h)

    def a_rest(k, h):
        came(a_slot(k, t, pd, h), a_recv.at[k, pd, h])
        a_share(k, pd, h)

    def a_other(k, h):
        came(acts.at[k, 1 - t, :, h * part_rows : (h + 1) * part_rows, :], ad_recv.at[k, h])

    def pool_all():
        pl.when(has_down)(edge.wait_recv)
        for j in range(n_fs):
            pool(j)
        publish(1)

    @pl.when(jnp.logical_not(has_down))
    def _():
        rim[...] = jnp.zeros(rim.shape, BF)

    pool_all()
    last(0)
    came(e_all.at[0 : n_fs - 1], e_recv)

    mine = pl.ds(pl.multiple_of(f * ch, ch), ch)
    gap_f = gap[:, mine]
    gain_f = rec_gain[:, mine]
    at = lax.broadcasted_iota(jnp.int32, (size, size), 0)
    causal = at >= lax.broadcasted_iota(jnp.int32, (size, size), 1)
    lower = jnp.where(causal, 1.0, 0.0).astype(BF)
    lower = jnp.concatenate([lower, lower], axis=1)

    steps = rows // size

    def spots(j, n):
        lo = j % 2 * rows + n * size
        return slice(n * size, (n + 1) * size), slice(lo, lo + size)

    def states(j):
        state = None
        so_far = jnp.zeros((1, ch), F32)
        e_cols = e_all[order[j]].T
        for n in range(steps):
            here, there = spots(j, n)
            v = acc0[j // 2, there, ch : 2 * ch].astype(BF)
            k = gap_f * jax.nn.sigmoid(-acc0[j // 2, there, 0:ch].astype(BF).astype(F32))
            logs = jnp.log1p(-k) + e_cols[here, 0:1]
            high = logs.astype(BF)
            low = (logs - high.astype(F32)).astype(BF)
            within = mm(lower, jnp.concatenate([high, low], axis=0), NN)
            mid = within[size // 2 - 1 : size // 2]
            end = within[size - 1 :]
            k = (k * jnp.exp(mid - within)).astype(BF)
            k_buf[j, here, :] = k
            rel[j, here, :] = within - mid
            lead[j, n] = jnp.broadcast_to(jnp.exp(mid + so_far), lead.shape[2:])
            fresh = mm(v, k, TN) * jnp.exp(end - mid)
            if n:
                st_buf[j, n - 1] = (state * jnp.exp(mid)).astype(BF)
            state = state * jnp.exp(end) + fresh if n else fresh
            so_far = so_far + end
        own_st[j] = state
        own_de[j] = jnp.broadcast_to(jnp.exp(so_far), own_de.shape[1:])

    def reads(j):
        for n in range(steps):
            here, there = spots(j, n)
            v = acc0[j // 2, there, ch : 2 * ch].astype(BF)
            q = jax.nn.silu(acc3[j // 2, there, :].astype(BF).astype(F32)) * jnp.exp(rel[j, here, :])
            q_up = q.astype(BF)
            scores = jnp.where(causal, mm(q_up, k_buf[j, here, :], NT), 0.0).astype(BF)
            out = mm(scores, v, NN)
            if n:
                out = out + mm(q_up, st_buf[j, n - 1], NT)
            local[j, here, :] = out
            qd[j, here, :] = (q * lead[j, n, 0:1, :]).astype(BF)

    def carry(g):
        return rcopy(t_out.at[g], t_in.at[g], t_send, t_recv.at[g], up)

    for j in range(n_fs):
        states(j)

        @pl.when(jnp.logical_not(has_down))
        def _():
            t_in[j] = jnp.zeros(t_in.shape[1:], BF)
            t_out[j] = own_st[j].astype(BF)
            carry(j).start()

    for d in range(2, n_sp - 1):
        relay(3, d)
    own_up(2, mid_high)
    own_down(2, mid_low)
    relay(2, 1, outward=False)
    for d in range(1, n_sp - 1):
        arrive(3, d)
    each_pair(lambda p: main(3, p))
    last(3)
    for j in range(n_fs):
        reads(j)
    pl.when(mid_low)(chain)
    relay(2, 1, inward=False)
    for d in range(2, n_sp - 1):
        relay(2, d)
    for k in range(3):
        ow_start(s, k, False, inner)
    a_forward(1, 0)
    pl.when(mid_high)(chain)
    for k in range(3):
        ow_start(s, k, True, inner)
        ow_rise(1, k, mid_low)
        ow_fall(1, k, mid_high)
    pl.when(inner)(lambda: each_pair(lambda p: gemm(2, p, slice(0, total_k), False)))
    a_forward(1, 1)
    ones = jnp.ones((8, ch), BF)

    def finish(j):
        g = order[j]
        rec = local[j] + mm(qd[j], t_in[j], NT)
        sums = mm(ones, (rec * rec).astype(BF), NT)
        for i in range(lanes):
            sq_src[pl.ds(g * lanes + i, 1), :] = sums[0:1, i * 128 : (i + 1) * 128]
        gate = jax.nn.silu(acc2[j // 2, j % 2 * rows : (j % 2 + 1) * rows, :].astype(BF).astype(F32))
        acts[0, t, f, rows_of(g), :] = (rec * gain_f * gate).astype(BF)

    def finish_all():
        for j in range(n_fs):
            finish(j)
        for u, g in [(1 - t, f)] + [(u, g) for g in order[1:] for u in (t, 1 - t)]:
            rcopy(sq_src, sq_all.at[t * n_fs + f], q_send, q_recv, (s, g, u)).start()
        publish(0)
        sq_all[t * n_fs + f] = sq_src[...]

    pl.when(inner)(finish_all)
    for k in range(3):
        ow_rise(1, k, mid_high)
    pl.when(inner)(lambda: a_forward(0, 0))
    for k in range(3):
        ow_fall(1, k, mid_low)
    pl.when(inner)(lambda: a_forward(0, 1))
    for d in range(1, n_sp - 1):
        arrive(2, d)
    pl.when(is_end)(lambda: each_pair(lambda p: gemm(2, p, near, False)))
    last(2)
    @pl.when(has_down & jnp.logical_not(has_up))
    def _():
        for g in range(n_fs):
            carry(g).wait_recv()

    pl.when(is_end)(finish_all)
    for d in range(2, n_sp - 1):
        ow_relay(d, 0)
    for h in range(2):
        a_rest(1, h)
    for d in range(2, n_sp - 1):
        ow_relay(d, 1)
        ow_relay(d, 2)
    pl.when(is_end)(lambda: a_forward(0, 0))
    pl.when(is_end)(lambda: a_forward(0, 1))
    for d in range(1, n_sp - 1):
        for k in range(3):
            ow_take(d, k)
    came(sq_all.at[0 : n_tp * n_fs - 1], q_recv)
    sums = sum(sq_all[i] for i in range(n_tp * n_fs))
    scale = lax.rsqrt(sums / (n_tp * width) + EPS).T
    half_lanes = n_fs * lanes // 2
    scales = [
        jnp.concatenate([scale[:, h * half_lanes + i : h * half_lanes + i + 1] for i in range(half_lanes)], axis=0)
        for h in range(2)
    ]
    late = s - t * n_half >= n_half - 1

    def spot_of(a, g):
        return pl.ds(pl.multiple_of((a * n_fs + g) * cw, cw), cw)

    def at_part(i, g, u):
        return (i * n_fs + g) * n_tp + u

    def piece(i, g, u):
        return rcopy(part.at[at_part(i, g, u)], final.at[:, spot_of(t * n_half + i, f)], m_send, m_recv, (s, g, u))

    def weight_side(k, a, i, h):
        here = slice(h * part_rows, (h + 1) * part_rows)
        side, heads = k // 3, range(n_fs)
        if k in (1, 2):
            side, heads = 1, range((k - 1) * n_fs // 2, k * n_fs // 2)
        total = None
        for u, w in ((t, cut_of(ow_buf, a, k)), (1 - t, cut_of(ow_oth, i, k))):
            left = jnp.concatenate([acts[side, u, b, here, :] for b in heads], axis=1)
            now = jnp.dot(left, w[...], preferred_element_type=F32)
            total = now if total is None else total + now
        return total

    def rec_side(a, i, h):
        half_way[h] = weight_side(0, a, i, h) * scales[h]

    def first_side(a, i, h):
        half_way[h] = half_way[h] + weight_side(1, a, i, h)

    def pool_side(a, i, h, k=2):
        mixed = (half_way[h] + weight_side(k, a, i, h)).astype(BF)
        for g in range(h * n_fs // 2, (h + 1) * n_fs // 2):
            for u in range(n_tp):
                lo = (g * n_tp + u) * out_rows - h * part_rows
                part[at_part(i, g, u)] = mixed[lo : lo + out_rows]
                when((g != f) | (u != t), piece(i, g, u))

    def ow_got(j, k):
        i = jnp.where(late, n_half - 1 - j, j)
        if j == n_half - 1:
            ow_take(n_sp - 1, k)
        came(cut_of(ow_oth, i, k), od_recv.at[i, k])
        return t * n_half + i, i

    owns = []
    for j in range(n_half):
        if j == 0:
            for k in range(3):
                a, i = ow_got(0, k)
            for h in range(2):
                a_rest(0, h)
                for k in range(2):
                    a_other(k, h)
                rec_side(a, i, h)
                pool_side(a, i, h, 3)
        else:
            a, i = ow_got(j, 0)
            for h in range(2):
                rec_side(a, i, h)
            a, i = ow_got(j, 1)
            for h in range(2):
                first_side(a, i, h)
            a, i = ow_got(j, 2)
            for h in range(2):
                pool_side(a, i, h)
        own = pltpu.make_async_copy(part.at[at_part(i, f, t)], final.at[:, spot_of(a, f)], in_sem.at[min(j, 1)])
        own.start()
        owns.append(own)

    pieces = part.at[0 : n_half * (n_tp * n_fs - 1)]
    came(pieces, m_recv)
    for own in owns:
        own.wait()
    sent(pieces, m_send)
    sent(xs.at[0:3, :, 0:half], x_send)
    sent(xs.at[:, :, 0:half], xd_send)
    sent(e_src.at[0 : n_fs - 1], e_send)
    for c in range(4):
        sent(srcs[c], w_send.at[c])
    sent(acts.at[:, 0, 0:3], a_send)
    sent(acts.at[:, 0], ad_send)
    sent(sq_all.at[0 : n_tp * n_fs - 1], q_send)
    pl.when(jnp.logical_not(is_end))(lambda: sent(ow_oth, od_send))
    pl.when(is_end & (s // n_half != t))(lambda: sent(ow_oth.at[0], od_send))
    for v in range(n_sp):
        @pl.when(s == v)
        def _():
            if v < n_sp - 1:
                for c in range(4):
                    sent(wss[c].at[0 : (v + 1) * blk, :], up_send.at[c])
                sent(ow_buf.at[0 : v + 1], ou_send)
                sent(rim_src, g_send)
                sent(t_out, t_send)
            if v > 0:
                for c in range(4):
                    sent(wss[c].at[0 : (n_sp - v) * blk, :], dn_send.at[c])
                sent(ow_buf.at[0 : n_sp - v], on_send)


def fused(
    n_sp, n_fs, n_tp, tokens, norm_gain, w_query, forget_weight, w_input, w_outgate, w_pool, forget_gap,
    extra_decay, rec_gain, group_weight, pool_gain, recurrent_output_weight, w_out_pool,
):
    rows, half = tokens.shape[1:]
    wr, width = w_query.shape
    ch = width // n_fs
    cw = w_out_pool.shape[1]
    n_half = n_sp // n_tp
    feats = n_sp * n_fs * wr
    lanes = rows // 128

    def buf(kind, *shape):
        return pltpu.VMEM(shape, kind)

    args = (
        tokens[0], w_query, forget_weight, w_input, w_outgate, w_pool, extra_decay[0].T, norm_gain[None],
        forget_gap[None], rec_gain[None], group_weight, pool_gain[None], recurrent_output_weight, w_out_pool,
    )
    extra, gain, gap, r_gain, gmap, pgain = args[6:12]
    (final,) = comm(
        functools.partial(layer_kernel, n_sp, n_fs, n_tp),
        [((rows // n_tp, n_sp * n_fs * cw), BF)],
        [
            buf(BF, n_fs - 1, wr, 2 * ch), buf(BF, n_fs - 1, wr, ch), buf(BF, n_fs - 1, wr, ch), buf(BF, n_fs - 1, wr, ch),
            buf(BF, feats, 2 * ch), buf(BF, feats, ch), buf(BF, feats, ch), buf(BF, feats, ch),
            buf(BF, n_fs, rows, n_tp * half), buf(BF, 2, n_fs // 2 * rows, n_tp * half),
            buf(F32, 2, n_fs // 2 * rows, 2 * ch), buf(F32, 2, n_fs // 2 * rows, ch), buf(F32, 2, n_fs // 2 * rows, ch),
            buf(F32, 2, n_fs // 2 * rows, ch), buf(BF, n_fs, rows, ch), buf(F32, n_fs, rows, ch),
            buf(BF, n_fs, rows // 128, ch, ch), buf(F32, n_fs, rows // 128, 8, ch),
            buf(F32, n_fs, 8, rows), buf(F32, n_fs, 8, rows),
            buf(F32, n_fs, rows, ch), buf(BF, n_fs, rows, ch),
            buf(F32, n_fs, ch, ch), buf(F32, n_fs, 8, ch),
            buf(BF, n_fs, ch, ch), buf(BF, n_fs, ch, ch),
            buf(BF, n_fs, 2**POOL_GROUPS, ch), buf(BF, n_fs, 2**POOL_GROUPS, ch),
            buf(BF, 2, n_tp, n_fs, n_fs * rows, ch),
            buf(F32, n_fs * lanes, 128), buf(F32, n_tp * n_fs, n_fs * lanes, 128),
            buf(BF, n_sp, 2, width, cw), buf(BF, n_half, 2, width, cw),
            buf(BF, n_half * n_fs * n_tp, rows // n_tp, cw), buf(F32, 2, n_fs // 2 * rows, cw),
        ]
        + [buf(a.dtype, *a.shape) for a in (extra, gain, gap, r_gain, gmap, pgain, w_out_pool)]
        + [
            dma(2), dma(4, 2), dma(7), dma(), dma(n_fs, 2), dma(), dma(n_fs),
            dma(4), dma(n_sp, n_fs), dma(3, n_sp), dma(3), dma(4), dma(4), dma(), dma(),
            dma(), dma(n_fs), dma(), dma(), dma(), dma(2, n_fs, 2), dma(), dma(2, 2), dma(), dma(),
            dma(), dma(), dma(n_sp, 3), dma(), dma(n_half, 3), dma(), dma(),
            pltpu.SemaphoreType.REGULAR,
        ],
        1, "layer", [pl.BlockSpec(memory_space=pltpu.HBM)] * len(args), 58,
    )(*args)
    return final[None]


def run(n_sp, n_fs, n_tp, *args):
    wr, width = args[2].shape
    whole = n_fs * wr % 128 == 0 and args[-1].shape[1] % 128 == 0 and args[0].shape[1] % 256 == 0
    return (fused if whole and width == n_fs * HEAD_DIM else body)(n_sp, n_fs, n_tp, *args)


def solution(mesh):
    sizes = dict(mesh.shape)
    weight = P(("sp", "fs"), "tp")
    placed = (
        P("fs", "sp", "tp"), P(), weight, weight, weight, weight, weight, P("tp"),
        P("fs", "sp", "tp"), P("tp"), P(), P("tp"), P("tp", ("sp", "fs")), P("tp", ("sp", "fs")),
    )
    return jax.shard_map(
        functools.partial(run, sizes["sp"], sizes["fs"], sizes["tp"]),
        mesh=mesh, in_specs=placed, out_specs=P("fs", ("sp", "tp"), None), check_vma=False,
    )
```
